512 devices in a mesh: sp: 64 (over z, y), tp: 4 (over x), dp: 2 (over core).
Axes of the slice: x: 4, y: 8, z: 8, core: 2. Of those that a mesh axis runs over, the one named last changes fastest.
Arguments:
- latent: bfloat16 [2, 8192, 2048], P('dp', ('sp', 'tp')), may hold values from -10 to 10
- condition: bfloat16 [2, 2048], P('dp'), may hold values from -6 to 6
- context: bfloat16 [2, 512, 2048], P('dp', 'sp'), may hold values from -6 to 6
- context_source: bfloat16 [2048], replicated, may hold values from -6 to 6
- mod_weight: bfloat16 [3, 2048, 2048], P(None, 'sp', 'tp'), may hold values from -0.125 to 0.125
- norm_gain: bfloat16 [2048], replicated, may hold values from 0.099609375 to 1.8984375
- w_x: bfloat16 [2048, 2048], P('dp', 'tp'), may hold values from -0.125 to 0.125
- w_b: bfloat16 [2048, 512], P('dp', 'tp'), may hold values from -0.125 to 0.125
- w_c: bfloat16 [2048, 512], P('dp', 'tp'), may hold values from -0.125 to 0.125
- w_z: bfloat16 [2048, 2048], P('dp', 'tp'), may hold values from -0.125 to 0.125
- w_dt: bfloat16 [2, 2048, 32], P(None, 'dp', 'tp'), may hold values from -0.125 to 0.125
- conv_x: bfloat16 [3, 2048], P(None, 'tp'), may hold values from -3.5 to 3.5
- conv_b: bfloat16 [3, 512], P(None, 'tp'), may hold values from -3.5 to 3.5
- conv_c: bfloat16 [3, 512], P(None, 'tp'), may hold values from -3.5 to 3.5
- decay_rate: float32 [2, 32], P(None, 'tp'), may hold values from 0 to 1, as said below
- out_gain: bfloat16 [2048], P('tp'), may hold values from 0.099609375 to 1.8984375
- w_out: bfloat16 [2048, 2048], P(('tp', 'dp')), may hold values from -0.125 to 0.125
Outputs:
- update: bfloat16 [2, 8192, 2048], P('dp', ('sp', 'tp'))
The draws below stay inside these ranges and needn't reach their ends.
Inputs may be any that keep to these rules, and one draw needn't show every extreme that they name: `decay_rate`: positive rates.
All inputs are finite; a program needn't handle non-finite values.
Results may differ from the reference program's by a relative error of at most 0.014.
Values may be sent and summed in bfloat16 or wider, within the bound.
A program may use at most 128 MiB of HBM per device.

```python
import jax
import jax.numpy as jnp
from jax import lax

D = 2048
HEADS = 32
HEAD_DIM = 64
GROUPS = 4
STATE = 128
CONV = 3
BLOCK = 128
TOK_DEV = 128
CTX = 512
INNER = 2048
SEQ = 8192
BATCH = 2
N_TP = 4


def draw_latent(key, part):
    noise_key, dir_key, span_key, block_key = jax.random.split(key, 4)
    shape = (BATCH, SEQ, D)
    noise = jax.random.truncated_normal(noise_key, -4.0, 4.0, shape, jnp.float32)
    direction = jax.random.truncated_normal(dir_key, -3.0, 3.0, (D,), jnp.float32)
    coarse = jnp.repeat(jax.random.uniform(span_key, (BATCH, SEQ // TOK_DEV, 1), jnp.float32, -1.5, 1.5), TOK_DEV, axis=1)
    finer = jnp.repeat(jax.random.uniform(block_key, (BATCH, SEQ // BLOCK, 1), jnp.float32, -0.5, 0.5), BLOCK, axis=1)
    return (noise + (coarse + finer) * direction).astype(jnp.bfloat16)


def draw_decay_rate(key, part):
    slow_key, fast_key, pick_key = jax.random.split(key, 3)
    chain = SEQ + CTX
    slow_rate = jax.random.uniform(slow_key, (2, HEADS), jnp.float32, 0.6, 2.0) / chain
    fast_rate = jax.random.uniform(fast_key, (2, HEADS), jnp.float32, 0.015, 0.04)
    picked = jax.random.uniform(pick_key, (2, HEADS), jnp.float32) < 0.25
    return jnp.where(picked, fast_rate, slow_rate)


def levels(rng, shape, cuts, smallest, top_value):
    def one(axis_at, blocks):
        steps = jax.random.uniform(jax.random.fold_in(jax.random.fold_in(rng, 6), axis_at), (blocks,), jnp.float32, smallest / len(cuts), top_value / len(cuts))
        return jnp.repeat(jnp.exp(steps), shape[axis_at] // blocks).reshape((-1,) + (1,) * (len(shape) - axis_at - 1))

    loudness = one(*cuts[0])
    for cut in cuts[1:]:
        loudness = loudness * one(*cut)
    return loudness


def gaussian(rng, shape, scale, limit, cuts=(), held_as=jnp.bfloat16):
    values = jax.random.normal(rng, shape, jnp.float32) * scale
    if len(cuts) > 0:
        values = levels(rng, shape, cuts, -0.22, 0.18) * values
    return jnp.clip(values, min=-limit, max=limit).astype(held_as)


def setup_inputs(seed: int = 0) -> dict:
    key_of = jax.random.split(jax.random.key(seed), 18)
    latent = draw_latent(jax.random.fold_in(key_of[17], 71), 0)
    condition = gaussian(key_of[1], (BATCH, D), 1.0, 6.0, ((0, 2),))
    context = gaussian(key_of[2], (BATCH, CTX, D), 1.0, 6.0, ((0, 2), (1, 64)))
    context_source = gaussian(key_of[3], (D,), 1.0, 6.0)
    mod_weight = gaussian(key_of[4], (3, D, D), D ** -0.5, 0.125, ((1, 64), (2, 4)))
    norm_gain = jnp.clip(1.0 + 0.18 * jax.random.normal(key_of[5], (D,), jnp.float32), 0.099609375, 1.8984375).astype(jnp.bfloat16)
    w_x = gaussian(key_of[6], (D, INNER), D ** -0.5, 0.125, ((0, 2), (1, 4)))
    w_b = gaussian(key_of[7], (D, GROUPS * STATE), D ** -0.5, 0.125, ((0, 2), (1, 4)))
    w_c = gaussian(key_of[8], (D, GROUPS * STATE), D ** -0.5, 0.125, ((0, 2), (1, 4)))
    w_z = gaussian(key_of[9], (D, INNER), D ** -0.5, 0.125, ((0, 2), (1, 4)))
    w_dt = gaussian(key_of[10], (2, D, HEADS), D ** -0.5, 0.125, ((1, 2), (2, 4)))
    conv_x = gaussian(key_of[11], (CONV, INNER), CONV ** -0.5, 3.5, ((1, 4),))
    conv_b = gaussian(key_of[12], (CONV, GROUPS * STATE), CONV ** -0.5, 3.5, ((1, 4),))
    conv_c = gaussian(key_of[13], (CONV, GROUPS * STATE), CONV ** -0.5, 3.5, ((1, 4),))
    decay_rate = draw_decay_rate(jax.random.fold_in(key_of[17], 71), 0)
    out_gain = jnp.clip(1.0 + 0.18 * jax.random.normal(key_of[15], (INNER,), jnp.float32), 0.099609375, 1.8984375).astype(jnp.bfloat16)
    w_out = gaussian(key_of[16], (INNER, D), INNER ** -0.5, 0.125, ((0, 8),))
    return dict(latent=latent, condition=condition, context=context, context_source=context_source, mod_weight=mod_weight, norm_gain=norm_gain, w_x=w_x, w_b=w_b, w_c=w_c, w_z=w_z, w_dt=w_dt, conv_x=conv_x, conv_b=conv_b, conv_c=conv_c, decay_rate=decay_rate, out_gain=out_gain, w_out=w_out)


EPSILON = 1e-06

def rounded(values):
    return lax.optimization_barrier(values.astype(jnp.bfloat16)).astype(jnp.float32)

def modulated(source, gain_vec, shift_vec, scale_vec):
    values = source.astype(jnp.float32)
    normed = values * lax.rsqrt(lax.optimization_barrier(jnp.mean(values * values, axis=-1, keepdims=True)) + EPSILON)
    return (normed * gain_vec.astype(jnp.float32) * (1.0 + scale_vec) + shift_vec).astype(jnp.bfloat16)

def project(source, weight):
    return jnp.dot(source, weight, preferred_element_type=jnp.float32).astype(jnp.bfloat16)

def centred_conv(source, weight):
    total_rows = source.shape[0]
    reach_rows = weight.shape[0] // 2
    padded = jnp.pad(source.astype(jnp.float32), ((reach_rows, reach_rows), (0, 0)))
    tap_weights = weight.astype(jnp.float32)
    summed = jnp.zeros(source.shape, jnp.float32)
    for offset in range(weight.shape[0]):
        summed = summed + padded[offset:offset + total_rows] * tap_weights[offset]
    return jax.nn.silu(summed).astype(jnp.bfloat16)

def final_state(x_vals, b_vals, step_size, rate_head):
    total_rows, head_count = step_size.shape
    per_group = head_count // GROUPS
    moved_x = rounded(x_vals.reshape(total_rows, head_count, HEAD_DIM).astype(jnp.float32) * step_size[:, :, None])
    running = jnp.cumsum(-rate_head * step_size, axis=0)
    weight = jnp.exp(running[-1:] - running)
    scaled = (moved_x * weight[:, :, None]).reshape(total_rows, GROUPS, per_group, HEAD_DIM)
    b_wide = b_vals.reshape(total_rows, GROUPS, STATE).astype(jnp.float32)
    return jnp.einsum('sgn,sghp->ghpn', b_wide, scaled, precision=lax.Precision.HIGHEST)

def ssd_direction(x_vals, b_vals, c_vals, step_size, rate_head, start_state):
    total_rows, head_count = step_size.shape
    per_group = head_count // GROUPS
    blocks = total_rows // BLOCK
    moved_x = rounded(x_vals.reshape(total_rows, head_count, HEAD_DIM).astype(jnp.float32) * step_size[:, :, None])
    decay_log = -rate_head * step_size
    lower_part = jnp.arange(BLOCK)[:, None] >= jnp.arange(BLOCK)[None, :]

    def advance(carried_in, inputs):
        x_block, b_block, c_block, d_block = inputs
        running = jnp.cumsum(d_block, axis=0)
        across = running.T
        spread = across[:, :, None] - across[:, None, :]
        decay_mask = jnp.where(lower_part, jnp.exp(jnp.minimum(spread, 0.0)), 0.0).reshape(GROUPS, per_group, BLOCK, BLOCK)
        b_wide = b_block.astype(jnp.float32)
        c_wide = c_block.astype(jnp.float32)
        scores = jnp.einsum('lgn,sgn->gls', c_wide, b_wide)
        weights = rounded(scores[:, None] * decay_mask)
        x_group = x_block.reshape(BLOCK, GROUPS, per_group, HEAD_DIM)
        inside = jnp.einsum('ghls,sghp->lghp', weights, x_group)
        carried = jnp.einsum('lgn,ghpn->lghp', c_wide, rounded(carried_in))
        growth = jnp.exp(running).reshape(BLOCK, GROUPS, per_group, 1)
        to_end = jnp.exp(running[-1:] - running).reshape(BLOCK, GROUPS, per_group, 1)
        fresh_state = jnp.einsum('sgn,sghp->ghpn', b_wide, rounded(x_group * to_end))
        ending = carried_in * jnp.exp(running[-1]).reshape(GROUPS, per_group, 1, 1) + fresh_state
        return (ending, inside + growth * carried)
    _, outputs = lax.scan(advance, start_state, (moved_x.reshape(blocks, BLOCK, head_count, HEAD_DIM), b_vals.reshape(blocks, BLOCK, GROUPS, STATE), c_vals.reshape(blocks, BLOCK, GROUPS, STATE), decay_log.reshape(blocks, BLOCK, head_count)))
    return outputs.reshape(total_rows, head_count * HEAD_DIM)

def reference(latent, condition, context, context_source, mod_weight, norm_gain, w_x, w_b, w_c, w_z, w_dt, conv_x, conv_b, conv_c, decay_rate, out_gain, w_out):
    activation = rounded(jax.nn.silu(condition.astype(jnp.float32)))
    source_act = rounded(jax.nn.silu(context_source.astype(jnp.float32)))
    weight_wide = mod_weight.astype(jnp.float32)
    mod_latent = jnp.einsum('bd,kdc->kbc', activation, weight_wide)
    mod_context = jnp.einsum('d,kdc->kc', source_act, weight_wide)
    part_width = INNER // N_TP
    outputs = []
    for sample in range(latent.shape[0]):
        ctx_rows = modulated(context[sample], norm_gain, mod_context[0], mod_context[1])
        ctx_x = centred_conv(project(ctx_rows, w_x), conv_x)
        ctx_b = centred_conv(project(ctx_rows, w_b), conv_b)
        ctx_fwd = jax.nn.softplus(project(ctx_rows, w_dt[0]).astype(jnp.float32))
        ctx_bwd = jax.nn.softplus(project(ctx_rows, w_dt[1]).astype(jnp.float32))
        state_fwd = final_state(ctx_x, ctx_b, ctx_fwd, decay_rate[0])
        state_bwd = final_state(jnp.flip(ctx_x, 0), jnp.flip(ctx_b, 0), jnp.flip(ctx_bwd, 0), decay_rate[1])
        latent_rows = modulated(latent[sample], norm_gain, mod_latent[0, sample], mod_latent[1, sample])
        x_vals = centred_conv(project(latent_rows, w_x), conv_x)
        b_vals = centred_conv(project(latent_rows, w_b), conv_b)
        c_vals = centred_conv(project(latent_rows, w_c), conv_c)
        step_fwd = jax.nn.softplus(project(latent_rows, w_dt[0]).astype(jnp.float32))
        step_bwd = jax.nn.softplus(project(latent_rows, w_dt[1]).astype(jnp.float32))
        gate_in = project(latent_rows, w_z)
        total_rows = latent_rows.shape[0]
        out_fwd = ssd_direction(x_vals, b_vals, c_vals, step_fwd, decay_rate[0], state_fwd)
        out_bwd = jnp.flip(ssd_direction(jnp.flip(x_vals, 0), jnp.flip(b_vals, 0), jnp.flip(c_vals, 0), jnp.flip(step_bwd, 0), decay_rate[1], state_bwd), 0)
        gated = (out_fwd + out_bwd) * jax.nn.silu(gate_in.astype(jnp.float32))
        grouped = gated.reshape(total_rows, GROUPS, -1)
        normed = grouped * lax.rsqrt(lax.optimization_barrier(jnp.mean(grouped * grouped, axis=-1, keepdims=True)) + EPSILON) * out_gain.reshape(GROUPS, -1).astype(jnp.float32)
        normed_out = normed.reshape(total_rows, -1).astype(jnp.bfloat16)
        mixed = jnp.zeros((total_rows, w_out.shape[1]), jnp.float32)
        for part_idx in range(N_TP):
            lower_col = part_idx * part_width
            term = jnp.dot(normed_out[:, lower_col:lower_col + part_width], w_out[lower_col:lower_col + part_width], preferred_element_type=jnp.float32)
            mixed = mixed + rounded(term)
        outputs.append((mod_latent[2, sample] * mixed).astype(jnp.bfloat16))
    return jnp.stack(outputs)
```

```python
import functools

import jax
import jax.numpy as jnp
from jax import lax
from jax.experimental import pallas as pl
from jax.experimental.pallas import tpu as pltpu
from jax.sharding import Mesh
from jax.sharding import PartitionSpec as P

SP = ("sp_0", "sp_1")
SP_TP = ("sp_0", "sp_1", "tp")
MESH = pl.DeviceIdType.MESH
EPSILON = 1e-06
F32 = jnp.float32
BF16 = jnp.bfloat16
TOKENS = 128
STATE = 128
LANES = 128
HEADS = 8
PAIRS = HEADS // 2
INNER = 512
MIXED = INNER + 2 * STATE
COL_Z = MIXED
COL_DT = COL_Z + INNER
COLS = COL_DT + LANES
ROWS = TOKENS + 16
CTX_ROWS = 8
CTX_COLS = INNER + STATE + LANES


def rounded(v):
    return v.astype(BF16).astype(F32)


def silu(v):
    return v / (1.0 + jnp.exp(-v))


def softplus(v):
    return jnp.maximum(v, 0.0) + jnp.log1p(jnp.exp(-jnp.abs(v)))


def rows_of(shape):
    return lax.broadcasted_iota(jnp.int32, shape, 0)


def lanes_of(shape):
    return lax.broadcasted_iota(jnp.int32, shape, 1)


def running_sums(v, heads):
    n = v.shape[0]
    row = rows_of(v.shape)
    down = up = v
    step = 1
    while step < n:
        down = down + jnp.where(row >= step, pltpu.roll(down, step, 0), 0.0)
        up = up + jnp.where(row < n - step, pltpu.roll(up, n - step, 0), 0.0)
        step *= 2
    return jnp.where(lanes_of(v.shape) < heads, down, up)


def spread(v, head):
    shape = (v.shape[0], LANES)
    left = jnp.broadcast_to(v[:, head : head + 1], shape)
    right = jnp.broadcast_to(v[:, head + 1 : head + 2], shape)
    return jnp.where(lanes_of(shape) < LANES // 2, left, right)


def convolved(mid, low, high, taps):
    n = mid.shape[0]
    row = rows_of(mid.shape)
    before = jnp.where(row == 0, low, pltpu.roll(mid, 1, 0))
    after = jnp.where(row == n - 1, high, pltpu.roll(mid, n - 1, 0))
    summed = before * taps[0:1] + mid * taps[1:2] + after * taps[2:3]
    return rounded(silu(summed))


class Exchange:
    def __init__(self, axis, size, place, source, target, sent, got):
        self.copies = []
        for k in range(1, size):
            peer = lax.rem(place + k, size)
            self.copies.append(
                pltpu.make_async_remote_copy(
                    src_ref=source(peer),
                    dst_ref=target(),
                    send_sem=sent(k - 1),
                    recv_sem=got(k - 1),
                    device_id={axis: peer},
                    device_id_type=MESH,
                )
            )

    def start(self):
        for c in self.copies:
            c.start()
        return self

    def arrived(self):
        for c in self.copies:
            c.wait_recv()

    def left(self):
        for c in self.copies:
            c.wait_send()


def mixer(
    dims,
    small,
    modw,
    latent,
    context,
    w_x,
    w_b,
    w_c,
    w_z,
    w_dt,
    w_out,
    out,
    weights,
    out_weights,
    lat,
    ctx,
    placed,
    mod_z,
    mod_y,
    mod_x,
    edge_send,
    edge_recv,
    misc,
    hidden,
    feats,
    moved,
    growth,
    inside,
    ctx_gather,
    ctx_full,
    ctx_z,
    ctx_dz,
    state_send,
    state_recv,
    decay_y,
    tot_z,
    tot_dz,
    before,
    enter_send,
    enter_recv,
    normed,
    part_send,
    part_recv,
    local_sem,
    core_send,
    core_recv,
    mod_sems,
    lat_sems,
    edge_sems,
    y_sems,
    z_sems,
    part_sems,
):
    nz, ny, nx, model = dims
    width = model // nx
    own_rows = TOKENS // nx
    slab = STATE // ny
    z = lax.axis_index("sp_0")
    y = lax.axis_index("sp_1")
    x = lax.axis_index("tp")
    core = lax.axis_index("dp")
    place = z * ny + y
    count = nz * ny

    half = model // 2
    own_half = pl.ds(pl.multiple_of(core * half, half), half)
    out_half = pl.ds(pl.multiple_of(core * (INNER // 2), INNER // 2), INNER // 2)
    pieces = (
        (w_x, weights.at[own_half, pl.ds(0, INNER)]),
        (w_b, weights.at[own_half, pl.ds(INNER, STATE)]),
        (w_c, weights.at[own_half, pl.ds(INNER + STATE, STATE)]),
        (w_dt, weights.at[own_half, pl.ds(COL_DT, LANES)]),
        (w_z, weights.at[own_half, pl.ds(COL_Z, INNER)]),
        (w_out, out_weights.at[out_half, :]),
    )
    local = [
        pltpu.make_async_copy(source, target, local_sem.at[i])
        for i, (source, target) in enumerate(pieces)
    ]
    own_latent = pltpu.make_async_copy(latent, lat.at[x], local_sem.at[len(pieces)])
    own_latent.start()
    barrier = pltpu.get_barrier_semaphore()
    up_place = lax.rem(place + 1, count)
    down_place = lax.rem(place + count - 1, count)
    above = {"sp_0": up_place // ny, "sp_1": lax.rem(up_place, ny)}
    below = {"sp_0": down_place // ny, "sp_1": lax.rem(down_place, ny)}
    peers = [{"sp_0": lax.rem(z + k, nz)} for k in range(1, nz)]
    peers += [{"sp_1": lax.rem(y + k, ny)} for k in range(1, ny)]
    peers += [{"tp": lax.rem(x + k, nx)} for k in range(1, nx)]
    peers += [{"dp": 1 - core}, above, below]
    for peer in peers:
        pl.semaphore_signal(barrier, inc=1, device_id=peer, device_id_type=MESH)
    for c in local:
        c.start()

    rows = modw.shape[1]
    chunk = placed.shape[1]
    per = chunk // rows
    placed[...] = jnp.zeros_like(placed)
    at = pl.ds(pl.multiple_of(lax.rem(place, per) * rows, rows), rows)
    placed[:, at, :] = modw[...]
    lane_at = pl.ds(pl.multiple_of((place // per) * chunk, chunk), chunk)
    act = jnp.broadcast_to(rounded(silu(small[0:1, lane_at])), (8, chunk))
    act_ctx = jnp.broadcast_to(rounded(silu(small[1:2, lane_at])), (8, chunk))
    row8 = rows_of((8, chunk))
    partial = jnp.zeros((8, width), F32)
    for k in range(3):
        left = jnp.where(row8 == k, act, 0.0)
        if k < 2:
            left = jnp.where(row8 == 3 + k, act_ctx, left)
        partial = partial + jnp.dot(
            left.astype(BF16), placed[k], preferred_element_type=F32
        )
    mod_z[z] = partial

    ctx[...] = context[...].astype(F32)
    edge_send[0] = ctx[0:1, :]
    edge_send[1] = ctx[CTX_ROWS - 1 : CTX_ROWS, :]

    pl.semaphore_wait(barrier, len(peers))
    mods = [
        Exchange(
            axis,
            size,
            me,
            lambda peer, buf=buf, me=me: buf.at[me],
            lambda buf=buf, me=me: buf.at[me],
            lambda k, i=i: mod_sems.at[0, i, k],
            lambda k, i=i: mod_sems.at[1, i, k],
        )
        for i, (axis, size, me, buf) in enumerate(
            (("sp_0", nz, z, mod_z), ("sp_1", ny, y, mod_y), ("tp", nx, x, mod_x))
        )
    ]
    mods[0].start()
    lat_copies = Exchange(
        "tp",
        nx,
        x,
        lambda peer: latent,
        lambda: lat.at[x],
        lambda k: lat_sems.at[0, k],
        lambda k: lat_sems.at[1, k],
    ).start()

    def edge(slot, to):
        return pltpu.make_async_remote_copy(
            src_ref=edge_send.at[slot],
            dst_ref=edge_recv.at[slot],
            send_sem=edge_sems.at[0, slot],
            recv_sem=edge_sems.at[1, slot],
            device_id=to,
            device_id_type=MESH,
        )

    edges = [edge(0, below), edge(1, above), edge(2, below), edge(3, above)]
    edges[0].start()
    edges[1].start()
    swaps = [
        pltpu.make_async_remote_copy(
            src_ref=source,
            dst_ref=target,
            send_sem=core_send.at[i],
            recv_sem=core_recv.at[i],
            device_id={"dp": 1 - core},
            device_id_type=MESH,
        )
        for i, (source, target) in enumerate(pieces)
    ]
    for c in swaps:
        c.start()

    mods[0].arrived()
    total = mod_z[0]
    for k in range(1, nz):
        total = total + mod_z[k]
    mod_y[y] = total
    mods[1].start()

    own_latent.wait()
    lat_copies.arrived()
    edge_send[2] = lat[0].astype(F32)[0:1, :]
    edge_send[3] = lat[nx - 1].astype(F32)[own_rows - 1 : own_rows, :]
    edges[2].start()
    edges[3].start()

    def inverse(v):
        return lax.rsqrt(jnp.mean(v * v, axis=1, keepdims=True) + EPSILON)

    scales = [inverse(lat[t].astype(F32)) for t in range(nx)]

    mods[1].arrived()
    total = mod_y[0]
    for k in range(1, ny):
        total = total + mod_y[k]
    mod_x[x] = total
    mods[2].start()

    misc[...] = jnp.zeros_like(misc)
    misc[8:16, :] = ctx[...]
    for e in edges:
        e.wait_recv()
    misc[0:1, :] = jnp.where(place > 0, edge_recv[3], 0.0)
    misc[1:2, :] = jnp.where(place < count - 1, edge_recv[2], 0.0)
    misc[2:3, :] = jnp.where(place > 0, edge_recv[1], 0.0)
    misc[3:4, :] = jnp.where(place < count - 1, edge_recv[0], 0.0)
    misc_scale = inverse(misc[...])
    row16 = rows_of((16, 1))
    is_lat = row16 < 2
    kept = jnp.logical_or(
        row16 >= 8,
        jnp.logical_or(
            jnp.logical_and(row16 % 2 == 0, place > 0),
            jnp.logical_and(row16 % 2 == 1, place < count - 1),
        ),
    )

    mods[2].arrived()
    for c in range(nx):
        cols = slice(c * width, (c + 1) * width)
        mod = mod_x[c]
        gain = small[2:3, cols]
        scale = gain * (1.0 + mod[1:2])
        shift = mod[0:1]
        scale_ctx = gain * (1.0 + mod[4:5])
        shift_ctx = mod[3:4]
        for t in range(nx):
            value = lat[t, :, cols].astype(F32) * scales[t] * scale + shift
            hidden[t * own_rows : (t + 1) * own_rows, cols] = value.astype(BF16)
        value = misc[:, cols] * misc_scale * jnp.where(is_lat, scale, scale_ctx)
        value = value + jnp.where(is_lat, shift, shift_ctx)
        hidden[TOKENS:ROWS, cols] = jnp.where(kept, value, 0.0).astype(BF16)

    for i in range(len(pieces)):
        local[i].wait()
        swaps[i].wait_recv()

    left = 0
    while left < COLS:
        wide = min(256, COLS - left)
        cols = slice(left, left + wide)
        feats[:, cols] = rounded(
            jnp.dot(hidden[...], weights[:, cols], preferred_element_type=F32)
        )
        left += wide

    for b in range((INNER + STATE) // LANES):
        cols = slice(b * LANES, (b + 1) * LANES)
        ctx_gather[y, :, cols] = convolved(
            feats[TOKENS + 8 : TOKENS + 16, cols],
            feats[TOKENS + 2 : TOKENS + 3, cols],
            feats[TOKENS + 3 : TOKENS + 4, cols],
            small[4:7, cols],
        )
    ctx_gather[y, :, INNER + STATE : CTX_COLS] = feats[TOKENS + 8 : TOKENS + 16, COL_DT:COLS]

    def along(axis, size, me, sems, index, source, target):
        return Exchange(
            axis,
            size,
            me,
            source,
            target,
            lambda k: sems.at[0, index, k],
            lambda k: sems.at[1, index, k],
        )

    ctx_copies = along(
        "sp_1", ny, y, y_sems, 0, lambda peer: ctx_gather.at[y], lambda: ctx_gather.at[y]
    ).start()

    rates = small[3:4, INNER : INNER + LANES]
    for b in range(MIXED // LANES):
        cols = slice(b * LANES, (b + 1) * LANES)
        feats[0:TOKENS, cols] = convolved(
            feats[0:TOKENS, cols],
            feats[TOKENS : TOKENS + 1, cols],
            feats[TOKENS + 1 : TOKENS + 2, cols],
            small[4:7, cols],
        )
    b_turned = feats[0:TOKENS, INNER : INNER + STATE].T.astype(BF16)
    c_vals = feats[0:TOKENS, INNER + STATE : MIXED].astype(BF16)
    steps = softplus(feats[0:TOKENS, COL_DT:COLS])
    sums = running_sums(-rates * steps, HEADS)
    for q in range(PAIRS):
        cols = slice(q * LANES, (q + 1) * LANES)
        x_vals = feats[0:TOKENS, cols]
        for way in range(2):
            head = way * HEADS + 2 * q
            step = spread(steps, head)
            decay = spread(sums, head)
            end = decay[TOKENS - 1 : TOKENS] if way == 0 else decay[0:1]
            moved_x = rounded(x_vals * step)
            moved[way * TOKENS : (way + 1) * TOKENS, cols] = moved_x.astype(BF16)
            growth[way, :, cols] = jnp.exp(decay)
            at_end = (moved_x * jnp.exp(end - decay)).astype(BF16)
            state = jnp.dot(b_turned, at_end, preferred_element_type=F32).astype(BF16)
            for p in range(ny):
                state_send[p, way * slab : (way + 1) * slab, cols] = state[
                    p * slab : (p + 1) * slab
                ]
            decay_y[y, way * PAIRS + q : way * PAIRS + q + 1, :] = end
    decay_copies = along(
        "sp_1", ny, y, y_sems, 1, lambda peer: decay_y.at[y], lambda: decay_y.at[y]
    ).start()
    state_copies = along(
        "sp_1", ny, y, y_sems, 2, lambda peer: state_send.at[peer], lambda: state_recv.at[y]
    ).start()
    state_recv[y] = state_send[y]

    ctx_copies.arrived()
    lines = ny * CTX_ROWS
    ctx_b = ctx_gather[:, :, INNER : INNER + STATE].reshape(lines, STATE).T
    ctx_steps = softplus(ctx_gather[:, :, INNER + STATE : CTX_COLS].reshape(lines, LANES))
    ctx_sums = running_sums(-rates * ctx_steps, HEADS)
    for q in range(PAIRS):
        cols = slice(q * LANES, (q + 1) * LANES)
        x_vals = ctx_gather[:, :, cols].reshape(lines, LANES)
        for way in range(2):
            head = way * HEADS + 2 * q
            decay = spread(ctx_sums, head)
            end = decay[lines - 1 : lines] if way == 0 else decay[0:1]
            scaled = rounded(x_vals * spread(ctx_steps, head)) * jnp.exp(end - decay)
            ctx_full[way, :, cols] = jnp.dot(
                ctx_b, scaled, preferred_element_type=F32, precision=lax.Precision.HIGHEST
            )
            ctx_dz[z, way * PAIRS + q : way * PAIRS + q + 1, :] = end
    own_slab = pl.ds(pl.multiple_of(y * slab, slab), slab)
    for way in range(2):
        ctx_z[z, way * slab : (way + 1) * slab, :] = ctx_full[way, own_slab, :].astype(BF16)
    ctx_dz_copies = along(
        "sp_0", nz, z, z_sems, 0, lambda peer: ctx_dz.at[z], lambda: ctx_dz.at[z]
    ).start()
    ctx_z_copies = along(
        "sp_0", nz, z, z_sems, 1, lambda peer: ctx_z.at[z], lambda: ctx_z.at[z]
    ).start()

    def attend():
        scores = jnp.dot(c_vals, b_turned, preferred_element_type=F32)
        turned = sums.T
        square = (TOKENS, TOKENS)
        lower = rows_of(square) >= lanes_of(square)
        upper = rows_of(square) <= lanes_of(square)
        for q in range(PAIRS):
            cols = slice(q * LANES, (q + 1) * LANES)
            halves = []
            for h in (2 * q, 2 * q + 1):
                both = []
                for way, mask in ((0, lower), (1, upper)):
                    lane = way * HEADS + h
                    gap = sums[:, lane : lane + 1] - turned[lane : lane + 1, :]
                    decayed = scores * jnp.exp(jnp.minimum(gap, 0.0))
                    both.append(jnp.where(mask, decayed, 0.0).astype(BF16))
                halves.append(
                    jnp.dot(
                        jnp.concatenate(both, axis=1),
                        moved[:, cols],
                        preferred_element_type=F32,
                    )
                )
            inside[:, cols] = jnp.where(lanes_of(square) < LANES // 2, halves[0], halves[1])

    attend()

    decay_copies.arrived()
    state_copies.arrived()
    decays = [decay_y[j] for j in range(ny)]
    is_fwd = rows_of((8, LANES)) < PAIRS
    ahead = [None] * ny
    acc_f = acc_b = jnp.zeros((8, LANES), F32)
    for j in range(ny):
        ahead[j] = acc_f
        acc_f = acc_f + decays[j]
    for j in reversed(range(ny)):
        ahead[j] = jnp.exp(jnp.where(is_fwd, ahead[j], acc_b))
        acc_b = acc_b + decays[j]
    tot_dz[z] = acc_f
    tot_dz_copies = along(
        "sp_0", nz, z, z_sems, 2, lambda peer: tot_dz.at[z], lambda: tot_dz.at[z]
    ).start()
    factors = [jnp.exp(d) for d in decays]
    for way in range(2):
        part = slice(way * slab, (way + 1) * slab)
        for q in range(PAIRS):
            cols = slice(q * LANES, (q + 1) * LANES)
            r = way * PAIRS + q
            state = jnp.zeros((slab, LANES), F32)
            for j in range(ny) if way == 0 else reversed(range(ny)):
                before[j, part, cols] = state
                state = state * factors[j][r : r + 1] + state_recv[j, part, cols].astype(F32)
            tot_z[z, part, cols] = state.astype(BF16)
    tot_z_copies = along(
        "sp_0", nz, z, z_sems, 3, lambda peer: tot_z.at[z], lambda: tot_z.at[z]
    ).start()

    ctx_dz_copies.arrived()
    ctx_z_copies.arrived()
    ctx_factors = [jnp.exp(ctx_dz[j]) for j in range(nz)]
    starts = {}
    for way in range(2):
        part = slice(way * slab, (way + 1) * slab)
        for q in range(PAIRS):
            cols = slice(q * LANES, (q + 1) * LANES)
            r = way * PAIRS + q
            state = jnp.zeros((slab, LANES), F32)
            for j in range(nz) if way == 0 else reversed(range(nz)):
                state = state * ctx_factors[j][r : r + 1] + ctx_z[j, part, cols].astype(F32)
            starts[way, q] = state

    tot_dz_copies.arrived()
    tot_z_copies.arrived()
    tot_factors = [jnp.exp(tot_dz[j]) for j in range(nz)]
    for way in range(2):
        part = slice(way * slab, (way + 1) * slab)
        for q in range(PAIRS):
            cols = slice(q * LANES, (q + 1) * LANES)
            r = way * PAIRS + q
            state = starts[way, q]
            for j in range(nz) if way == 0 else reversed(range(nz)):
                passed = j < z if way == 0 else j > z
                later = state * tot_factors[j][r : r + 1] + tot_z[j, part, cols].astype(F32)
                state = jnp.where(passed, later, state)
            for j in range(ny):
                enter_send[j, part, cols] = (
                    before[j, part, cols] + ahead[j][r : r + 1] * state
                ).astype(BF16)
    enter_copies = along(
        "sp_1", ny, y, y_sems, 3, lambda peer: enter_send.at[peer], lambda: enter_recv.at[y]
    ).start()
    enter_recv[y] = enter_send[y]

    enter_copies.arrived()
    carried = [
        jnp.dot(
            c_vals,
            enter_recv[:, way * slab : (way + 1) * slab, :].reshape(STATE, INNER),
            preferred_element_type=F32,
        )
        for way in range(2)
    ]
    squares = jnp.zeros((TOKENS, 1), F32)
    for q in range(PAIRS):
        cols = slice(q * LANES, (q + 1) * LANES)
        value = inside[:, cols]
        for way in range(2):
            value = value + growth[way, :, cols] * carried[way][:, cols]
        value = value * silu(feats[0:TOKENS, COL_Z + q * LANES : COL_Z + (q + 1) * LANES])
        inside[:, cols] = value
        squares = squares + jnp.sum(value * value, axis=1, keepdims=True)
    scale = lax.rsqrt(squares / INNER + EPSILON)
    for q in range(PAIRS):
        cols = slice(q * LANES, (q + 1) * LANES)
        normed[:, cols] = (inside[:, cols] * scale * small[3:4, cols]).astype(BF16)

    part_copies = []
    for c in range(nx):
        cols = slice(c * width, (c + 1) * width)
        term = jnp.dot(normed[...], out_weights[:, cols], preferred_element_type=F32)
        term = term.astype(BF16)
        for t in range(nx):
            part_send[t, :, cols] = term[t * own_rows : (t + 1) * own_rows]
        part_copies.append(
            along(
                "tp",
                nx,
                x,
                part_sems,
                c,
                lambda peer, cols=cols: part_send.at[peer, :, cols],
                lambda cols=cols: part_recv.at[x, :, cols],
            ).start()
        )
        part_recv[x, :, cols] = part_send[x, :, cols]
    for c in range(nx):
        cols = slice(c * width, (c + 1) * width)
        part_copies[c].arrived()
        value = part_recv[0, :, cols].astype(F32)
        for t in range(1, nx):
            value = value + part_recv[t, :, cols].astype(F32)
        out[:, cols] = (mod_x[c, 2:3, :] * value).astype(BF16)

    for e in edges + swaps:
        e.wait_send()
    everything = mods + part_copies + [lat_copies, ctx_copies, decay_copies, state_copies]
    everything += [ctx_dz_copies, ctx_z_copies, tot_dz_copies, tot_z_copies, enter_copies]
    for e in everything:
        e.left()


def shards(
    sizes,
    latent,
    condition,
    context,
    context_source,
    mod_weight,
    norm_gain,
    w_x,
    w_b,
    w_c,
    w_z,
    w_dt,
    conv_x,
    conv_b,
    conv_c,
    decay_rate,
    out_gain,
    w_out,
):
    nz, ny, nx = sizes
    model = latent.shape[-1]
    own_rows = latent.shape[1]
    width = model // nx
    slab = STATE // ny
    span = max(model, 1024)

    def row(*pieces):
        flat = jnp.concatenate([p.astype(F32) for p in pieces])
        return jnp.pad(flat, (0, span - flat.shape[0]))

    small = jnp.stack(
        [
            row(condition[0]),
            row(context_source),
            row(norm_gain),
            row(out_gain, decay_rate[0], decay_rate[1]),
            *[row(conv_x[k], conv_b[k], conv_c[k]) for k in range(3)],
            jnp.zeros((span,), F32),
        ]
    )
    step_weights = jnp.pad(
        jnp.concatenate([w_dt[0], w_dt[1]], axis=1), ((0, 0), (0, LANES - 2 * HEADS))
    )
    rows = mod_weight.shape[1]
    vmem = pl.BlockSpec(memory_space=pltpu.VMEM)
    hbm = pl.BlockSpec(memory_space=pl.ANY)
    dma = pltpu.SemaphoreType.DMA
    most = max(nz, ny, nx) - 1
    scratch = [
        pltpu.VMEM((model, COLS), BF16),
        pltpu.VMEM((INNER, model), BF16),
        pltpu.VMEM((nx, own_rows, model), BF16),
        pltpu.VMEM((CTX_ROWS, model), F32),
        pltpu.VMEM((3, max(rows, LANES), width), BF16),
        pltpu.VMEM((nz, 8, width), F32),
        pltpu.VMEM((ny, 8, width), F32),
        pltpu.VMEM((nx, 8, width), F32),
        pltpu.VMEM((4, 1, model), F32),
        pltpu.VMEM((4, 1, model), F32),
        pltpu.VMEM((16, model), F32),
        pltpu.VMEM((ROWS, model), BF16),
        pltpu.VMEM((ROWS, COLS), F32),
        pltpu.VMEM((2 * TOKENS, INNER), BF16),
        pltpu.VMEM((2, TOKENS, INNER), F32),
        pltpu.VMEM((TOKENS, INNER), F32),
        pltpu.VMEM((ny, CTX_ROWS, CTX_COLS), F32),
        pltpu.VMEM((2, STATE, INNER), F32),
        pltpu.VMEM((nz, 2 * slab, INNER), BF16),
        pltpu.VMEM((nz, 8, LANES), F32),
        pltpu.VMEM((ny, 2 * slab, INNER), BF16),
        pltpu.VMEM((ny, 2 * slab, INNER), BF16),
        pltpu.VMEM((ny, 8, LANES), F32),
        pltpu.VMEM((nz, 2 * slab, INNER), BF16),
        pltpu.VMEM((nz, 8, LANES), F32),
        pltpu.VMEM((ny, 2 * slab, INNER), F32),
        pltpu.VMEM((ny, 2 * slab, INNER), BF16),
        pltpu.VMEM((ny, 2 * slab, INNER), BF16),
        pltpu.VMEM((TOKENS, INNER), BF16),
        pltpu.VMEM((nx, own_rows, model), BF16),
        pltpu.VMEM((nx, own_rows, model), BF16),
        dma((7,)),
        dma((6,)),
        dma((6,)),
        dma((2, 3, most)),
        dma((2, nx - 1)),
        dma((2, 4)),
        dma((2, 4, ny - 1)),
        dma((2, 4, nz - 1)),
        dma((2, nx, nx - 1)),
    ]
    update = pl.pallas_call(
        functools.partial(mixer, (nz, ny, nx, model)),
        out_shape=jax.ShapeDtypeStruct((own_rows, model), BF16),
        in_specs=[vmem, vmem, hbm, vmem] + [hbm] * 6,
        out_specs=vmem,
        scratch_shapes=scratch,
        compiler_params=pltpu.CompilerParams(
            collective_id=0, has_side_effects=True, vmem_limit_bytes=56 * 1024 * 1024
        ),
    )(small, mod_weight, latent[0], context[0], w_x, w_b, w_c, w_z, step_weights, w_out)
    return update[None]


def solution(mesh):
    nx = mesh.shape["tp"]
    ny = 8
    nz = mesh.shape["sp"] // ny
    return program(mesh, nz, ny, nx)


def program(mesh, nz, ny, nx):
    torus = Mesh(
        mesh.devices.reshape(nz, ny, nx, mesh.shape["dp"]), ("sp_0", "sp_1", "tp", "dp")
    )
    placed = (
        P("dp", SP_TP, None),
        P("dp", None),
        P("dp", SP, None),
        P(),
        P(None, SP, "tp"),
        P(),
        P("dp", "tp"),
        P("dp", "tp"),
        P("dp", "tp"),
        P("dp", "tp"),
        P(None, "dp", "tp"),
        P(None, "tp"),
        P(None, "tp"),
        P(None, "tp"),
        P(None, "tp"),
        P("tp"),
        P(("tp", "dp"), None),
    )
    return jax.shard_map(
        functools.partial(shards, (nz, ny, nx)),
        mesh=torus,
        in_specs=placed,
        out_specs=P("dp", SP_TP, None),
        check_vma=False,
    )
```

```python
import functools

import jax
import jax.numpy as jnp
from jax import lax
from jax.experimental import pallas as pl
from jax.experimental.pallas import tpu as pltpu
from jax.sharding import Mesh
from jax.sharding import PartitionSpec as P

SP = ("sp_0", "sp_1")
SP_TP = ("sp_0", "sp_1", "tp")
MESH = pl.DeviceIdType.MESH
EPSILON = 1e-06
F32 = jnp.float32
BF16 = jnp.bfloat16
TOKENS = 128
STATE = 128
LANES = 128
HEADS = 8
PAIRS = HEADS // 2
INNER = 512
MIXED = INNER + 2 * STATE
COL_Z = MIXED
COL_DT = COL_Z + INNER
COLS = COL_DT + LANES
CTX_ROWS = 8


def rounded(v):
    return v.astype(BF16).astype(F32)


def silu(v):
    return v / (1.0 + jnp.exp(-v))


def softplus(v):
    return jnp.maximum(v, 0.0) + jnp.log1p(jnp.exp(-jnp.abs(v)))


def rows_of(shape):
    return lax.broadcasted_iota(jnp.int32, shape, 0)


def lanes_of(shape):
    return lax.broadcasted_iota(jnp.int32, shape, 1)


def running_sums(v, heads):
    n = v.shape[0]
    row = rows_of(v.shape)
    down = up = v
    step = 1
    while step < n:
        down = down + jnp.where(row >= step, pltpu.roll(down, step, 0), 0.0)
        up = up + jnp.where(row < n - step, pltpu.roll(up, n - step, 0), 0.0)
        step *= 2
    return jnp.where(lanes_of(v.shape) < heads, down, up)


def spread(v, head):
    shape = (v.shape[0], LANES)
    left = jnp.broadcast_to(v[:, head : head + 1], shape)
    right = jnp.broadcast_to(v[:, head + 1 : head + 2], shape)
    return jnp.where(lanes_of(shape) < LANES // 2, left, right)


def convolved(mid, low, high, taps):
    n = mid.shape[0]
    row = rows_of(mid.shape)
    before = jnp.where(row == 0, low, pltpu.roll(mid, 1, 0))
    after = jnp.where(row == n - 1, high, pltpu.roll(mid, n - 1, 0))
    summed = before * taps[0:1] + mid * taps[1:2] + after * taps[2:3]
    return rounded(silu(summed))


class Exchange:
    def __init__(self, axis, size, place, source, target, sent, got, sends=None, gets=None):
        self.sends, self.gets = sends, gets
        self.copies = []
        for k in range(1, size):
            peer = lax.rem(place + k, size)
            self.copies.append(
                pltpu.make_async_remote_copy(
                    src_ref=source(peer),
                    dst_ref=target(),
                    send_sem=sent(k - 1),
                    recv_sem=got(k - 1),
                    device_id={axis: peer},
                    device_id_type=MESH,
                )
            )

    def each(self, taken, act):
        for k, c in enumerate(self.copies, 1):
            if taken is None:
                act(c)
            else:
                pl.when(taken(k))(functools.partial(act, c))

    def start(self):
        self.each(self.sends, lambda c: c.start())
        return self

    def arrived(self):
        self.each(self.gets, lambda c: c.wait_recv())

    def left(self):
        self.each(self.sends, lambda c: c.wait_send())


def mixer(
    dims,
    condition,
    source,
    gain_in,
    out_gain,
    conv_x,
    conv_b,
    conv_c,
    rate,
    modw,
    context,
    latent,
    w_x,
    w_b,
    w_c,
    w_z,
    w_dt,
    w_out,
    parts,
    gate,
    weights,
    out_weights,
    dt_rows,
    dt_wide,
    small,
    lat,
    ctx,
    placed,
    mod_z,
    mod_y,
    mod_x,
    edge_send,
    edge_recv,
    misc,
    hidden,
    feats,
    moved,
    growth,
    inside,
    ctx_full,
    ctx_z,
    ctx_dz,
    state_send,
    state_recv,
    decay_y,
    tot_z,
    tot_dz,
    before,
    enter_send,
    enter_recv,
    normed,
    part_send,
    local_sem,
    core_send,
    core_recv,
    mod_sems,
    lat_sems,
    edge_sems,
    edge_got,
    y_sems,
    z_sems,
    part_sems,
):
    nz, ny, nx, model = dims
    width = model // nx
    own_rows = TOKENS // nx
    slab = STATE // ny
    lines = ny * CTX_ROWS
    ctx_at = TOKENS + 16
    z = lax.axis_index("sp_0")
    y = lax.axis_index("sp_1")
    x = lax.axis_index("tp")
    core = lax.axis_index("dp")
    place = z * ny + y
    count = nz * ny

    own_latent = pltpu.make_async_copy(latent, lat.at[x], local_sem.at[6])
    own_latent.start()
    half = model // 2
    own_half = pl.ds(pl.multiple_of(core * half, half), half)
    out_half = pl.ds(pl.multiple_of(core * (INNER // 2), INNER // 2), INNER // 2)
    pieces = (
        (w_dt, dt_rows.at[:, :, own_half]),
        (w_x, weights.at[own_half, pl.ds(0, INNER)]),
        (w_b, weights.at[own_half, pl.ds(INNER, STATE)]),
        (w_c, weights.at[own_half, pl.ds(INNER + STATE, STATE)]),
        (w_z, weights.at[own_half, pl.ds(COL_Z, INNER)]),
        (w_out, out_weights.at[out_half, :]),
    )
    local = [
        pltpu.make_async_copy(origin, target, local_sem.at[i])
        for i, (origin, target) in enumerate(pieces)
    ]
    barrier = pltpu.get_barrier_semaphore()
    up_place = lax.rem(place + 1, count)
    down_place = lax.rem(place + count - 1, count)
    above = {"sp_0": up_place // ny, "sp_1": lax.rem(up_place, ny)}
    below = {"sp_0": down_place // ny, "sp_1": lax.rem(down_place, ny)}
    peers = [{"sp_0": lax.rem(z + k, nz)} for k in range(1, nz)]
    peers += [{"sp_1": lax.rem(y + k, ny)} for k in range(1, ny)]
    peers += [{"tp": lax.rem(x + k, nx)} for k in range(1, nx)]
    peers += [{"dp": 1 - core}]
    for k in range(nx):
        peers += [dict(above, tp=k), dict(below, tp=k)]
    for peer in peers:
        pl.semaphore_signal(barrier, inc=1, device_id=peer, device_id_type=MESH)

    small[...] = jnp.zeros_like(small)
    for r, ref in ((1, source), (2, gain_in), (3, out_gain)):
        piece = ref[...].astype(F32)
        for k in range(piece.shape[0]):
            small[r : r + 1, k * LANES : (k + 1) * LANES] = piece[k : k + 1]
    small[0:1, 0:model] = condition[...].astype(F32)
    small[4:7, 0:INNER] = conv_x[...].astype(F32)
    small[4:7, INNER : INNER + STATE] = conv_b[...].astype(F32)
    small[4:7, INNER + STATE : MIXED] = conv_c[...].astype(F32)

    rows = modw.shape[1]
    chunk = placed.shape[1]
    per = chunk // rows
    placed[...] = jnp.zeros_like(placed)
    at = pl.ds(pl.multiple_of(lax.rem(place, per) * rows, rows), rows)
    placed[:, at, :] = modw[...]
    lane_at = pl.ds(pl.multiple_of((place // per) * chunk, chunk), chunk)
    act = jnp.broadcast_to(rounded(silu(small[0:1, lane_at])), (8, chunk))
    act_ctx = jnp.broadcast_to(rounded(silu(small[1:2, lane_at])), (8, chunk))
    row8 = rows_of((8, chunk))
    partial = jnp.zeros((8, width), F32)
    for k in range(3):
        left = jnp.where(row8 == k, act, 0.0)
        if k < 2:
            left = jnp.where(row8 == 3 + k, act_ctx, left)
        partial = partial + jnp.dot(
            left.astype(BF16), placed[k], preferred_element_type=F32
        )
    for r in range(5):
        mod_z[z, r] = partial[r : r + 1]

    pl.semaphore_wait(barrier, len(peers))
    mods = [
        Exchange(
            axis,
            size,
            me,
            lambda peer, buf=buf, me=me: buf.at[me],
            lambda buf=buf, me=me: buf.at[me],
            lambda k, i=i: mod_sems.at[0, i, k],
            lambda k, i=i: mod_sems.at[1, i, k],
        )
        for i, (axis, size, me, buf) in enumerate(
            (("sp_0", nz, z, mod_z), ("sp_1", ny, y, mod_y), ("tp", nx, x, mod_x))
        )
    ]

    def along(axis, size, me, sems, index, origin, target, sends=None, gets=None):
        return Exchange(
            axis,
            size,
            me,
            origin,
            target,
            lambda k: sems.at[0, index, k],
            lambda k: sems.at[1, index, k],
            sends,
            gets,
        )

    mods[0].start()
    ctx_copies = along(
        "sp_1", ny, y, y_sems, 0, lambda peer: context, lambda: ctx.at[y]
    ).start()
    lat_copies = along(
        "tp", nx, x, lat_sems, 0, lambda peer: latent, lambda: lat.at[x]
    ).start()
    swaps = [
        pltpu.make_async_remote_copy(
            src_ref=origin,
            dst_ref=target,
            send_sem=core_send.at[i],
            recv_sem=core_recv.at[i],
            device_id={"dp": 1 - core},
            device_id_type=MESH,
        )
        for i, (origin, target) in enumerate(pieces)
    ]
    for c, d in zip(swaps, local):
        c.start()
        d.start()
    ctx[y] = context[...]

    def edge(slot, k, to):
        return pltpu.make_async_remote_copy(
            src_ref=edge_send.at[slot],
            dst_ref=edge_recv.at[slot],
            send_sem=edge_sems.at[slot, k],
            recv_sem=edge_got.at[slot],
            device_id=to,
            device_id_type=MESH,
        )

    to_above = [edge(0, k, dict(above, tp=k)) for k in range(nx)]
    to_below = [edge(1, k, dict(below, tp=k)) for k in range(nx)]
    own_latent.wait()

    @pl.when(x == nx - 1)
    def _():
        edge_send[0] = lat[x].astype(F32)[own_rows - 1 : own_rows, :]
        for c in to_above:
            c.start()

    @pl.when(x == 0)
    def _():
        edge_send[1] = lat[x].astype(F32)[0:1, :]
        for c in to_below:
            c.start()

    mods[0].arrived()
    total = mod_z[0]
    for k in range(1, nz):
        total = total + mod_z[k]
    mod_y[y] = total
    mods[1].start()

    ctx_copies.arrived()
    edge_send[2] = ctx[ny - 1].astype(F32)[CTX_ROWS - 1 : CTX_ROWS, :]
    edge_send[3] = ctx[0].astype(F32)[0:1, :]
    ctx_edges = [
        edge(2, 0, {"sp_0": lax.rem(z + 1, nz)}),
        edge(3, 0, {"sp_0": lax.rem(z + nz - 1, nz)}),
    ]
    for c in ctx_edges:
        c.start()

    def inverse(v):
        return lax.rsqrt(jnp.mean(v * v, axis=1, keepdims=True) + EPSILON)

    ctx_scales = [inverse(ctx[j].astype(F32)) for j in range(ny)]

    mods[1].arrived()
    total = mod_y[0]
    for k in range(1, ny):
        total = total + mod_y[k]
    mod_x[x] = total
    mods[2].start()

    lat_copies.arrived()
    scales = [inverse(lat[t].astype(F32)) for t in range(nx)]
    misc[...] = jnp.zeros_like(misc)
    for c in (to_above[0], to_below[0], *ctx_edges):
        c.wait_recv()
    has = (place > 0, place < count - 1, z > 0, z < nz - 1)
    for slot in range(4):
        misc[slot : slot + 1, :] = jnp.where(has[slot], edge_recv[slot], 0.0)
    misc_scale = inverse(misc[...])
    row16 = rows_of((16, 1))
    kept = jnp.zeros((16, 1), jnp.bool_)
    for slot in range(4):
        kept = jnp.logical_or(kept, jnp.logical_and(row16 == slot, has[slot]))
    local[0].wait()
    swaps[0].wait_recv()
    dt_wide[...] = jnp.zeros_like(dt_wide)
    for way in range(2):
        dt_wide[way * HEADS : (way + 1) * HEADS, :] = dt_rows[way].astype(F32)
    for b in range(model // LANES):
        at = slice(b * LANES, (b + 1) * LANES)
        weights[at, COL_DT:COLS] = dt_wide[:, at].T.astype(BF16)
    for i in range(1, len(pieces) - 1):
        local[i].wait()
        swaps[i].wait_recv()

    mods[2].arrived()
    for c in range(nx):
        cols = slice(c * width, (c + 1) * width)
        mod = [mod_x[c, r] for r in range(5)]
        gain = small[2:3, cols]
        scale = gain * (1.0 + mod[1])
        shift = mod[0]
        scale_ctx = gain * (1.0 + mod[4])
        shift_ctx = mod[3]
        gate[:, cols] = mod[2]
        for t in range(nx):
            value = lat[t, :, cols].astype(F32) * scales[t] * scale + shift
            hidden[t * own_rows : (t + 1) * own_rows, cols] = value.astype(BF16)
        value = misc[:, cols] * misc_scale * jnp.where(row16 < 2, scale, scale_ctx)
        value = value + jnp.where(row16 < 2, shift, shift_ctx)
        hidden[TOKENS:ctx_at, cols] = jnp.where(kept, value, 0.0).astype(BF16)
        for j in range(0, ny, 2):
            pair = [
                ctx[i, :, cols].astype(F32) * ctx_scales[i] * scale_ctx + shift_ctx
                for i in (j, j + 1)
            ]
            at = ctx_at + j * CTX_ROWS
            hidden[at : at + 2 * CTX_ROWS, cols] = jnp.concatenate(pair, axis=0).astype(BF16)

    def project(left, right):
        while left < right:
            wide = min(256, right - left)
            cols = slice(left, left + wide)
            feats[:, cols] = rounded(
                jnp.dot(hidden[...], weights[:, cols], preferred_element_type=F32)
            )
            left += wide

    project(0, COL_Z)
    project(COL_DT, COLS)

    lane = lanes_of((1, LANES))
    rates = jnp.zeros((1, LANES), F32)
    for way in range(2):
        for h in range(HEADS):
            rates = jnp.where(lane == way * HEADS + h, rate[way : way + 1, h : h + 1], rates)
    ctx_rows = slice(ctx_at, ctx_at + lines)
    for b in range((INNER + STATE) // LANES):
        cols = slice(b * LANES, (b + 1) * LANES)
        feats[ctx_rows, cols] = convolved(
            feats[ctx_rows, cols],
            feats[TOKENS + 2 : TOKENS + 3, cols],
            feats[TOKENS + 3 : TOKENS + 4, cols],
            small[4:7, cols],
        )
    ctx_b = feats[ctx_rows, INNER : INNER + STATE].T
    ctx_steps = softplus(feats[ctx_rows, COL_DT:COLS])
    ctx_sums = running_sums(-rates * ctx_steps, HEADS)
    own_slab = pl.ds(pl.multiple_of(y * slab, slab), slab)
    for way in range(2):
        for q in range(PAIRS):
            cols = slice(q * LANES, (q + 1) * LANES)
            head = way * HEADS + 2 * q
            decay = spread(ctx_sums, head)
            end = decay[lines - 1 : lines] if way == 0 else decay[0:1]
            moved_x = rounded(feats[ctx_rows, cols] * spread(ctx_steps, head))
            ctx_full[way, :, cols] = jnp.dot(
                ctx_b,
                moved_x * jnp.exp(end - decay),
                preferred_element_type=F32,
                precision=lax.Precision.HIGHEST,
            )
            ctx_dz[z, way * PAIRS + q : way * PAIRS + q + 1, :] = end
        ctx_z[z, way * slab : (way + 1) * slab, :] = ctx_full[way, own_slab, :].astype(BF16)
    ctx_dz_copies = along(
        "sp_0", nz, z, z_sems, 0, lambda peer: ctx_dz.at[z], lambda: ctx_dz.at[z]
    ).start()
    ctx_z_copies = along(
        "sp_0", nz, z, z_sems, 1, lambda peer: ctx_z.at[z], lambda: ctx_z.at[z]
    ).start()

    for b in range(MIXED // LANES):
        cols = slice(b * LANES, (b + 1) * LANES)
        feats[0:TOKENS, cols] = convolved(
            feats[0:TOKENS, cols],
            feats[TOKENS : TOKENS + 1, cols],
            feats[TOKENS + 1 : TOKENS + 2, cols],
            small[4:7, cols],
        )
    b_turned = feats[0:TOKENS, INNER : INNER + STATE].T.astype(BF16)
    c_vals = feats[0:TOKENS, INNER + STATE : MIXED].astype(BF16)
    steps = softplus(feats[0:TOKENS, COL_DT:COLS])
    sums = running_sums(-rates * steps, HEADS)
    ends = jnp.where(lane < HEADS, sums[TOKENS - 1 : TOKENS], sums[0:1])
    for way in range(2):
        for q in range(PAIRS):
            r = way * PAIRS + q
            decay_y[y, r : r + 1, :] = spread(ends, 2 * r)
    decay_copies = along(
        "sp_1", ny, y, y_sems, 1, lambda peer: decay_y.at[y], lambda: decay_y.at[y]
    ).start()
    state_copies = []
    for way in range(2):
        for q in range(PAIRS):
            cols = slice(q * LANES, (q + 1) * LANES)
            head = way * HEADS + 2 * q
            step = spread(steps, head)
            decay = spread(sums, head)
            end = decay[TOKENS - 1 : TOKENS] if way == 0 else decay[0:1]
            moved_x = rounded(feats[0:TOKENS, cols] * step)
            moved[way * TOKENS : (way + 1) * TOKENS, cols] = moved_x.astype(BF16)
            growth[way, :, cols] = jnp.exp(decay)
            at_end = (moved_x * jnp.exp(end - decay)).astype(BF16)
            state = jnp.dot(b_turned, at_end, preferred_element_type=F32).astype(BF16)
            for p in range(ny):
                state_send[way, p, :, cols] = state[p * slab : (p + 1) * slab]
        state_copies.append(
            along(
                "sp_1",
                ny,
                y,
                y_sems,
                2 + way,
                lambda peer, way=way: state_send.at[way, peer],
                lambda way=way: state_recv.at[way, y],
            ).start()
        )
        state_recv[way, y] = state_send[way, y]

    project(COL_Z, COL_DT)
    scores = jnp.dot(c_vals, b_turned, preferred_element_type=F32)
    turned = sums.T
    square = (TOKENS, TOKENS)
    lower = rows_of(square) >= lanes_of(square)
    upper = rows_of(square) <= lanes_of(square)
    for q in range(PAIRS):
        cols = slice(q * LANES, (q + 1) * LANES)
        halves = []
        for h in (2 * q, 2 * q + 1):
            both = []
            for way, mask in ((0, lower), (1, upper)):
                col = way * HEADS + h
                gap = sums[:, col : col + 1] - turned[col : col + 1, :]
                decayed = scores * jnp.exp(jnp.minimum(gap, 0.0))
                both.append(jnp.where(mask, decayed, 0.0).astype(BF16))
            halves.append(
                jnp.dot(
                    jnp.concatenate(both, axis=1),
                    moved[:, cols],
                    preferred_element_type=F32,
                )
            )
        inside[:, cols] = jnp.where(lanes_of(square) < LANES // 2, halves[0], halves[1])

    decay_copies.arrived()
    decays = [decay_y[j] for j in range(ny)]
    is_fwd = rows_of((8, LANES)) < PAIRS
    ahead = [None] * ny
    acc_f = acc_b = jnp.zeros((8, LANES), F32)
    for j in range(ny):
        ahead[j] = acc_f
        acc_f = acc_f + decays[j]
    for j in reversed(range(ny)):
        ahead[j] = jnp.exp(jnp.where(is_fwd, ahead[j], acc_b))
        acc_b = acc_b + decays[j]
    tot_dz[z] = acc_f
    tot_dz_copies = along(
        "sp_0", nz, z, z_sems, 2, lambda peer: tot_dz.at[z], lambda: tot_dz.at[z]
    ).start()
    factors = [jnp.exp(d) for d in decays]
    tot_copies = []
    for way in range(2):
        state_copies[way].arrived()
        for q in range(PAIRS):
            cols = slice(q * LANES, (q + 1) * LANES)
            r = way * PAIRS + q
            state = jnp.zeros((slab, LANES), F32)
            for j in range(ny) if way == 0 else reversed(range(ny)):
                before[way, j, :, cols] = state
                state = state * factors[j][r : r + 1] + state_recv[way, j, :, cols].astype(F32)
            tot_z[way, z, :, cols] = state.astype(BF16)
        tot_copies.append(
            along(
                "sp_0",
                nz,
                z,
                z_sems,
                3 + way,
                lambda peer, way=way: tot_z.at[way, z],
                lambda way=way: tot_z.at[way, z],
                (lambda k: z + k < nz) if way == 0 else (lambda k: z + k >= nz),
                (lambda k: z >= k) if way == 0 else (lambda k: z < k),
            ).start()
        )

    ctx_dz_copies.arrived()
    ctx_z_copies.arrived()
    ctx_factors = [jnp.exp(ctx_dz[j]) for j in range(nz)]
    tot_dz_copies.arrived()
    tot_factors = [jnp.exp(tot_dz[j]) for j in range(nz)]
    enter_copies = []
    for way in range(2):
        part = slice(way * slab, (way + 1) * slab)
        starts = []
        for q in range(PAIRS):
            cols = slice(q * LANES, (q + 1) * LANES)
            r = way * PAIRS + q
            state = jnp.zeros((slab, LANES), F32)
            for j in range(nz) if way == 0 else reversed(range(nz)):
                state = state * ctx_factors[j][r : r + 1] + ctx_z[j, part, cols].astype(F32)
            starts.append(state)
        tot_copies[way].arrived()
        for q in range(PAIRS):
            cols = slice(q * LANES, (q + 1) * LANES)
            r = way * PAIRS + q
            state = starts[q]
            for j in range(nz) if way == 0 else reversed(range(nz)):
                passed = j < z if way == 0 else j > z
                later = state * tot_factors[j][r : r + 1] + tot_z[way, j, :, cols].astype(F32)
                state = jnp.where(passed, later, state)
            for j in range(ny):
                enter_send[way, j, :, cols] = (
                    before[way, j, :, cols] + ahead[j][r : r + 1] * state
                ).astype(BF16)
        enter_copies.append(
            along(
                "sp_1",
                ny,
                y,
                y_sems,
                4 + way,
                lambda peer, way=way: enter_send.at[way, peer],
                lambda way=way: enter_recv.at[way, y],
            ).start()
        )
        enter_recv[way, y] = enter_send[way, y]

    squares = jnp.zeros((TOKENS, 1), F32)
    for way in range(2):
        enter_copies[way].arrived()
        carried = jnp.dot(
            c_vals, enter_recv[way].reshape(STATE, INNER), preferred_element_type=F32
        )
        for q in range(PAIRS):
            cols = slice(q * LANES, (q + 1) * LANES)
            value = inside[:, cols] + growth[way, :, cols] * carried[:, cols]
            if way == 1:
                at = COL_Z + q * LANES
                value = value * silu(feats[0:TOKENS, at : at + LANES])
                squares = squares + jnp.sum(value * value, axis=1, keepdims=True)
            inside[:, cols] = value
    scale = lax.rsqrt(squares / INNER + EPSILON)
    for q in range(PAIRS):
        cols = slice(q * LANES, (q + 1) * LANES)
        normed[:, cols] = (inside[:, cols] * scale * small[3:4, cols]).astype(BF16)

    local[-1].wait()
    swaps[-1].wait_recv()
    part_copies = []
    for c in range(nx):
        cols = slice(c * width, (c + 1) * width)
        term = jnp.dot(normed[...], out_weights[:, cols], preferred_element_type=F32)
        term = term.astype(BF16)
        for t in range(nx):
            part_send[t, :, cols] = term[t * own_rows : (t + 1) * own_rows]
        part_copies.append(
            along(
                "tp",
                nx,
                x,
                part_sems,
                c,
                lambda peer, cols=cols: part_send.at[peer, :, cols],
                lambda cols=cols: parts.at[x, :, cols],
            ).start()
        )
    own_part = pltpu.make_async_copy(part_send.at[x], parts.at[x], local_sem.at[7])
    own_part.start()
    for e in swaps + ctx_edges:
        e.wait_send()

    @pl.when(x == nx - 1)
    def _():
        for c in to_above:
            c.wait_send()

    @pl.when(x == 0)
    def _():
        for c in to_below:
            c.wait_send()

    done = mods + [ctx_copies, lat_copies, decay_copies, ctx_dz_copies, ctx_z_copies]
    done += [tot_dz_copies] + state_copies + tot_copies + enter_copies
    for e in done + part_copies:
        e.left()
    own_part.wait()
    for e in part_copies:
        e.arrived()


def shards(
    sizes,
    latent,
    condition,
    context,
    context_source,
    mod_weight,
    norm_gain,
    w_x,
    w_b,
    w_c,
    w_z,
    w_dt,
    conv_x,
    conv_b,
    conv_c,
    decay_rate,
    out_gain,
    w_out,
):
    nz, ny, nx = sizes
    model = latent.shape[-1]
    own_rows = latent.shape[1]
    width = model // nx
    slab = STATE // ny
    span = max(model, 1024)
    rows = mod_weight.shape[1]
    lines = ny * CTX_ROWS
    total_rows = TOKENS + 16 + lines
    vmem = pl.BlockSpec(memory_space=pltpu.VMEM)
    hbm = pl.BlockSpec(memory_space=pl.ANY)
    dma = pltpu.SemaphoreType.DMA
    most = max(nz, ny, nx) - 1
    scratch = [
        pltpu.VMEM((model, COLS), BF16),
        pltpu.VMEM((INNER, model), BF16),
        pltpu.VMEM((2, HEADS, model), BF16),
        pltpu.VMEM((LANES, model), F32),
        pltpu.VMEM((8, span), F32),
        pltpu.VMEM((nx, own_rows, model), BF16),
        pltpu.VMEM((ny, CTX_ROWS, model), BF16),
        pltpu.VMEM((3, max(rows, LANES), width), BF16),
        pltpu.VMEM((nz, 5, 1, width), F32),
        pltpu.VMEM((ny, 5, 1, width), F32),
        pltpu.VMEM((nx, 5, 1, width), F32),
        pltpu.VMEM((4, 1, model), F32),
        pltpu.VMEM((4, 1, model), F32),
        pltpu.VMEM((16, model), F32),
        pltpu.VMEM((total_rows, model), BF16),
        pltpu.VMEM((total_rows, COLS), F32),
        pltpu.VMEM((2 * TOKENS, INNER), BF16),
        pltpu.VMEM((2, TOKENS, INNER), F32),
        pltpu.VMEM((TOKENS, INNER), F32),
        pltpu.VMEM((2, STATE, INNER), F32),
        pltpu.VMEM((nz, 2 * slab, INNER), BF16),
        pltpu.VMEM((nz, 8, LANES), F32),
        pltpu.VMEM((2, ny, slab, INNER), BF16),
        pltpu.VMEM((2, ny, slab, INNER), BF16),
        pltpu.VMEM((ny, 8, LANES), F32),
        pltpu.VMEM((2, nz, slab, INNER), BF16),
        pltpu.VMEM((nz, 8, LANES), F32),
        pltpu.VMEM((2, ny, slab, INNER), F32),
        pltpu.VMEM((2, ny, slab, INNER), BF16),
        pltpu.VMEM((2, ny, slab, INNER), BF16),
        pltpu.VMEM((TOKENS, INNER), BF16),
        pltpu.VMEM((nx, own_rows, model), BF16),
        dma((8,)),
        dma((6,)),
        dma((6,)),
        dma((2, 3, most)),
        dma((2, 1, nx - 1)),
        dma((4, nx)),
        dma((4,)),
        dma((2, 6, ny - 1)),
        dma((2, 5, nz - 1)),
        dma((2, nx, nx - 1)),
    ]
    parts, gate = pl.pallas_call(
        functools.partial(mixer, (nz, ny, nx, model)),
        out_shape=(
            jax.ShapeDtypeStruct((nx, own_rows, model), BF16),
            jax.ShapeDtypeStruct((1, model), F32),
        ),
        in_specs=[vmem] * 10 + [hbm] * 7,
        out_specs=(hbm, vmem),
        scratch_shapes=scratch,
        compiler_params=pltpu.CompilerParams(
            collective_id=0, has_side_effects=True, vmem_limit_bytes=56 * 1024 * 1024
        ),
    )(
        condition,
        context_source.reshape(-1, LANES),
        norm_gain.reshape(-1, LANES),
        out_gain.reshape(-1, LANES),
        conv_x,
        conv_b,
        conv_c,
        decay_rate,
        mod_weight,
        context[0],
        latent[0],
        w_x,
        w_b,
        w_c,
        w_z,
        jnp.swapaxes(w_dt, 1, 2),
        w_out,
    )
    mixed = jnp.sum(parts.astype(F32), axis=0)
    return (gate * mixed).astype(BF16)[None]


def solution(mesh):
    nx = mesh.shape["tp"]
    ny = 8
    nz = mesh.shape["sp"] // ny
    return program(mesh, nz, ny, nx)


def program(mesh, nz, ny, nx):
    torus = Mesh(
        mesh.devices.reshape(nz, ny, nx, mesh.shape["dp"]), ("sp_0", "sp_1", "tp", "dp")
    )
    placed = (
        P("dp", SP_TP, None),
        P("dp", None),
        P("dp", SP, None),
        P(),
        P(None, SP, "tp"),
        P(),
        P("dp", "tp"),
        P("dp", "tp"),
        P("dp", "tp"),
        P("dp", "tp"),
        P(None, "dp", "tp"),
        P(None, "tp"),
        P(None, "tp"),
        P(None, "tp"),
        P(None, "tp"),
        P("tp"),
        P(("tp", "dp"), None),
    )
    return jax.shard_map(
        functools.partial(shards, (nz, ny, nx)),
        mesh=torus,
        in_specs=placed,
        out_specs=P("dp", SP_TP, None),
        check_vma=False,
    )
```

```python
import functools

import jax
import jax.numpy as jnp
from jax import lax
from jax.experimental import pallas as pl
from jax.experimental.pallas import tpu as pltpu
from jax.sharding import Mesh
from jax.sharding import PartitionSpec as P

SP = ("sp_0", "sp_1")
SP_TP = ("sp_0", "sp_1", "tp")
MESH = pl.DeviceIdType.MESH
EPSILON = 1e-06
F32 = jnp.float32
BF16 = jnp.bfloat16
TOKENS = 128
STATE = 128
LANES = 128
HEADS = 8
PAIRS = HEADS // 2
INNER = 512
MIXED = INNER + 2 * STATE
COL_B = INNER
COL_DT = COL_B + STATE
COL_C = COL_DT + LANES
COL_Z = COL_C + STATE
COLS = COL_Z + INNER
CTX_ROWS = 8


def rounded(v):
    return v.astype(BF16).astype(F32)


def silu(v):
    return v / (1.0 + jnp.exp(-v))


def softplus(v):
    return jnp.maximum(v, 0.0) + jnp.log1p(jnp.exp(-jnp.abs(v)))


def rows_of(shape):
    return lax.broadcasted_iota(jnp.int32, shape, 0)


def lanes_of(shape):
    return lax.broadcasted_iota(jnp.int32, shape, 1)


def running_sums(v, heads):
    n = v.shape[0]
    row = rows_of(v.shape)
    down = up = v
    step = 1
    while step < n:
        down = down + jnp.where(row >= step, pltpu.roll(down, step, 0), 0.0)
        up = up + jnp.where(row < n - step, pltpu.roll(up, n - step, 0), 0.0)
        step *= 2
    return jnp.where(lanes_of(v.shape) < heads, down, up)


def spread(v, head):
    shape = (v.shape[0], LANES)
    left = jnp.broadcast_to(v[:, head : head + 1], shape)
    right = jnp.broadcast_to(v[:, head + 1 : head + 2], shape)
    return jnp.where(lanes_of(shape) < LANES // 2, left, right)


def convolved(mid, low, high, taps):
    n = mid.shape[0]
    row = rows_of(mid.shape)
    before = jnp.where(row == 0, low, pltpu.roll(mid, 1, 0))
    after = jnp.where(row == n - 1, high, pltpu.roll(mid, n - 1, 0))
    summed = before * taps[0:1] + mid * taps[1:2] + after * taps[2:3]
    return rounded(silu(summed))


class Exchange:
    def __init__(self, axis, size, place, source, target, sems, bulk):
        def copy(peer, origin, end):
            return pltpu.make_async_remote_copy(
                src_ref=origin,
                dst_ref=end,
                send_sem=sems.at[0],
                recv_sem=sems.at[1],
                device_id={axis: peer},
                device_id_type=MESH,
            )

        peers = [lax.rem(place + k, size) for k in range(1, size)]
        self.copies = [copy(peer, source(peer), target) for peer in peers]
        self.whole = copy(peers[0], bulk, bulk)

    def start(self):
        for c in self.copies:
            c.start()
        return self

    def arrived(self):
        self.whole.wait_recv()

    def left(self):
        self.whole.wait_send()


class Totals:
    def __init__(self, way, buf, size, place, sems):
        self.sends, self.gets, self.copies = [], [], []
        for k in range(1, size):
            later = place + k < size
            passed = place >= k
            self.sends.append(later if way == 0 else jnp.logical_not(later))
            self.gets.append(passed if way == 0 else jnp.logical_not(passed))
            self.copies.append(
                pltpu.make_async_remote_copy(
                    src_ref=buf.at[way, place],
                    dst_ref=buf.at[way, place],
                    send_sem=sems.at[0, k - 1],
                    recv_sem=sems.at[1, k - 1],
                    device_id={"sp_0": lax.rem(place + k, size)},
                    device_id_type=MESH,
                )
            )

    def start(self):
        for taken, c in zip(self.sends, self.copies):
            pl.when(taken)(c.start)
        return self

    def arrived(self):
        for taken, c in zip(self.gets, self.copies):
            pl.when(taken)(c.wait_recv)

    def left(self):
        for taken, c in zip(self.sends, self.copies):
            pl.when(taken)(c.wait_send)


def mixer(
    dims,
    condition,
    source,
    gain_in,
    out_gain,
    conv_x,
    conv_b,
    conv_c,
    rate,
    modw,
    context,
    latent,
    w_x,
    w_b,
    w_c,
    w_z,
    w_dt,
    w_out,
    parts,
    gate,
    weights,
    out_weights,
    dt_rows,
    dt_wide,
    small,
    lat,
    ctx,
    placed,
    mod_z,
    mod_y,
    mod_x,
    edge_send,
    edge_recv,
    misc,
    hidden,
    feats,
    moved,
    growth,
    inside,
    ctx_full,
    ctx_z,
    ctx_dz,
    state_send,
    state_recv,
    decay_y,
    tot_z,
    tot_dz,
    before,
    enter_send,
    enter_recv,
    normed,
    part_send,
    local_sem,
    core_send,
    core_recv,
    pair_sems,
    edge_sems,
    edge_got,
    tot_sems,
):
    nz, ny, nx, model = dims
    width = model // nx
    own_rows = TOKENS // nx
    slab = STATE // ny
    lines = ny * CTX_ROWS
    ctx_at = TOKENS + 16
    z = lax.axis_index("sp_0")
    y = lax.axis_index("sp_1")
    x = lax.axis_index("tp")
    core = lax.axis_index("dp")
    place = z * ny + y
    count = nz * ny

    own_latent = pltpu.make_async_copy(latent, lat.at[x], local_sem.at[3])
    own_latent.start()
    half = model // 2
    own_half = pl.ds(pl.multiple_of(core * half, half), half)
    out_half = pl.ds(pl.multiple_of(core * (INNER // 2), INNER // 2), INNER // 2)
    pieces = (
        (w_dt, dt_rows.at[:, :, own_half]),
        (w_x, weights.at[own_half, pl.ds(0, INNER)]),
        (w_b, weights.at[own_half, pl.ds(COL_B, STATE)]),
        (w_c, weights.at[own_half, pl.ds(COL_C, STATE)]),
        (w_z, weights.at[own_half, pl.ds(COL_Z, INNER)]),
        (w_out, out_weights.at[out_half, :]),
    )
    groups = (0, 1, 1, 1, 1, 2)
    local = [
        pltpu.make_async_copy(origin, target, local_sem.at[i])
        for i, (origin, target) in zip(groups, pieces)
    ]
    in_bulk = weights.at[own_half, pl.ds(0, COLS - LANES)]
    bulk_local = [
        local[0],
        pltpu.make_async_copy(in_bulk, in_bulk, local_sem.at[1]),
        local[-1],
    ]
    barrier = pltpu.get_barrier_semaphore()
    up_place = lax.rem(place + 1, count)
    down_place = lax.rem(place + count - 1, count)
    above = {"sp_0": up_place // ny, "sp_1": lax.rem(up_place, ny)}
    below = {"sp_0": down_place // ny, "sp_1": lax.rem(down_place, ny)}
    peers = [{"sp_0": lax.rem(z + k, nz)} for k in range(1, nz)]
    peers += [{"sp_1": lax.rem(y + k, ny)} for k in range(1, ny)]
    peers += [{"tp": lax.rem(x + k, nx)} for k in range(1, nx)]
    peers += [{"dp": 1 - core}]
    for k in range(nx):
        peers += [dict(above, tp=k), dict(below, tp=k)]
    for peer in peers:
        pl.semaphore_signal(barrier, inc=1, device_id=peer, device_id_type=MESH)

    def unpack(r, ref):
        piece = ref[...].astype(F32)
        for k in range(piece.shape[0]):
            small[r : r + 1, k * LANES : (k + 1) * LANES] = piece[k : k + 1]

    unpack(1, source)
    small[0:1, 0:model] = condition[...].astype(F32)

    rows = modw.shape[1]
    chunk = placed.shape[1]
    per = chunk // rows
    placed[...] = jnp.zeros_like(placed)
    at = pl.ds(pl.multiple_of(lax.rem(place, per) * rows, rows), rows)
    placed[:, at, :] = modw[...]
    lane_at = pl.ds(pl.multiple_of((place // per) * chunk, chunk), chunk)
    act = jnp.broadcast_to(rounded(silu(small[0:1, lane_at])), (8, chunk))
    act_ctx = jnp.broadcast_to(rounded(silu(small[1:2, lane_at])), (8, chunk))
    row8 = rows_of((8, chunk))
    partial = jnp.zeros((8, width), F32)
    for k in range(3):
        left = jnp.where(row8 == k, act, 0.0)
        if k < 2:
            left = jnp.where(row8 == 3 + k, act_ctx, left)
        partial = partial + jnp.dot(
            left.astype(BF16), placed[k], preferred_element_type=F32
        )
    for r in range(5):
        mod_y[y, r] = partial[r : r + 1]

    pl.semaphore_wait(barrier, len(peers))
    pairs = iter(range(32))

    def along(axis, size, me, origin, target, bulk):
        return Exchange(axis, size, me, origin, target, pair_sems.at[next(pairs)], bulk)

    def gather(axis, size, me, buf):
        own = buf.at[me]
        return along(axis, size, me, lambda peer: own, own, buf.at[pl.ds(0, size - 1)])

    mods = [
        gather("sp_1", ny, y, mod_y),
        gather("sp_0", nz, z, mod_z),
        gather("tp", nx, x, mod_x),
    ]
    mods[0].start()
    ctx_copies = along(
        "sp_1", ny, y, lambda peer: context, ctx.at[y], ctx.at[pl.ds(0, ny - 1)]
    ).start()
    lat_copies = along(
        "tp", nx, x, lambda peer: latent, lat.at[x], lat.at[pl.ds(0, nx - 1)]
    ).start()
    swaps = [
        pltpu.make_async_remote_copy(
            src_ref=origin,
            dst_ref=target,
            send_sem=core_send.at[i],
            recv_sem=core_recv.at[i],
            device_id={"dp": 1 - core},
            device_id_type=MESH,
        )
        for i, (origin, target) in zip(groups, pieces)
    ]
    bulk_swaps = [
        swaps[0],
        pltpu.make_async_remote_copy(
            src_ref=in_bulk,
            dst_ref=in_bulk,
            send_sem=core_send.at[1],
            recv_sem=core_recv.at[1],
            device_id={"dp": 1 - core},
            device_id_type=MESH,
        ),
        swaps[-1],
    ]
    for c, d in zip(swaps, local):
        c.start()
        d.start()
    ctx[y] = context[...]

    def edge(slot, k, to):
        return pltpu.make_async_remote_copy(
            src_ref=edge_send.at[slot],
            dst_ref=edge_recv.at[slot],
            send_sem=edge_sems.at[slot, k],
            recv_sem=edge_got.at[slot],
            device_id=to,
            device_id_type=MESH,
        )

    to_above = [edge(0, k, dict(above, tp=k)) for k in range(nx)]
    to_below = [edge(1, k, dict(below, tp=k)) for k in range(nx)]
    own_latent.wait()

    @pl.when(x == nx - 1)
    def _():
        edge_send[0] = lat[x].astype(F32)[own_rows - 1 : own_rows, :]
        for c in to_above:
            c.start()

    @pl.when(x == 0)
    def _():
        edge_send[1] = lat[x].astype(F32)[0:1, :]
        for c in to_below:
            c.start()

    small[2:7, :] = jnp.zeros((5, small.shape[1]), F32)
    unpack(2, gain_in)
    unpack(3, out_gain)
    small[4:7, 0:INNER] = conv_x[...].astype(F32)
    small[4:7, INNER : INNER + STATE] = conv_b[...].astype(F32)
    small[4:7, INNER + STATE : MIXED] = conv_c[...].astype(F32)
    lane = lanes_of((1, LANES))
    rates = jnp.zeros((1, LANES), F32)
    for way in range(2):
        for h in range(HEADS):
            rates = jnp.where(lane == way * HEADS + h, rate[way : way + 1, h : h + 1], rates)

    mods[0].arrived()
    total = mod_y[0]
    for k in range(1, ny):
        total = total + mod_y[k]
    mod_z[z] = total
    mods[1].start()

    def inverse(v):
        return lax.rsqrt(jnp.mean(v * v, axis=1, keepdims=True) + EPSILON)

    mods[1].arrived()
    total = mod_z[0]
    for k in range(1, nz):
        total = total + mod_z[k]
    mod_x[x] = total
    mods[2].start()

    ctx_copies.arrived()
    edge_send[2] = ctx[ny - 1].astype(F32)[CTX_ROWS - 1 : CTX_ROWS, :]
    edge_send[3] = ctx[0].astype(F32)[0:1, :]
    ctx_edges = [
        edge(2, 0, {"sp_0": lax.rem(z + 1, nz)}),
        edge(3, 0, {"sp_0": lax.rem(z + nz - 1, nz)}),
    ]
    for c in ctx_edges:
        c.start()

    lat_copies.arrived()
    scales = [inverse(lat[t].astype(F32)) for t in range(nx)]
    misc[...] = jnp.zeros_like(misc)
    for c in (to_above[0], to_below[0]):
        c.wait_recv()
    has = (place > 0, place < count - 1, z > 0, z < nz - 1)
    for slot in range(2):
        misc[slot : slot + 1, :] = jnp.where(has[slot], edge_recv[slot], 0.0)
    misc_scale = inverse(misc[0:8, :])
    row8 = rows_of((8, 1))

    def kept(low, high):
        return jnp.logical_or(
            jnp.logical_and(row8 == 0, low), jnp.logical_and(row8 == 1, high)
        )

    bulk_local[0].wait()
    bulk_swaps[0].wait_recv()
    dt_wide[...] = jnp.zeros_like(dt_wide)
    for way in range(2):
        dt_wide[way * HEADS : (way + 1) * HEADS, :] = dt_rows[way].astype(F32)
    for b in range(model // LANES):
        at = slice(b * LANES, (b + 1) * LANES)
        weights[at, COL_DT:COL_C] = dt_wide[:, at].T.astype(BF16)
    bulk_local[1].wait()
    bulk_swaps[1].wait_recv()

    mods[2].arrived()

    def modulations(c, shift, scale):
        cols = slice(c * width, (c + 1) * width)
        return cols, small[2:3, cols] * (1.0 + mod_x[c, scale]), mod_x[c, shift]

    def edge_rows(cols, scale, shift, known, at):
        value = misc[at : at + 8, cols] * misc_scale * scale + shift
        value = jnp.where(known, value, 0.0)
        return jnp.concatenate([value, jnp.zeros_like(value)], axis=0).astype(BF16)

    for c in range(nx):
        cols, scale, shift = modulations(c, 0, 1)
        for t in range(nx):
            value = lat[t, :, cols].astype(F32) * scales[t] * scale + shift
            hidden[t * own_rows : (t + 1) * own_rows, cols] = value.astype(BF16)
        hidden[TOKENS:ctx_at, cols] = edge_rows(cols, scale, shift, kept(has[0], has[1]), 0)

    def project(rows, left, right):
        while left < right:
            wide = min(256, right - left)
            cols = slice(left, left + wide)
            feats[rows, cols] = rounded(
                jnp.dot(hidden[rows, :], weights[:, cols], preferred_element_type=F32)
            )
            left += wide

    def smooth(rows, low, at, tap_at):
        cols = slice(at, at + LANES)
        feats[rows, cols] = convolved(
            feats[rows, cols],
            feats[low : low + 1, cols],
            feats[low + 1 : low + 2, cols],
            small[4:7, tap_at : tap_at + LANES],
        )

    own = slice(0, TOKENS)
    project(slice(0, ctx_at), 0, COL_C)
    for at in range(0, COL_DT, LANES):
        smooth(own, TOKENS, at, at)
    b_turned = feats[own, COL_B:COL_DT].T.astype(BF16)
    steps = softplus(feats[own, COL_DT:COL_C])
    sums = running_sums(-rates * steps, HEADS)
    ends = jnp.where(lane < HEADS, sums[TOKENS - 1 : TOKENS], sums[0:1])
    for way in range(2):
        for q in range(PAIRS):
            r = way * PAIRS + q
            decay_y[y, r : r + 1, :] = spread(ends, 2 * r)
    decay_copies = gather("sp_1", ny, y, decay_y).start()

    def slabs(axis, size, me, origin, target, way):
        return along(
            axis,
            size,
            me,
            lambda peer: origin.at[way, peer],
            target.at[way, me],
            target.at[way, pl.ds(0, size - 1)],
        )

    state_copies = []
    for way in range(2):
        for q in range(PAIRS):
            cols = slice(q * LANES, (q + 1) * LANES)
            head = way * HEADS + 2 * q
            step = spread(steps, head)
            decay = spread(sums, head)
            end = decay[TOKENS - 1 : TOKENS] if way == 0 else decay[0:1]
            moved_x = rounded(feats[own, cols] * step)
            moved[way * TOKENS : (way + 1) * TOKENS, cols] = moved_x.astype(BF16)
            growth[way, :, cols] = jnp.exp(decay)
            at_end = (moved_x * jnp.exp(end - decay)).astype(BF16)
            state = jnp.dot(b_turned, at_end, preferred_element_type=F32).astype(BF16)
            for p in range(ny):
                state_send[way, p, :, cols] = state[p * slab : (p + 1) * slab]
        state_copies.append(slabs("sp_1", ny, y, state_send, state_recv, way).start())
        state_recv[way, y] = state_send[way, y]

    project(slice(0, ctx_at), COL_C, COL_Z)

    for c in ctx_edges:
        c.wait_recv()
    for slot in (2, 3):
        at = 6 + slot
        misc[at : at + 1, :] = jnp.where(has[slot], edge_recv[slot], 0.0)
    misc_scale = inverse(misc[8:16, :])
    ctx_scales = [inverse(ctx[j].astype(F32)) for j in range(ny)]
    for c in range(nx):
        cols, scale, shift = modulations(c, 3, 4)
        hidden[TOKENS:ctx_at, cols] = edge_rows(cols, scale, shift, kept(has[2], has[3]), 8)
        for j in range(0, ny, 2):
            two = [
                ctx[i, :, cols].astype(F32) * ctx_scales[i] * scale + shift
                for i in (j, j + 1)
            ]
            at = ctx_at + j * CTX_ROWS
            hidden[at : at + 2 * CTX_ROWS, cols] = jnp.concatenate(two, axis=0).astype(BF16)
    project(slice(TOKENS, ctx_at + lines), 0, COL_C)
    ctx_rows = slice(ctx_at, ctx_at + lines)
    for at in range(0, COL_DT, LANES):
        smooth(ctx_rows, TOKENS, at, at)
    ctx_b = feats[ctx_rows, COL_B:COL_DT].T
    ctx_steps = softplus(feats[ctx_rows, COL_DT:COL_C])
    ctx_sums = running_sums(-rates * ctx_steps, HEADS)
    own_slab = pl.ds(pl.multiple_of(y * slab, slab), slab)
    for way in range(2):
        for q in range(PAIRS):
            cols = slice(q * LANES, (q + 1) * LANES)
            head = way * HEADS + 2 * q
            decay = spread(ctx_sums, head)
            end = decay[lines - 1 : lines] if way == 0 else decay[0:1]
            moved_x = rounded(feats[ctx_rows, cols] * spread(ctx_steps, head))
            ctx_full[way, :, cols] = jnp.dot(
                ctx_b,
                moved_x * jnp.exp(end - decay),
                preferred_element_type=F32,
                precision=lax.Precision.HIGHEST,
            )
            ctx_dz[z, way * PAIRS + q : way * PAIRS + q + 1, :] = end
        ctx_z[z, way * slab : (way + 1) * slab, :] = ctx_full[way, own_slab, :].astype(BF16)
    ctx_dz_copies = gather("sp_0", nz, z, ctx_dz).start()
    ctx_z_copies = gather("sp_0", nz, z, ctx_z).start()

    smooth(own, TOKENS, COL_C, INNER + STATE)
    c_vals = feats[own, COL_C:COL_Z].astype(BF16)
    project(own, COL_Z, COLS)
    for at in range(COL_Z, COLS, LANES):
        feats[own, at : at + LANES] = silu(feats[own, at : at + LANES])
    for c in range(nx):
        gate[:, c * width : (c + 1) * width] = mod_x[c, 2]
    scores = jnp.dot(c_vals, b_turned, preferred_element_type=F32)
    turned = sums.T
    square = (TOKENS, TOKENS)
    lower = rows_of(square) >= lanes_of(square)
    upper = rows_of(square) <= lanes_of(square)
    for q in range(PAIRS):
        cols = slice(q * LANES, (q + 1) * LANES)
        halves = []
        for h in (2 * q, 2 * q + 1):
            both = []
            for way, mask in ((0, lower), (1, upper)):
                col = way * HEADS + h
                gap = sums[:, col : col + 1] - turned[col : col + 1, :]
                decayed = scores * jnp.exp(jnp.minimum(gap, 0.0))
                both.append(jnp.where(mask, decayed, 0.0).astype(BF16))
            halves.append(
                jnp.dot(
                    jnp.concatenate(both, axis=1),
                    moved[:, cols],
                    preferred_element_type=F32,
                )
            )
        inside[:, cols] = jnp.where(lanes_of(square) < LANES // 2, halves[0], halves[1])

    decay_copies.arrived()
    decays = [decay_y[j] for j in range(ny)]
    is_fwd = rows_of((8, LANES)) < PAIRS
    ahead = [None] * ny
    acc_f = acc_b = jnp.zeros((8, LANES), F32)
    for j in range(ny):
        ahead[j] = acc_f
        acc_f = acc_f + decays[j]
    for j in reversed(range(ny)):
        ahead[j] = jnp.exp(jnp.where(is_fwd, ahead[j], acc_b))
        acc_b = acc_b + decays[j]
    tot_dz[z] = acc_f
    tot_dz_copies = gather("sp_0", nz, z, tot_dz).start()
    factors = [jnp.exp(d) for d in decays]
    tot_copies = []
    for way in range(2):
        state_copies[way].arrived()
        for q in range(PAIRS):
            cols = slice(q * LANES, (q + 1) * LANES)
            r = way * PAIRS + q
            state = jnp.zeros((slab, LANES), F32)
            for j in range(ny) if way == 0 else reversed(range(ny)):
                before[way, j, :, cols] = state
                state = state * factors[j][r : r + 1] + state_recv[way, j, :, cols].astype(F32)
            tot_z[way, z, :, cols] = state.astype(BF16)
        tot_copies.append(Totals(way, tot_z, nz, z, tot_sems).start())

    ctx_dz_copies.arrived()
    ctx_z_copies.arrived()
    ctx_factors = [jnp.exp(ctx_dz[j]) for j in range(nz)]
    tot_dz_copies.arrived()
    tot_factors = [jnp.exp(tot_dz[j]) for j in range(nz)]
    enter_copies = []
    for way in range(2):
        part = slice(way * slab, (way + 1) * slab)
        starts = []
        for q in range(PAIRS):
            cols = slice(q * LANES, (q + 1) * LANES)
            r = way * PAIRS + q
            state = jnp.zeros((slab, LANES), F32)
            for j in range(nz) if way == 0 else reversed(range(nz)):
                state = state * ctx_factors[j][r : r + 1] + ctx_z[j, part, cols].astype(F32)
            starts.append(state)
        tot_copies[way].arrived()
        for q in range(PAIRS):
            cols = slice(q * LANES, (q + 1) * LANES)
            r = way * PAIRS + q
            state = starts[q]
            for j in range(nz) if way == 0 else reversed(range(nz)):
                passed = j < z if way == 0 else j > z
                later = state * tot_factors[j][r : r + 1] + tot_z[way, j, :, cols].astype(F32)
                state = jnp.where(passed, later, state)
            for j in range(ny):
                enter_send[way, j, :, cols] = (
                    before[way, j, :, cols] + ahead[j][r : r + 1] * state
                ).astype(BF16)
        enter_copies.append(slabs("sp_1", ny, y, enter_send, enter_recv, way).start())
        enter_recv[way, y] = enter_send[way, y]

    squares = jnp.zeros((TOKENS, 1), F32)
    for way in range(2):
        enter_copies[way].arrived()
        carried = jnp.dot(
            c_vals, enter_recv[way].reshape(STATE, INNER), preferred_element_type=F32
        )
        for q in range(PAIRS):
            cols = slice(q * LANES, (q + 1) * LANES)
            value = inside[:, cols] + growth[way, :, cols] * carried[:, cols]
            if way == 1:
                at = COL_Z + q * LANES
                value = value * feats[own, at : at + LANES]
                squares = squares + jnp.sum(value * value, axis=1, keepdims=True)
            inside[:, cols] = value
    scale = lax.rsqrt(squares / INNER + EPSILON)
    for q in range(PAIRS):
        cols = slice(q * LANES, (q + 1) * LANES)
        normed[:, cols] = (inside[:, cols] * scale * small[3:4, cols]).astype(BF16)

    bulk_local[-1].wait()
    bulk_swaps[-1].wait_recv()
    part_copies = []
    for c in range(nx):
        cols = slice(c * width, (c + 1) * width)
        term = jnp.dot(normed[...], out_weights[:, cols], preferred_element_type=F32)
        term = term.astype(BF16)
        for t in range(nx):
            part_send[t, :, cols] = term[t * own_rows : (t + 1) * own_rows]
        part_copies.append(
            along(
                "tp",
                nx,
                x,
                lambda peer, cols=cols: part_send.at[peer, :, cols],
                parts.at[x, :, cols],
                parts.at[pl.ds(0, nx - 1), :, cols],
            ).start()
        )
    own_part = pltpu.make_async_copy(part_send.at[x], parts.at[x], local_sem.at[4])
    own_part.start()
    for e in bulk_swaps + ctx_edges:
        e.wait_send()

    @pl.when(x == nx - 1)
    def _():
        for c in to_above:
            c.wait_send()

    @pl.when(x == 0)
    def _():
        for c in to_below:
            c.wait_send()

    done = mods + [ctx_copies, lat_copies, decay_copies, ctx_dz_copies, ctx_z_copies]
    done += [tot_dz_copies] + state_copies + tot_copies + enter_copies
    for e in done + part_copies:
        e.left()
    own_part.wait()
    for e in part_copies:
        e.arrived()


def shards(
    sizes,
    latent,
    condition,
    context,
    context_source,
    mod_weight,
    norm_gain,
    w_x,
    w_b,
    w_c,
    w_z,
    w_dt,
    conv_x,
    conv_b,
    conv_c,
    decay_rate,
    out_gain,
    w_out,
):
    nz, ny, nx = sizes
    model = latent.shape[-1]
    own_rows = latent.shape[1]
    width = model // nx
    slab = STATE // ny
    span = max(model, 1024)
    rows = mod_weight.shape[1]
    lines = ny * CTX_ROWS
    total_rows = TOKENS + 16 + lines
    vmem = pl.BlockSpec(memory_space=pltpu.VMEM)
    hbm = pl.BlockSpec(memory_space=pl.ANY)
    dma = pltpu.SemaphoreType.DMA
    scratch = [
        pltpu.VMEM((model, COLS), BF16),
        pltpu.VMEM((INNER, model), BF16),
        pltpu.VMEM((2, HEADS, model), BF16),
        pltpu.VMEM((LANES, model), F32),
        pltpu.VMEM((8, span), F32),
        pltpu.VMEM((nx, own_rows, model), BF16),
        pltpu.VMEM((ny, CTX_ROWS, model), BF16),
        pltpu.VMEM((3, max(rows, LANES), width), BF16),
        pltpu.VMEM((nz, 5, 1, width), F32),
        pltpu.VMEM((ny, 5, 1, width), F32),
        pltpu.VMEM((nx, 5, 1, width), F32),
        pltpu.VMEM((4, 1, model), F32),
        pltpu.VMEM((4, 1, model), F32),
        pltpu.VMEM((16, model), F32),
        pltpu.VMEM((total_rows, model), BF16),
        pltpu.VMEM((total_rows, COLS), F32),
        pltpu.VMEM((2 * TOKENS, INNER), BF16),
        pltpu.VMEM((2, TOKENS, INNER), F32),
        pltpu.VMEM((TOKENS, INNER), F32),
        pltpu.VMEM((2, STATE, INNER), F32),
        pltpu.VMEM((nz, 2 * slab, INNER), BF16),
        pltpu.VMEM((nz, 8, LANES), F32),
        pltpu.VMEM((2, ny, slab, INNER), BF16),
        pltpu.VMEM((2, ny, slab, INNER), BF16),
        pltpu.VMEM((ny, 8, LANES), F32),
        pltpu.VMEM((2, nz, slab, INNER), BF16),
        pltpu.VMEM((nz, 8, LANES), F32),
        pltpu.VMEM((2, ny, slab, INNER), F32),
        pltpu.VMEM((2, ny, slab, INNER), BF16),
        pltpu.VMEM((2, ny, slab, INNER), BF16),
        pltpu.VMEM((TOKENS, INNER), BF16),
        pltpu.VMEM((nx, own_rows, model), BF16),
        dma((5,)),
        dma((3,)),
        dma((3,)),
        dma((13 + nx, 2)),
        dma((4, nx)),
        dma((4,)),
        dma((2, nz - 1)),
    ]
    parts, gate = pl.pallas_call(
        functools.partial(mixer, (nz, ny, nx, model)),
        out_shape=(
            jax.ShapeDtypeStruct((nx, own_rows, model), BF16),
            jax.ShapeDtypeStruct((1, model), F32),
        ),
        in_specs=[vmem] * 10 + [hbm] * 7,
        out_specs=(hbm, vmem),
        scratch_shapes=scratch,
        compiler_params=pltpu.CompilerParams(
            collective_id=0, has_side_effects=True, vmem_limit_bytes=56 * 1024 * 1024
        ),
    )(
        condition,
        context_source.reshape(-1, LANES),
        norm_gain.reshape(-1, LANES),
        out_gain.reshape(-1, LANES),
        conv_x,
        conv_b,
        conv_c,
        decay_rate,
        mod_weight,
        context[0],
        latent[0],
        w_x,
        w_b,
        w_c,
        w_z,
        jnp.swapaxes(w_dt, 1, 2),
        w_out,
    )
    mixed = parts[0].astype(F32)
    for k in range(1, nx):
        mixed = mixed + parts[k].astype(F32)
    return (gate * mixed).astype(BF16)[None]


def solution(mesh):
    nx = mesh.shape["tp"]
    ny = 8
    nz = mesh.shape["sp"] // ny
    return program(mesh, nz, ny, nx)


def program(mesh, nz, ny, nx):
    torus = Mesh(
        mesh.devices.reshape(nz, ny, nx, mesh.shape["dp"]), ("sp_0", "sp_1", "tp", "dp")
    )
    placed = (
        P("dp", SP_TP, None),
        P("dp", None),
        P("dp", SP, None),
        P(),
        P(None, SP, "tp"),
        P(),
        P("dp", "tp"),
        P("dp", "tp"),
        P("dp", "tp"),
        P("dp", "tp"),
        P(None, "dp", "tp"),
        P(None, "tp"),
        P(None, "tp"),
        P(None, "tp"),
        P(None, "tp"),
        P("tp"),
        P(("tp", "dp"), None),
    )
    return jax.shard_map(
        functools.partial(shards, (nz, ny, nx)),
        mesh=torus,
        in_specs=placed,
        out_specs=P("dp", SP_TP, None),
        check_vma=False,
    )
```

```python
import functools

import jax
import jax.numpy as jnp
from jax import lax
from jax.experimental import pallas as pl
from jax.experimental.pallas import tpu as pltpu
from jax.sharding import Mesh
from jax.sharding import PartitionSpec as P

SP = ("sp_0", "sp_1")
SP_TP = ("sp_0", "sp_1", "tp")
MESH = pl.DeviceIdType.MESH
EPSILON = 1e-06
F32 = jnp.float32
BF16 = jnp.bfloat16
TOKENS = 128
STATE = 128
LANES = 128
HEADS = 8
PAIRS = HEADS // 2
INNER = 512
MIXED = INNER + 2 * STATE
COL_B = INNER
COL_DT = COL_B + STATE
COL_C = COL_DT + LANES
COL_Z = COL_C + STATE
COLS = COL_Z + INNER
PIECE = 2 * LANES
CTX_ROWS = 8


def rounded(v):
    return v.astype(BF16).astype(F32)


def silu(v):
    return v / (1.0 + jnp.exp(-v))


def softplus(v):
    return jnp.maximum(v, 0.0) + jnp.log1p(jnp.exp(-jnp.abs(v)))


def rows_of(shape):
    return lax.broadcasted_iota(jnp.int32, shape, 0)


def lanes_of(shape):
    return lax.broadcasted_iota(jnp.int32, shape, 1)


def running_sums(v, heads):
    n = v.shape[0]
    row = rows_of(v.shape)
    down = up = v
    step = 1
    while step < n:
        down = down + jnp.where(row >= step, pltpu.roll(down, step, 0), 0.0)
        up = up + jnp.where(row < n - step, pltpu.roll(up, n - step, 0), 0.0)
        step *= 2
    return jnp.where(lanes_of(v.shape) < heads, down, up)


def spread(v, head):
    shape = (v.shape[0], LANES)
    left = jnp.broadcast_to(v[:, head : head + 1], shape)
    right = jnp.broadcast_to(v[:, head + 1 : head + 2], shape)
    return jnp.where(lanes_of(shape) < LANES // 2, left, right)


def convolved(mid, low, high, taps):
    n = mid.shape[0]
    row = rows_of(mid.shape)
    before = jnp.where(row == 0, low, pltpu.roll(mid, 1, 0))
    after = jnp.where(row == n - 1, high, pltpu.roll(mid, n - 1, 0))
    summed = before * taps[0:1] + mid * taps[1:2] + after * taps[2:3]
    return rounded(silu(summed))


class Exchange:
    def __init__(self, axis, size, place, source, target, sems, bulk):
        def copy(peer, origin, end):
            return pltpu.make_async_remote_copy(
                src_ref=origin,
                dst_ref=end,
                send_sem=sems.at[0],
                recv_sem=sems.at[1],
                device_id={axis: peer},
                device_id_type=MESH,
            )

        peers = [lax.rem(place + k, size) for k in range(1, size)]
        self.copies = [copy(peer, source(peer), target) for peer in peers]
        self.whole = copy(peers[0], bulk, bulk)

    def start(self):
        for c in self.copies:
            c.start()
        return self

    def arrived(self):
        self.whole.wait_recv()

    def left(self):
        self.whole.wait_send()


class Totals:
    def __init__(self, way, buf, size, place, sems):
        self.sends, self.gets, self.copies = [], [], []
        for k in range(1, size):
            later = place + k < size
            passed = place >= k
            self.sends.append(later if way == 0 else jnp.logical_not(later))
            self.gets.append(passed if way == 0 else jnp.logical_not(passed))
            self.copies.append(
                pltpu.make_async_remote_copy(
                    src_ref=buf.at[place],
                    dst_ref=buf.at[place],
                    send_sem=sems.at[0, k - 1],
                    recv_sem=sems.at[1, k - 1],
                    device_id={"sp_0": lax.rem(place + k, size)},
                    device_id_type=MESH,
                )
            )

    def start(self):
        for taken, c in zip(self.sends, self.copies):
            pl.when(taken)(c.start)
        return self

    def arrived(self):
        for taken, c in zip(self.gets, self.copies):
            pl.when(taken)(c.wait_recv)

    def left(self):
        for taken, c in zip(self.sends, self.copies):
            pl.when(taken)(c.wait_send)


def mixer(
    dims,
    condition_in,
    source_in,
    gain_in,
    out_gain_in,
    conv_x_in,
    conv_b_in,
    conv_c_in,
    rate_in,
    modw_in,
    context,
    latent,
    w_x,
    w_b,
    w_c,
    w_z,
    w_dt,
    w_out,
    parts,
    gate,
    condition,
    source,
    gain,
    out_gain,
    conv_x,
    conv_b,
    conv_c,
    rate,
    modw,
    weights,
    out_weights,
    dt_rows,
    dt_wide,
    small,
    lat,
    ctx,
    placed,
    mod_z,
    mod_y,
    mod_x,
    edge_send,
    edge_recv,
    misc,
    hidden,
    feats,
    moved,
    growth,
    inside,
    ctx_bt,
    ctx_z,
    ctx_dz,
    state_send,
    state_recv,
    decay_y,
    tot_z,
    tot_dz,
    before,
    enter_send,
    enter_recv,
    normed,
    part_send,
    local_sem,
    core_send,
    core_recv,
    pair_sems,
    edge_sems,
    edge_got,
    tot_sems,
):
    nz, ny, nx, model = dims
    width = model // nx
    own_rows = TOKENS // nx
    slab = STATE // ny
    lines = ny * CTX_ROWS
    ctx_at = TOKENS + 16
    z = lax.axis_index("sp_0")
    y = lax.axis_index("sp_1")
    x = lax.axis_index("tp")
    core = lax.axis_index("dp")
    place = z * ny + y
    count = nz * ny

    barrier = pltpu.get_barrier_semaphore()
    up_place = lax.rem(place + 1, count)
    down_place = lax.rem(place + count - 1, count)
    above = {"sp_0": up_place // ny, "sp_1": lax.rem(up_place, ny)}
    below = {"sp_0": down_place // ny, "sp_1": lax.rem(down_place, ny)}
    peers = [{"sp_1": lax.rem(y + k, ny)} for k in range(1, ny)]
    peers += [{"sp_0": lax.rem(z + k, nz)} for k in range(1, nz)]
    peers += [{"tp": lax.rem(x + k, nx)} for k in range(1, nx)]
    peers += [{"dp": 1 - core}]
    for k in range(nx):
        peers += [dict(above, tp=k), dict(below, tp=k)]
    for peer in peers:
        pl.semaphore_signal(barrier, inc=1, device_id=peer, device_id_type=MESH)

    loads = [
        pltpu.make_async_copy(origin, target, local_sem.at[5 + i])
        for i, (origin, target) in enumerate(
            (
                (modw_in, modw),
                (condition_in, condition),
                (source_in, source),
                (gain_in, gain),
                (out_gain_in, out_gain),
                (conv_x_in, conv_x),
                (conv_b_in, conv_b),
                (conv_c_in, conv_c),
                (rate_in, rate),
                (context, ctx.at[y]),
            )
        )
    ]
    own_latent = pltpu.make_async_copy(latent, lat.at[x], local_sem.at[3])
    for c in loads[:3]:
        c.start()
    own_latent.start()
    for c in loads[3:]:
        c.start()
    half = model // 2
    own_half = pl.ds(pl.multiple_of(core * half, half), half)
    out_half = pl.ds(pl.multiple_of(core * (INNER // 2), INNER // 2), INNER // 2)
    pieces = (
        (w_dt, dt_rows.at[:, :, own_half]),
        (w_x, weights.at[own_half, pl.ds(0, INNER)]),
        (w_b, weights.at[own_half, pl.ds(COL_B, STATE)]),
        (w_c, weights.at[own_half, pl.ds(COL_C, STATE)]),
        (w_z, weights.at[own_half, pl.ds(COL_Z, INNER)]),
        (w_out, out_weights.at[out_half, :]),
    )
    groups = (0, 1, 1, 1, 1, 2)
    local = [
        pltpu.make_async_copy(origin, target, local_sem.at[i])
        for i, (origin, target) in zip(groups, pieces)
    ]
    in_bulk = weights.at[own_half, pl.ds(0, COLS - LANES)]
    bulk_local = [
        local[0],
        pltpu.make_async_copy(in_bulk, in_bulk, local_sem.at[1]),
        local[-1],
    ]
    def unpack(r, ref):
        piece = ref[...].astype(F32)
        for k in range(piece.shape[0]):
            small[r : r + 1, k * LANES : (k + 1) * LANES] = piece[k : k + 1]

    placed[...] = jnp.zeros_like(placed)
    for c in loads[:3]:
        c.wait()
    unpack(1, source)
    small[0:1, 0:model] = condition[...].astype(F32)

    rows = modw.shape[1]
    chunk = placed.shape[1]
    per = chunk // rows
    at = pl.ds(pl.multiple_of(lax.rem(place, per) * rows, rows), rows)
    placed[:, at, :] = modw[...]
    lane_at = pl.ds(pl.multiple_of((place // per) * chunk, chunk), chunk)
    act = jnp.broadcast_to(rounded(silu(small[0:1, lane_at])), (8, chunk))
    act_ctx = jnp.broadcast_to(rounded(silu(small[1:2, lane_at])), (8, chunk))
    row8 = rows_of((8, chunk))
    partial = jnp.zeros((8, width), F32)
    for k in range(3):
        left = jnp.where(row8 == k, act, 0.0)
        if k < 2:
            left = jnp.where(row8 == 3 + k, act_ctx, left)
        partial = partial + jnp.dot(
            left.astype(BF16), placed[k], preferred_element_type=F32
        )
    for r in range(5):
        mod_y[y, r] = partial[r : r + 1]

    pl.semaphore_wait(barrier, len(peers))
    pairs = iter(range(32))

    def along(axis, size, me, origin, target, bulk):
        return Exchange(axis, size, me, origin, target, pair_sems.at[next(pairs)], bulk)

    def gather(axis, size, me, buf):
        own = buf.at[me]
        return along(axis, size, me, lambda peer: own, own, buf.at[pl.ds(0, size - 1)])

    mods = [
        gather("sp_1", ny, y, mod_y),
        gather("sp_0", nz, z, mod_z),
        gather("tp", nx, x, mod_x),
    ]
    mods[0].start()
    ctx_copies = along(
        "sp_1", ny, y, lambda peer: context, ctx.at[y], ctx.at[pl.ds(0, ny - 1)]
    ).start()
    lat_copies = along(
        "tp", nx, x, lambda peer: latent, lat.at[x], lat.at[pl.ds(0, nx - 1)]
    ).start()
    swaps = [
        pltpu.make_async_remote_copy(
            src_ref=origin,
            dst_ref=target,
            send_sem=core_send.at[i],
            recv_sem=core_recv.at[i],
            device_id={"dp": 1 - core},
            device_id_type=MESH,
        )
        for i, (origin, target) in zip(groups, pieces)
    ]
    bulk_swaps = [
        swaps[0],
        pltpu.make_async_remote_copy(
            src_ref=in_bulk,
            dst_ref=in_bulk,
            send_sem=core_send.at[1],
            recv_sem=core_recv.at[1],
            device_id={"dp": 1 - core},
            device_id_type=MESH,
        ),
        swaps[-1],
    ]
    for c, d in zip(swaps, local):
        c.start()
        d.start()

    def edge(slot, k, to):
        return pltpu.make_async_remote_copy(
            src_ref=edge_send.at[slot],
            dst_ref=edge_recv.at[slot],
            send_sem=edge_sems.at[slot, k],
            recv_sem=edge_got.at[slot],
            device_id=to,
            device_id_type=MESH,
        )

    to_above = [edge(0, k, dict(above, tp=k)) for k in range(nx)]
    to_below = [edge(1, k, dict(below, tp=k)) for k in range(nx)]
    own_latent.wait()

    @pl.when(x == nx - 1)
    def _():
        edge_send[0] = lat[x].astype(F32)[own_rows - 1 : own_rows, :]
        for c in to_above:
            c.start()

    @pl.when(x == 0)
    def _():
        edge_send[1] = lat[x].astype(F32)[0:1, :]
        for c in to_below:
            c.start()

    small[2:7, :] = jnp.zeros((5, small.shape[1]), F32)
    for c in loads[3:]:
        c.wait()
    unpack(2, gain)
    unpack(3, out_gain)
    small[4:7, 0:INNER] = conv_x[...].astype(F32)
    small[4:7, INNER : INNER + STATE] = conv_b[...].astype(F32)
    small[4:7, INNER + STATE : MIXED] = conv_c[...].astype(F32)
    lane = lanes_of((1, LANES))
    rates = jnp.zeros((1, LANES), F32)
    for way in range(2):
        for h in range(HEADS):
            rates = jnp.where(lane == way * HEADS + h, rate[way : way + 1, h : h + 1], rates)

    mods[0].arrived()
    total = mod_y[0]
    for k in range(1, ny):
        total = total + mod_y[k]
    mod_z[z] = total
    mods[1].start()

    def inverse(v):
        return lax.rsqrt(jnp.mean(v * v, axis=1, keepdims=True) + EPSILON)

    mods[1].arrived()
    total = mod_z[0]
    for k in range(1, nz):
        total = total + mod_z[k]
    mod_x[x] = total
    mods[2].start()

    ctx_copies.arrived()
    edge_send[2] = ctx[ny - 1].astype(F32)[CTX_ROWS - 1 : CTX_ROWS, :]
    edge_send[3] = ctx[0].astype(F32)[0:1, :]
    ctx_edges = [
        edge(2, 0, {"sp_0": lax.rem(z + 1, nz)}),
        edge(3, 0, {"sp_0": lax.rem(z + nz - 1, nz)}),
    ]
    for c in ctx_edges:
        c.start()

    lat_copies.arrived()
    scales = [inverse(lat[t].astype(F32)) for t in range(nx)]
    misc[...] = jnp.zeros_like(misc)
    for c in (to_above[0], to_below[0], *ctx_edges):
        c.wait_recv()
    has = (place > 0, place < count - 1, z > 0, z < nz - 1)
    for slot in range(4):
        misc[slot : slot + 1, :] = jnp.where(has[slot], edge_recv[slot], 0.0)
    misc_scale = inverse(misc[...])
    ctx_scales = [inverse(ctx[j].astype(F32)) for j in range(ny)]
    row16 = rows_of((16, 1))
    kept = jnp.zeros((16, 1), jnp.bool_)
    for slot in range(4):
        kept = jnp.logical_or(kept, jnp.logical_and(row16 == slot, has[slot]))

    bulk_local[0].wait()
    bulk_swaps[0].wait_recv()
    dt_wide[...] = jnp.zeros_like(dt_wide)
    for way in range(2):
        dt_wide[way * HEADS : (way + 1) * HEADS, :] = dt_rows[way].astype(F32)
    for b in range(model // LANES):
        at = slice(b * LANES, (b + 1) * LANES)
        weights[at, COL_DT:COL_C] = dt_wide[:, at].T.astype(BF16)
    bulk_local[1].wait()
    bulk_swaps[1].wait_recv()

    mods[2].arrived()

    def modulations(c, shift, scale):
        cols = slice(c * width, (c + 1) * width)
        return cols, small[2:3, cols] * (1.0 + mod_x[c, scale]), mod_x[c, shift]

    for c in range(nx):
        cols, scale, shift = modulations(c, 0, 1)
        _, scale_ctx, shift_ctx = modulations(c, 3, 4)
        for t in range(nx):
            value = lat[t, :, cols].astype(F32) * scales[t] * scale + shift
            hidden[t * own_rows : (t + 1) * own_rows, cols] = value.astype(BF16)
        value = misc[:, cols] * misc_scale * jnp.where(row16 < 2, scale, scale_ctx)
        value = value + jnp.where(row16 < 2, shift, shift_ctx)
        hidden[TOKENS:ctx_at, cols] = jnp.where(kept, value, 0.0).astype(BF16)
        for j in range(0, ny, 2):
            two = [
                ctx[i, :, cols].astype(F32) * ctx_scales[i] * scale_ctx + shift_ctx
                for i in (j, j + 1)
            ]
            at = ctx_at + j * CTX_ROWS
            hidden[at : at + 2 * CTX_ROWS, cols] = jnp.concatenate(two, axis=0).astype(BF16)

    def project(rows, left, right):
        while left < right:
            wide = min(256, right - left)
            cols = slice(left, left + wide)
            feats[rows, cols] = rounded(
                jnp.dot(hidden[rows, :], weights[:, cols], preferred_element_type=F32)
            )
            left += wide

    def smooth(rows, low, at, tap_at):
        cols = slice(at, at + LANES)
        feats[rows, cols] = convolved(
            feats[rows, cols],
            feats[low : low + 1, cols],
            feats[low + 1 : low + 2, cols],
            small[4:7, tap_at : tap_at + LANES],
        )

    own = slice(0, TOKENS)
    project(slice(0, ctx_at + lines), 0, COL_C)
    for at in range(0, COL_DT, LANES):
        smooth(own, TOKENS, at, at)
    b_turned = feats[own, COL_B:COL_DT].T.astype(BF16)
    steps = softplus(feats[own, COL_DT:COL_C])
    sums = running_sums(-rates * steps, HEADS)
    ends = jnp.where(lane < HEADS, sums[TOKENS - 1 : TOKENS], sums[0:1])
    for way in range(2):
        for q in range(PAIRS):
            r = way * PAIRS + q
            decay_y[y, r : r + 1, :] = spread(ends, 2 * r)
    decay_copies = gather("sp_1", ny, y, decay_y).start()

    def slabs(axis, size, me, origin, target, piece):
        return along(
            axis,
            size,
            me,
            lambda peer: origin.at[piece, peer],
            target.at[piece, me],
            target.at[piece, pl.ds(0, size - 1)],
        )

    state_copies = []

    def send_states(way):
        for q in range(PAIRS):
            cols = slice(q * LANES, (q + 1) * LANES)
            piece = way * 2 + q // 2
            at = slice(q % 2 * LANES, (q % 2 + 1) * LANES)
            head = way * HEADS + 2 * q
            step = spread(steps, head)
            decay = spread(sums, head)
            end = decay[TOKENS - 1 : TOKENS] if way == 0 else decay[0:1]
            moved_x = rounded(feats[own, cols] * step)
            moved[way * TOKENS : (way + 1) * TOKENS, cols] = moved_x.astype(BF16)
            growth[way, :, cols] = jnp.exp(decay)
            at_end = (moved_x * jnp.exp(end - decay)).astype(BF16)
            state = jnp.dot(b_turned, at_end, preferred_element_type=F32).astype(BF16)
            for p in range(ny):
                state_send[piece, p, :, at] = state[p * slab : (p + 1) * slab]
            if q % 2 == 1:
                state_copies.append(
                    slabs("sp_1", ny, y, state_send, state_recv, piece).start()
                )
                state_recv[piece, y] = state_send[piece, y]

    send_states(0)

    ctx_rows = slice(ctx_at, ctx_at + lines)
    for at in range(0, COL_DT, LANES):
        smooth(ctx_rows, TOKENS + 2, at, at)
    ctx_bt[...] = feats[ctx_rows, COL_B:COL_DT].T
    ctx_b = ctx_bt[pl.ds(pl.multiple_of(y * slab, slab), slab), :]
    ctx_steps = softplus(feats[ctx_rows, COL_DT:COL_C])
    ctx_sums = running_sums(-rates * ctx_steps, HEADS)
    ctx_ends = jnp.where(lane < HEADS, ctx_sums[lines - 1 : lines], ctx_sums[0:1])
    for r in range(2 * PAIRS):
        ctx_dz[z, r : r + 1, :] = spread(ctx_ends, 2 * r)
    ctx_dz_copies = gather("sp_0", nz, z, ctx_dz).start()
    ctx_copies_z = []
    for way in range(2):
        for q in range(PAIRS):
            cols = slice(q * LANES, (q + 1) * LANES)
            head = way * HEADS + 2 * q
            decay = spread(ctx_sums, head)
            end = decay[lines - 1 : lines] if way == 0 else decay[0:1]
            moved_x = rounded(feats[ctx_rows, cols] * spread(ctx_steps, head))
            ctx_z[way, z, :, cols] = jnp.dot(
                ctx_b,
                moved_x * jnp.exp(end - decay),
                preferred_element_type=F32,
                precision=lax.Precision.HIGHEST,
            ).astype(BF16)
        ctx_copies_z.append(gather("sp_0", nz, z, ctx_z.at[way]).start())

    send_states(1)
    project(slice(0, ctx_at), COL_C, COL_Z)

    smooth(own, TOKENS, COL_C, INNER + STATE)
    c_vals = feats[own, COL_C:COL_Z].astype(BF16)
    project(own, COL_Z, COLS)
    for at in range(COL_Z, COLS, LANES):
        feats[own, at : at + LANES] = silu(feats[own, at : at + LANES])
    for c in range(nx):
        gate[:, c * width : (c + 1) * width] = mod_x[c, 2]
    scores = jnp.dot(c_vals, b_turned, preferred_element_type=F32)
    turned = sums.T
    square = (TOKENS, TOKENS)
    lower = rows_of(square) >= lanes_of(square)
    upper = rows_of(square) <= lanes_of(square)
    for q in range(PAIRS):
        cols = slice(q * LANES, (q + 1) * LANES)
        halves = []
        for h in (2 * q, 2 * q + 1):
            both = []
            for way, mask in ((0, lower), (1, upper)):
                col = way * HEADS + h
                gap = sums[:, col : col + 1] - turned[col : col + 1, :]
                decayed = scores * jnp.exp(jnp.minimum(gap, 0.0))
                both.append(jnp.where(mask, decayed, 0.0).astype(BF16))
            halves.append(
                jnp.dot(
                    jnp.concatenate(both, axis=1),
                    moved[:, cols],
                    preferred_element_type=F32,
                )
            )
        inside[:, cols] = jnp.where(lanes_of(square) < LANES // 2, halves[0], halves[1])

    decay_copies.arrived()
    decays = [decay_y[j] for j in range(ny)]
    is_fwd = rows_of((8, LANES)) < PAIRS
    ahead = [None] * ny
    acc_f = acc_b = jnp.zeros((8, LANES), F32)
    for j in range(ny):
        ahead[j] = acc_f
        acc_f = acc_f + decays[j]
    for j in reversed(range(ny)):
        ahead[j] = jnp.exp(jnp.where(is_fwd, ahead[j], acc_b))
        acc_b = acc_b + decays[j]
    tot_dz[z] = acc_f
    tot_dz_copies = gather("sp_0", nz, z, tot_dz).start()
    factors = [jnp.exp(d) for d in decays]
    tot_copies = []
    for piece in range(4):
        way = piece // 2
        state_copies[piece].arrived()
        for q in range(2):
            cols = slice(q * LANES, (q + 1) * LANES)
            r = piece * 2 + q
            state = jnp.zeros((slab, LANES), F32)
            for j in range(ny) if way == 0 else reversed(range(ny)):
                before[piece, j, :, cols] = state
                state = state * factors[j][r : r + 1] + state_recv[piece, j, :, cols].astype(F32)
            tot_z[piece, z, :, cols] = state.astype(BF16)
        tot_copies.append(
            Totals(way, tot_z.at[piece], nz, z, tot_sems.at[piece % 2]).start()
        )

    ctx_dz_copies.arrived()
    ctx_factors = [jnp.exp(ctx_dz[j]) for j in range(nz)]
    tot_dz_copies.arrived()
    tot_factors = [jnp.exp(tot_dz[j]) for j in range(nz)]
    enter_copies = []
    for piece in range(4):
        way = piece // 2
        order = list(range(nz)) if way == 0 else list(reversed(range(nz)))
        if piece % 2 == 0:
            ctx_copies_z[way].arrived()
        starts = []
        for q in range(2):
            cols = slice(q * LANES, (q + 1) * LANES)
            r = piece * 2 + q
            at = (piece % 2) * PIECE + q * LANES
            state = jnp.zeros((slab, LANES), F32)
            for j in order:
                fresh = ctx_z[way, j, :, at : at + LANES].astype(F32)
                state = state * ctx_factors[j][r : r + 1] + fresh
            starts.append(state)
        tot_copies[piece].arrived()
        for q in range(2):
            cols = slice(q * LANES, (q + 1) * LANES)
            r = piece * 2 + q
            state = starts[q]
            for j in order:
                passed = j < z if way == 0 else j > z
                later = state * tot_factors[j][r : r + 1] + tot_z[piece, j, :, cols].astype(F32)
                state = jnp.where(passed, later, state)
            for j in range(ny):
                enter_send[piece, j, :, cols] = (
                    before[piece, j, :, cols] + ahead[j][r : r + 1] * state
                ).astype(BF16)
        enter_copies.append(slabs("sp_1", ny, y, enter_send, enter_recv, piece).start())
        enter_recv[piece, y] = enter_send[piece, y]

    squares = jnp.zeros((TOKENS, 1), F32)
    for piece in range(4):
        way = piece // 2
        enter_copies[piece].arrived()
        carried = jnp.dot(
            c_vals, enter_recv[piece].reshape(STATE, PIECE), preferred_element_type=F32
        )
        for q in range(2):
            at = (piece % 2) * PIECE + q * LANES
            cols = slice(at, at + LANES)
            value = inside[:, cols]
            value = value + growth[way, :, cols] * carried[:, q * LANES : (q + 1) * LANES]
            if way == 1:
                value = value * feats[own, COL_Z + at : COL_Z + at + LANES]
                squares = squares + jnp.sum(value * value, axis=1, keepdims=True)
            inside[:, cols] = value
    scale = lax.rsqrt(squares / INNER + EPSILON)
    for q in range(PAIRS):
        cols = slice(q * LANES, (q + 1) * LANES)
        normed[:, cols] = (inside[:, cols] * scale * small[3:4, cols]).astype(BF16)

    bulk_local[-1].wait()
    bulk_swaps[-1].wait_recv()
    part_copies = []
    for c in range(nx):
        cols = slice(c * width, (c + 1) * width)
        term = jnp.dot(normed[...], out_weights[:, cols], preferred_element_type=F32)
        term = term.astype(BF16)
        for t in range(nx):
            part_send[t, :, cols] = term[t * own_rows : (t + 1) * own_rows]
        part_copies.append(
            along(
                "tp",
                nx,
                x,
                lambda peer, cols=cols: part_send.at[peer, :, cols],
                parts.at[x, :, cols],
                parts.at[pl.ds(0, nx - 1), :, cols],
            ).start()
        )
    own_part = pltpu.make_async_copy(part_send.at[x], parts.at[x], local_sem.at[4])
    own_part.start()
    for e in bulk_swaps + ctx_edges:
        e.wait_send()

    @pl.when(x == nx - 1)
    def _():
        for c in to_above:
            c.wait_send()

    @pl.when(x == 0)
    def _():
        for c in to_below:
            c.wait_send()

    done = mods + [ctx_copies, lat_copies, decay_copies, ctx_dz_copies, tot_dz_copies]
    done += ctx_copies_z + state_copies + tot_copies + enter_copies
    for e in done + part_copies:
        e.left()
    own_part.wait()
    for e in part_copies:
        e.arrived()


def shards(
    sizes,
    latent,
    condition,
    context,
    context_source,
    mod_weight,
    norm_gain,
    w_x,
    w_b,
    w_c,
    w_z,
    w_dt,
    conv_x,
    conv_b,
    conv_c,
    decay_rate,
    out_gain,
    w_out,
):
    nz, ny, nx = sizes
    model = latent.shape[-1]
    own_rows = latent.shape[1]
    width = model // nx
    slab = STATE // ny
    span = max(model, 1024)
    rows = mod_weight.shape[1]
    lines = ny * CTX_ROWS
    total_rows = TOKENS + 16 + lines
    vmem = pl.BlockSpec(memory_space=pltpu.VMEM)
    hbm = pl.BlockSpec(memory_space=pl.ANY)
    dma = pltpu.SemaphoreType.DMA
    scratch = [
        pltpu.VMEM((1, model), BF16),
        pltpu.VMEM((model // LANES, LANES), BF16),
        pltpu.VMEM((model // LANES, LANES), BF16),
        pltpu.VMEM((INNER // LANES, LANES), BF16),
        pltpu.VMEM((3, INNER), BF16),
        pltpu.VMEM((3, STATE), BF16),
        pltpu.VMEM((3, STATE), BF16),
        pltpu.VMEM((2, HEADS), F32),
        pltpu.VMEM((3, rows, width), BF16),
        pltpu.VMEM((model, COLS), BF16),
        pltpu.VMEM((INNER, model), BF16),
        pltpu.VMEM((2, HEADS, model), BF16),
        pltpu.VMEM((LANES, model), F32),
        pltpu.VMEM((8, span), F32),
        pltpu.VMEM((nx, own_rows, model), BF16),
        pltpu.VMEM((ny, CTX_ROWS, model), BF16),
        pltpu.VMEM((3, max(rows, LANES), width), BF16),
        pltpu.VMEM((nz, 5, 1, width), F32),
        pltpu.VMEM((ny, 5, 1, width), F32),
        pltpu.VMEM((nx, 5, 1, width), F32),
        pltpu.VMEM((4, 1, model), F32),
        pltpu.VMEM((4, 1, model), F32),
        pltpu.VMEM((16, model), F32),
        pltpu.VMEM((total_rows, model), BF16),
        pltpu.VMEM((total_rows, COLS), F32),
        pltpu.VMEM((2 * TOKENS, INNER), BF16),
        pltpu.VMEM((2, TOKENS, INNER), F32),
        pltpu.VMEM((TOKENS, INNER), F32),
        pltpu.VMEM((STATE, lines), F32),
        pltpu.VMEM((2, nz, slab, INNER), BF16),
        pltpu.VMEM((nz, 8, LANES), F32),
        pltpu.VMEM((4, ny, slab, PIECE), BF16),
        pltpu.VMEM((4, ny, slab, PIECE), BF16),
        pltpu.VMEM((ny, 8, LANES), F32),
        pltpu.VMEM((4, nz, slab, PIECE), BF16),
        pltpu.VMEM((nz, 8, LANES), F32),
        pltpu.VMEM((4, ny, slab, PIECE), F32),
        pltpu.VMEM((4, ny, slab, PIECE), BF16),
        pltpu.VMEM((4, ny, slab, PIECE), BF16),
        pltpu.VMEM((TOKENS, INNER), BF16),
        pltpu.VMEM((nx, own_rows, model), BF16),
        dma((15,)),
        dma((3,)),
        dma((3,)),
        dma((18 + nx, 2)),
        dma((4, nx)),
        dma((4,)),
        dma((2, 2, nz - 1)),
    ]
    parts, gate = pl.pallas_call(
        functools.partial(mixer, (nz, ny, nx, model)),
        out_shape=(
            jax.ShapeDtypeStruct((nx, own_rows, model), BF16),
            jax.ShapeDtypeStruct((1, model), F32),
        ),
        in_specs=[hbm] * 17,
        out_specs=(hbm, vmem),
        scratch_shapes=scratch,
        compiler_params=pltpu.CompilerParams(
            collective_id=0, has_side_effects=True, vmem_limit_bytes=56 * 1024 * 1024
        ),
    )(
        condition,
        context_source.reshape(-1, LANES),
        norm_gain.reshape(-1, LANES),
        out_gain.reshape(-1, LANES),
        conv_x,
        conv_b,
        conv_c,
        decay_rate,
        mod_weight,
        context[0],
        latent[0],
        w_x,
        w_b,
        w_c,
        w_z,
        jnp.swapaxes(w_dt, 1, 2),
        w_out,
    )
    mixed = parts[0].astype(F32)
    for k in range(1, nx):
        mixed = mixed + parts[k].astype(F32)
    return (gate * mixed).astype(BF16)[None]


def solution(mesh):
    nx = mesh.shape["tp"]
    ny = 8
    nz = mesh.shape["sp"] // ny
    return program(mesh, nz, ny, nx)


def program(mesh, nz, ny, nx):
    torus = Mesh(
        mesh.devices.reshape(nz, ny, nx, mesh.shape["dp"]), ("sp_0", "sp_1", "tp", "dp")
    )
    placed = (
        P("dp", SP_TP, None),
        P("dp", None),
        P("dp", SP, None),
        P(),
        P(None, SP, "tp"),
        P(),
        P("dp", "tp"),
        P("dp", "tp"),
        P("dp", "tp"),
        P("dp", "tp"),
        P(None, "dp", "tp"),
        P(None, "tp"),
        P(None, "tp"),
        P(None, "tp"),
        P(None, "tp"),
        P("tp"),
        P(("tp", "dp"), None),
    )
    return jax.shard_map(
        functools.partial(shards, (nz, ny, nx)),
        mesh=torus,
        in_specs=placed,
        out_specs=P("dp", SP_TP, None),
        check_vma=False,
    )
```

```python
import functools

import jax
import jax.numpy as jnp
from jax import lax
from jax.experimental import pallas as pl
from jax.experimental.pallas import tpu as pltpu
from jax.sharding import Mesh
from jax.sharding import PartitionSpec as P

SP = ("sp_0", "sp_1")
SP_TP = ("sp_0", "sp_1", "tp")
MESH = pl.DeviceIdType.MESH
EPSILON = 1e-06
F32 = jnp.float32
BF16 = jnp.bfloat16
TOKENS = 128
STATE = 128
LANES = 128
HEADS = 8
PAIRS = HEADS // 2
INNER = 512
MIXED = INNER + 2 * STATE
COL_B = INNER
COL_DT = COL_B + STATE
COL_C = COL_DT + LANES
COL_Z = COL_C + STATE
COLS = COL_Z + INNER
PIECE = 2 * LANES
CTX_ROWS = 8


def rounded(v):
    return v.astype(BF16).astype(F32)


def silu(v):
    return v / (1.0 + jnp.exp(-v))


def softplus(v):
    return jnp.maximum(v, 0.0) + jnp.log1p(jnp.exp(-jnp.abs(v)))


def rows_of(shape):
    return lax.broadcasted_iota(jnp.int32, shape, 0)


def lanes_of(shape):
    return lax.broadcasted_iota(jnp.int32, shape, 1)


def running_sums(v, heads):
    n = v.shape[0]
    row = rows_of(v.shape)
    down = up = v
    step = 1
    while step < n:
        down = down + jnp.where(row >= step, pltpu.roll(down, step, 0), 0.0)
        up = up + jnp.where(row < n - step, pltpu.roll(up, n - step, 0), 0.0)
        step *= 2
    return jnp.where(lanes_of(v.shape) < heads, down, up)


def spread(v, head):
    shape = (v.shape[0], LANES)
    left = jnp.broadcast_to(v[:, head : head + 1], shape)
    right = jnp.broadcast_to(v[:, head + 1 : head + 2], shape)
    return jnp.where(lanes_of(shape) < LANES // 2, left, right)


def convolved(mid, low, high, taps):
    n = mid.shape[0]
    row = rows_of(mid.shape)
    before = jnp.where(row == 0, low, pltpu.roll(mid, 1, 0))
    after = jnp.where(row == n - 1, high, pltpu.roll(mid, n - 1, 0))
    summed = before * taps[0:1] + mid * taps[1:2] + after * taps[2:3]
    return rounded(silu(summed))


class Exchange:
    def __init__(self, axis, size, place, source, target, sems, bulk):
        def copy(peer, origin, end):
            return pltpu.make_async_remote_copy(
                src_ref=origin,
                dst_ref=end,
                send_sem=sems.at[0],
                recv_sem=sems.at[1],
                device_id={axis: peer},
                device_id_type=MESH,
            )

        peers = [lax.rem(place + k, size) for k in range(1, size)]
        self.copies = [copy(peer, source(peer), target) for peer in peers]
        self.whole = copy(peers[0], bulk, bulk)

    def start(self):
        for c in self.copies:
            c.start()
        return self

    def arrived(self):
        self.whole.wait_recv()

    def left(self):
        self.whole.wait_send()


class Totals:
    def __init__(self, way, buf, size, place, sems):
        self.sends, self.gets, self.copies = [], [], []
        for k in range(1, size):
            later = place + k < size
            passed = place >= k
            self.sends.append(later if way == 0 else jnp.logical_not(later))
            self.gets.append(passed if way == 0 else jnp.logical_not(passed))
            self.copies.append(
                pltpu.make_async_remote_copy(
                    src_ref=buf.at[place],
                    dst_ref=buf.at[place],
                    send_sem=sems.at[0, k - 1],
                    recv_sem=sems.at[1, k - 1],
                    device_id={"sp_0": lax.rem(place + k, size)},
                    device_id_type=MESH,
                )
            )

    def start(self):
        for taken, c in zip(self.sends, self.copies):
            pl.when(taken)(c.start)
        return self

    def arrived(self):
        for taken, c in zip(self.gets, self.copies):
            pl.when(taken)(c.wait_recv)

    def left(self):
        for taken, c in zip(self.sends, self.copies):
            pl.when(taken)(c.wait_send)


def mixer(
    dims,
    condition_in,
    source_in,
    gain_in,
    out_gain_in,
    conv_x_in,
    conv_b_in,
    conv_c_in,
    rate_in,
    modw_in,
    context,
    latent,
    w_x,
    w_b,
    w_c,
    w_z,
    w_dt,
    w_out,
    update,
    condition,
    source,
    gain,
    out_gain,
    conv_x,
    conv_b,
    conv_c,
    rate,
    modw,
    weights,
    out_weights,
    dt_rows,
    dt_wide,
    small,
    lat,
    ctx,
    placed,
    mod_z,
    mod_y,
    mod_x,
    edge_send,
    edge_recv,
    misc,
    hidden,
    feats,
    moved,
    growth,
    inside,
    ctx_bt,
    ctx_z,
    ctx_dz,
    state_send,
    state_recv,
    decay_y,
    tot_z,
    tot_dz,
    before,
    enter_send,
    enter_recv,
    normed,
    part_send,
    parts,
    local_sem,
    core_send,
    core_recv,
    pair_sems,
    edge_sems,
    edge_got,
    tot_sems,
):
    nz, ny, nx, model = dims
    width = model // nx
    own_rows = TOKENS // nx
    slab = STATE // ny
    lines = ny * CTX_ROWS
    ctx_at = TOKENS + 16
    z = lax.axis_index("sp_0")
    y = lax.axis_index("sp_1")
    x = lax.axis_index("tp")
    core = lax.axis_index("dp")
    place = z * ny + y
    count = nz * ny

    barrier = pltpu.get_barrier_semaphore()
    up_place = lax.rem(place + 1, count)
    down_place = lax.rem(place + count - 1, count)
    above = {"sp_0": up_place // ny, "sp_1": lax.rem(up_place, ny)}
    below = {"sp_0": down_place // ny, "sp_1": lax.rem(down_place, ny)}
    peers = [{"sp_1": lax.rem(y + k, ny)} for k in range(1, ny)]
    peers += [{"sp_0": lax.rem(z + k, nz)} for k in range(1, nz)]
    peers += [{"tp": lax.rem(x + k, nx)} for k in range(1, nx)]
    peers += [{"dp": 1 - core}]
    for k in range(nx):
        peers += [dict(above, tp=k), dict(below, tp=k)]
    for peer in peers:
        pl.semaphore_signal(barrier, inc=1, device_id=peer, device_id_type=MESH)

    loads = [
        pltpu.make_async_copy(origin, target, local_sem.at[5 + i])
        for i, (origin, target) in enumerate(
            (
                (modw_in, modw),
                (condition_in, condition),
                (source_in, source),
                (gain_in, gain),
                (out_gain_in, out_gain),
                (conv_x_in, conv_x),
                (conv_b_in, conv_b),
                (conv_c_in, conv_c),
                (rate_in, rate),
                (context, ctx.at[y]),
            )
        )
    ]
    own_latent = pltpu.make_async_copy(latent, lat.at[x], local_sem.at[3])
    for c in loads[:3]:
        c.start()
    own_latent.start()
    for c in loads[3:]:
        c.start()
    half = model // 2
    own_half = pl.ds(pl.multiple_of(core * half, half), half)
    out_half = pl.ds(pl.multiple_of(core * (INNER // 2), INNER // 2), INNER // 2)
    pieces = (
        (w_dt, dt_rows.at[:, :, own_half]),
        (w_x, weights.at[own_half, pl.ds(0, INNER)]),
        (w_b, weights.at[own_half, pl.ds(COL_B, STATE)]),
        (w_c, weights.at[own_half, pl.ds(COL_C, STATE)]),
        (w_z, weights.at[own_half, pl.ds(COL_Z, INNER)]),
        (w_out, out_weights.at[out_half, :]),
    )
    groups = (0, 1, 1, 1, 1, 2)
    local = [
        pltpu.make_async_copy(origin, target, local_sem.at[i])
        for i, (origin, target) in zip(groups, pieces)
    ]
    in_bulk = weights.at[own_half, pl.ds(0, COLS - LANES)]
    bulk_local = [
        local[0],
        pltpu.make_async_copy(in_bulk, in_bulk, local_sem.at[1]),
        local[-1],
    ]
    def unpack(r, ref):
        piece = ref[...].astype(F32)
        for k in range(piece.shape[0]):
            small[r : r + 1, k * LANES : (k + 1) * LANES] = piece[k : k + 1]

    placed[...] = jnp.zeros_like(placed)
    for c in loads[:3]:
        c.wait()
    unpack(1, source)
    small[0:1, 0:model] = condition[...].astype(F32)

    rows = modw.shape[1]
    chunk = placed.shape[1]
    per = chunk // rows
    at = pl.ds(pl.multiple_of(lax.rem(place, per) * rows, rows), rows)
    placed[:, at, :] = modw[...]
    lane_at = pl.ds(pl.multiple_of((place // per) * chunk, chunk), chunk)
    act = jnp.broadcast_to(rounded(silu(small[0:1, lane_at])), (8, chunk))
    act_ctx = jnp.broadcast_to(rounded(silu(small[1:2, lane_at])), (8, chunk))
    row8 = rows_of((8, chunk))
    partial = jnp.zeros((8, width), F32)
    for k in range(3):
        left = jnp.where(row8 == k, act, 0.0)
        if k < 2:
            left = jnp.where(row8 == 3 + k, act_ctx, left)
        partial = partial + jnp.dot(
            left.astype(BF16), placed[k], preferred_element_type=F32
        )
    for r in range(5):
        mod_y[y, r] = partial[r : r + 1]

    pl.semaphore_wait(barrier, len(peers))
    pairs = iter(range(32))

    def along(axis, size, me, origin, target, bulk):
        return Exchange(axis, size, me, origin, target, pair_sems.at[next(pairs)], bulk)

    def gather(axis, size, me, buf):
        own = buf.at[me]
        return along(axis, size, me, lambda peer: own, own, buf.at[pl.ds(0, size - 1)])

    mods = [
        gather("sp_1", ny, y, mod_y),
        gather("sp_0", nz, z, mod_z),
        gather("tp", nx, x, mod_x),
    ]
    mods[0].start()
    ctx_copies = along(
        "sp_1", ny, y, lambda peer: context, ctx.at[y], ctx.at[pl.ds(0, ny - 1)]
    ).start()
    lat_copies = along(
        "tp", nx, x, lambda peer: latent, lat.at[x], lat.at[pl.ds(0, nx - 1)]
    ).start()
    swaps = [
        pltpu.make_async_remote_copy(
            src_ref=origin,
            dst_ref=target,
            send_sem=core_send.at[i],
            recv_sem=core_recv.at[i],
            device_id={"dp": 1 - core},
            device_id_type=MESH,
        )
        for i, (origin, target) in zip(groups, pieces)
    ]
    bulk_swaps = [
        swaps[0],
        pltpu.make_async_remote_copy(
            src_ref=in_bulk,
            dst_ref=in_bulk,
            send_sem=core_send.at[1],
            recv_sem=core_recv.at[1],
            device_id={"dp": 1 - core},
            device_id_type=MESH,
        ),
        swaps[-1],
    ]
    for c, d in zip(swaps, local):
        c.start()
        d.start()

    def edge(slot, k, to):
        return pltpu.make_async_remote_copy(
            src_ref=edge_send.at[slot],
            dst_ref=edge_recv.at[slot],
            send_sem=edge_sems.at[slot, k],
            recv_sem=edge_got.at[slot],
            device_id=to,
            device_id_type=MESH,
        )

    to_above = [edge(0, k, dict(above, tp=k)) for k in range(nx)]
    to_below = [edge(1, k, dict(below, tp=k)) for k in range(nx)]
    own_latent.wait()

    @pl.when(x == nx - 1)
    def _():
        edge_send[0] = lat[x].astype(F32)[own_rows - 1 : own_rows, :]
        for c in to_above:
            c.start()

    @pl.when(x == 0)
    def _():
        edge_send[1] = lat[x].astype(F32)[0:1, :]
        for c in to_below:
            c.start()

    small[2:7, :] = jnp.zeros((5, small.shape[1]), F32)
    for c in loads[3:]:
        c.wait()
    unpack(2, gain)
    unpack(3, out_gain)
    small[4:7, 0:INNER] = conv_x[...].astype(F32)
    small[4:7, INNER : INNER + STATE] = conv_b[...].astype(F32)
    small[4:7, INNER + STATE : MIXED] = conv_c[...].astype(F32)
    lane = lanes_of((1, LANES))
    rates = jnp.zeros((1, LANES), F32)
    for way in range(2):
        for h in range(HEADS):
            rates = jnp.where(lane == way * HEADS + h, rate[way : way + 1, h : h + 1], rates)

    mods[0].arrived()
    total = mod_y[0]
    for k in range(1, ny):
        total = total + mod_y[k]
    mod_z[z] = total
    mods[1].start()

    def inverse(v):
        return lax.rsqrt(jnp.mean(v * v, axis=1, keepdims=True) + EPSILON)

    mods[1].arrived()
    total = mod_z[0]
    for k in range(1, nz):
        total = total + mod_z[k]
    mod_x[x] = total
    mods[2].start()

    ctx_copies.arrived()
    edge_send[2] = ctx[ny - 1].astype(F32)[CTX_ROWS - 1 : CTX_ROWS, :]
    edge_send[3] = ctx[0].astype(F32)[0:1, :]
    ctx_edges = [
        edge(2, 0, {"sp_0": lax.rem(z + 1, nz)}),
        edge(3, 0, {"sp_0": lax.rem(z + nz - 1, nz)}),
    ]
    for c in ctx_edges:
        c.start()

    lat_copies.arrived()
    scales = [inverse(lat[t].astype(F32)) for t in range(nx)]
    misc[...] = jnp.zeros_like(misc)
    for c in (to_above[0], to_below[0], *ctx_edges):
        c.wait_recv()
    has = (place > 0, place < count - 1, z > 0, z < nz - 1)
    for slot in range(4):
        misc[slot : slot + 1, :] = jnp.where(has[slot], edge_recv[slot], 0.0)
    misc_scale = inverse(misc[...])
    ctx_scales = [inverse(ctx[j].astype(F32)) for j in range(ny)]
    row16 = rows_of((16, 1))
    kept = jnp.zeros((16, 1), jnp.bool_)
    for slot in range(4):
        kept = jnp.logical_or(kept, jnp.logical_and(row16 == slot, has[slot]))

    bulk_local[0].wait()
    bulk_swaps[0].wait_recv()
    dt_wide[...] = jnp.zeros_like(dt_wide)
    for way in range(2):
        dt_wide[way * HEADS : (way + 1) * HEADS, :] = dt_rows[way].astype(F32)
    for b in range(model // LANES):
        at = slice(b * LANES, (b + 1) * LANES)
        weights[at, COL_DT:COL_C] = dt_wide[:, at].T.astype(BF16)
    bulk_local[1].wait()
    bulk_swaps[1].wait_recv()

    mods[2].arrived()

    def modulations(c, shift, scale):
        cols = slice(c * width, (c + 1) * width)
        return cols, small[2:3, cols] * (1.0 + mod_x[c, scale]), mod_x[c, shift]

    for c in range(nx):
        cols, scale, shift = modulations(c, 0, 1)
        _, scale_ctx, shift_ctx = modulations(c, 3, 4)
        for t in range(nx):
            value = lat[t, :, cols].astype(F32) * scales[t] * scale + shift
            hidden[t * own_rows : (t + 1) * own_rows, cols] = value.astype(BF16)
        value = misc[:, cols] * misc_scale * jnp.where(row16 < 2, scale, scale_ctx)
        value = value + jnp.where(row16 < 2, shift, shift_ctx)
        hidden[TOKENS:ctx_at, cols] = jnp.where(kept, value, 0.0).astype(BF16)
        for j in range(0, ny, 2):
            two = [
                ctx[i, :, cols].astype(F32) * ctx_scales[i] * scale_ctx + shift_ctx
                for i in (j, j + 1)
            ]
            at = ctx_at + j * CTX_ROWS
            hidden[at : at + 2 * CTX_ROWS, cols] = jnp.concatenate(two, axis=0).astype(BF16)

    def project(rows, left, right):
        while left < right:
            wide = min(256, right - left)
            cols = slice(left, left + wide)
            feats[rows, cols] = rounded(
                jnp.dot(hidden[rows, :], weights[:, cols], preferred_element_type=F32)
            )
            left += wide

    def smooth(rows, low, at, tap_at):
        cols = slice(at, at + LANES)
        feats[rows, cols] = convolved(
            feats[rows, cols],
            feats[low : low + 1, cols],
            feats[low + 1 : low + 2, cols],
            small[4:7, tap_at : tap_at + LANES],
        )

    own = slice(0, TOKENS)
    project(slice(0, ctx_at + lines), 0, COL_C)
    for at in range(0, COL_DT, LANES):
        smooth(own, TOKENS, at, at)
    b_turned = feats[own, COL_B:COL_DT].T.astype(BF16)
    steps = softplus(feats[own, COL_DT:COL_C])
    sums = running_sums(-rates * steps, HEADS)
    ends = jnp.where(lane < HEADS, sums[TOKENS - 1 : TOKENS], sums[0:1])
    for way in range(2):
        for q in range(PAIRS):
            r = way * PAIRS + q
            decay_y[y, r : r + 1, :] = spread(ends, 2 * r)
    decay_copies = gather("sp_1", ny, y, decay_y).start()

    def slabs(axis, size, me, origin, target, piece):
        return along(
            axis,
            size,
            me,
            lambda peer: origin.at[piece, peer],
            target.at[piece, me],
            target.at[piece, pl.ds(0, size - 1)],
        )

    state_copies = []

    def send_states(way):
        for q in range(PAIRS):
            cols = slice(q * LANES, (q + 1) * LANES)
            piece = way * 2 + q // 2
            at = slice(q % 2 * LANES, (q % 2 + 1) * LANES)
            head = way * HEADS + 2 * q
            step = spread(steps, head)
            decay = spread(sums, head)
            end = decay[TOKENS - 1 : TOKENS] if way == 0 else decay[0:1]
            moved_x = rounded(feats[own, cols] * step)
            moved[way * TOKENS : (way + 1) * TOKENS, cols] = moved_x.astype(BF16)
            growth[way, :, cols] = jnp.exp(decay)
            at_end = (moved_x * jnp.exp(end - decay)).astype(BF16)
            state = jnp.dot(b_turned, at_end, preferred_element_type=F32).astype(BF16)
            for p in range(ny):
                state_send[piece, p, :, at] = state[p * slab : (p + 1) * slab]
            if q % 2 == 1:
                state_copies.append(
                    slabs("sp_1", ny, y, state_send, state_recv, piece).start()
                )
                state_recv[piece, y] = state_send[piece, y]

    send_states(0)

    ctx_rows = slice(ctx_at, ctx_at + lines)
    for at in range(0, COL_DT, LANES):
        smooth(ctx_rows, TOKENS + 2, at, at)
    ctx_bt[...] = feats[ctx_rows, COL_B:COL_DT].T
    ctx_b = ctx_bt[pl.ds(pl.multiple_of(y * slab, slab), slab), :]
    ctx_steps = softplus(feats[ctx_rows, COL_DT:COL_C])
    ctx_sums = running_sums(-rates * ctx_steps, HEADS)
    ctx_ends = jnp.where(lane < HEADS, ctx_sums[lines - 1 : lines], ctx_sums[0:1])
    for r in range(2 * PAIRS):
        ctx_dz[z, r : r + 1, :] = spread(ctx_ends, 2 * r)
    ctx_dz_copies = gather("sp_0", nz, z, ctx_dz).start()
    ctx_copies_z = []
    for way in range(2):
        for q in range(PAIRS):
            cols = slice(q * LANES, (q + 1) * LANES)
            head = way * HEADS + 2 * q
            decay = spread(ctx_sums, head)
            end = decay[lines - 1 : lines] if way == 0 else decay[0:1]
            moved_x = rounded(feats[ctx_rows, cols] * spread(ctx_steps, head))
            ctx_z[way, z, :, cols] = jnp.dot(
                ctx_b,
                moved_x * jnp.exp(end - decay),
                preferred_element_type=F32,
                precision=lax.Precision.HIGHEST,
            ).astype(BF16)
        ctx_copies_z.append(gather("sp_0", nz, z, ctx_z.at[way]).start())

    send_states(1)
    project(slice(0, ctx_at), COL_C, COL_Z)

    smooth(own, TOKENS, COL_C, INNER + STATE)
    c_vals = feats[own, COL_C:COL_Z].astype(BF16)
    project(own, COL_Z, COLS)
    for at in range(COL_Z, COLS, LANES):
        feats[own, at : at + LANES] = silu(feats[own, at : at + LANES])
    scores = jnp.dot(c_vals, b_turned, preferred_element_type=F32)
    turned = sums.T
    square = (TOKENS, TOKENS)
    lower = rows_of(square) >= lanes_of(square)
    upper = rows_of(square) <= lanes_of(square)
    for q in range(PAIRS):
        cols = slice(q * LANES, (q + 1) * LANES)
        halves = []
        for h in (2 * q, 2 * q + 1):
            both = []
            for way, mask in ((0, lower), (1, upper)):
                col = way * HEADS + h
                gap = sums[:, col : col + 1] - turned[col : col + 1, :]
                decayed = scores * jnp.exp(jnp.minimum(gap, 0.0))
                both.append(jnp.where(mask, decayed, 0.0).astype(BF16))
            halves.append(
                jnp.dot(
                    jnp.concatenate(both, axis=1),
                    moved[:, cols],
                    preferred_element_type=F32,
                )
            )
        inside[:, cols] = jnp.where(lanes_of(square) < LANES // 2, halves[0], halves[1])

    decay_copies.arrived()
    decays = [decay_y[j] for j in range(ny)]
    is_fwd = rows_of((8, LANES)) < PAIRS
    ahead = [None] * ny
    acc_f = acc_b = jnp.zeros((8, LANES), F32)
    for j in range(ny):
        ahead[j] = acc_f
        acc_f = acc_f + decays[j]
    for j in reversed(range(ny)):
        ahead[j] = jnp.exp(jnp.where(is_fwd, ahead[j], acc_b))
        acc_b = acc_b + decays[j]
    tot_dz[z] = acc_f
    tot_dz_copies = gather("sp_0", nz, z, tot_dz).start()
    factors = [jnp.exp(d) for d in decays]
    tot_copies = []
    for piece in range(4):
        way = piece // 2
        state_copies[piece].arrived()
        for q in range(2):
            cols = slice(q * LANES, (q + 1) * LANES)
            r = piece * 2 + q
            state = jnp.zeros((slab, LANES), F32)
            for j in range(ny) if way == 0 else reversed(range(ny)):
                before[piece, j, :, cols] = state
                state = state * factors[j][r : r + 1] + state_recv[piece, j, :, cols].astype(F32)
            tot_z[piece, z, :, cols] = state.astype(BF16)
        tot_copies.append(
            Totals(way, tot_z.at[piece], nz, z, tot_sems.at[piece % 2]).start()
        )

    ctx_dz_copies.arrived()
    ctx_factors = [jnp.exp(ctx_dz[j]) for j in range(nz)]
    tot_dz_copies.arrived()
    tot_factors = [jnp.exp(tot_dz[j]) for j in range(nz)]
    enter_copies = []
    for piece in range(4):
        way = piece // 2
        order = list(range(nz)) if way == 0 else list(reversed(range(nz)))
        if piece % 2 == 0:
            ctx_copies_z[way].arrived()
        starts = []
        for q in range(2):
            cols = slice(q * LANES, (q + 1) * LANES)
            r = piece * 2 + q
            at = (piece % 2) * PIECE + q * LANES
            state = jnp.zeros((slab, LANES), F32)
            for j in order:
                fresh = ctx_z[way, j, :, at : at + LANES].astype(F32)
                state = state * ctx_factors[j][r : r + 1] + fresh
            starts.append(state)
        tot_copies[piece].arrived()
        for q in range(2):
            cols = slice(q * LANES, (q + 1) * LANES)
            r = piece * 2 + q
            state = starts[q]
            for j in order:
                passed = j < z if way == 0 else j > z
                later = state * tot_factors[j][r : r + 1] + tot_z[piece, j, :, cols].astype(F32)
                state = jnp.where(passed, later, state)
            for j in range(ny):
                enter_send[piece, j, :, cols] = (
                    before[piece, j, :, cols] + ahead[j][r : r + 1] * state
                ).astype(BF16)
        enter_copies.append(slabs("sp_1", ny, y, enter_send, enter_recv, piece).start())
        enter_recv[piece, y] = enter_send[piece, y]

    squares = jnp.zeros((TOKENS, 1), F32)
    for piece in range(4):
        way = piece // 2
        enter_copies[piece].arrived()
        carried = jnp.dot(
            c_vals, enter_recv[piece].reshape(STATE, PIECE), preferred_element_type=F32
        )
        for q in range(2):
            at = (piece % 2) * PIECE + q * LANES
            cols = slice(at, at + LANES)
            value = inside[:, cols]
            value = value + growth[way, :, cols] * carried[:, q * LANES : (q + 1) * LANES]
            if way == 1:
                value = value * feats[own, COL_Z + at : COL_Z + at + LANES]
                squares = squares + jnp.sum(value * value, axis=1, keepdims=True)
            inside[:, cols] = value
    scale = lax.rsqrt(squares / INNER + EPSILON)
    for q in range(PAIRS):
        cols = slice(q * LANES, (q + 1) * LANES)
        normed[:, cols] = (inside[:, cols] * scale * small[3:4, cols]).astype(BF16)

    bulk_local[-1].wait()
    bulk_swaps[-1].wait_recv()
    part_copies = []
    for c in range(nx):
        cols = slice(c * width, (c + 1) * width)
        term = jnp.dot(normed[...], out_weights[:, cols], preferred_element_type=F32)
        term = term.astype(BF16)
        for t in range(nx):
            part_send[t, :, cols] = term[t * own_rows : (t + 1) * own_rows]
        part_copies.append(
            along(
                "tp",
                nx,
                x,
                lambda peer, cols=cols: part_send.at[peer, :, cols],
                parts.at[x, :, cols],
                parts.at[pl.ds(0, nx - 1), :, cols],
            ).start()
        )
    parts[x] = part_send[x]
    for e in bulk_swaps + ctx_edges:
        e.wait_send()

    @pl.when(x == nx - 1)
    def _():
        for c in to_above:
            c.wait_send()

    @pl.when(x == 0)
    def _():
        for c in to_below:
            c.wait_send()

    done = mods + [ctx_copies, lat_copies, decay_copies, ctx_dz_copies, tot_dz_copies]
    done += ctx_copies_z + state_copies + tot_copies + enter_copies
    for e in done + part_copies:
        e.left()
    for c in range(nx):
        cols = slice(c * width, (c + 1) * width)
        part_copies[c].arrived()
        value = parts[0, :, cols].astype(F32)
        for t in range(1, nx):
            value = value + parts[t, :, cols].astype(F32)
        update[:, cols] = (mod_x[c, 2] * value).astype(BF16)


def shards(
    sizes,
    latent,
    condition,
    context,
    context_source,
    mod_weight,
    norm_gain,
    w_x,
    w_b,
    w_c,
    w_z,
    w_dt,
    conv_x,
    conv_b,
    conv_c,
    decay_rate,
    out_gain,
    w_out,
):
    nz, ny, nx = sizes
    model = latent.shape[-1]
    own_rows = latent.shape[1]
    width = model // nx
    slab = STATE // ny
    span = max(model, 1024)
    rows = mod_weight.shape[1]
    lines = ny * CTX_ROWS
    total_rows = TOKENS + 16 + lines
    vmem = pl.BlockSpec(memory_space=pltpu.VMEM)
    hbm = pl.BlockSpec(memory_space=pl.ANY)
    dma = pltpu.SemaphoreType.DMA
    scratch = [
        pltpu.VMEM((1, model), BF16),
        pltpu.VMEM((model // LANES, LANES), BF16),
        pltpu.VMEM((model // LANES, LANES), BF16),
        pltpu.VMEM((INNER // LANES, LANES), BF16),
        pltpu.VMEM((3, INNER), BF16),
        pltpu.VMEM((3, STATE), BF16),
        pltpu.VMEM((3, STATE), BF16),
        pltpu.VMEM((2, HEADS), F32),
        pltpu.VMEM((3, rows, width), BF16),
        pltpu.VMEM((model, COLS), BF16),
        pltpu.VMEM((INNER, model), BF16),
        pltpu.VMEM((2, HEADS, model), BF16),
        pltpu.VMEM((LANES, model), F32),
        pltpu.VMEM((8, span), F32),
        pltpu.VMEM((nx, own_rows, model), BF16),
        pltpu.VMEM((ny, CTX_ROWS, model), BF16),
        pltpu.VMEM((3, max(rows, LANES), width), BF16),
        pltpu.VMEM((nz, 5, 1, width), F32),
        pltpu.VMEM((ny, 5, 1, width), F32),
        pltpu.VMEM((nx, 5, 1, width), F32),
        pltpu.VMEM((4, 1, model), F32),
        pltpu.VMEM((4, 1, model), F32),
        pltpu.VMEM((16, model), F32),
        pltpu.VMEM((total_rows, model), BF16),
        pltpu.VMEM((total_rows, COLS), F32),
        pltpu.VMEM((2 * TOKENS, INNER), BF16),
        pltpu.VMEM((2, TOKENS, INNER), F32),
        pltpu.VMEM((TOKENS, INNER), F32),
        pltpu.VMEM((STATE, lines), F32),
        pltpu.VMEM((2, nz, slab, INNER), BF16),
        pltpu.VMEM((nz, 8, LANES), F32),
        pltpu.VMEM((4, ny, slab, PIECE), BF16),
        pltpu.VMEM((4, ny, slab, PIECE), BF16),
        pltpu.VMEM((ny, 8, LANES), F32),
        pltpu.VMEM((4, nz, slab, PIECE), BF16),
        pltpu.VMEM((nz, 8, LANES), F32),
        pltpu.VMEM((4, ny, slab, PIECE), F32),
        pltpu.VMEM((4, ny, slab, PIECE), BF16),
        pltpu.VMEM((4, ny, slab, PIECE), BF16),
        pltpu.VMEM((TOKENS, INNER), BF16),
        pltpu.VMEM((nx, own_rows, model), BF16),
        pltpu.VMEM((nx, own_rows, model), BF16),
        dma((15,)),
        dma((3,)),
        dma((3,)),
        dma((18 + nx, 2)),
        dma((4, nx)),
        dma((4,)),
        dma((2, 2, nz - 1)),
    ]
    update = pl.pallas_call(
        functools.partial(mixer, (nz, ny, nx, model)),
        out_shape=pltpu.VMEM((own_rows, model), BF16),
        in_specs=[hbm] * 17,
        out_specs=vmem,
        scratch_shapes=scratch,
        compiler_params=pltpu.CompilerParams(
            collective_id=0, has_side_effects=True, vmem_limit_bytes=56 * 1024 * 1024
        ),
    )(
        condition,
        context_source.reshape(-1, LANES),
        norm_gain.reshape(-1, LANES),
        out_gain.reshape(-1, LANES),
        conv_x,
        conv_b,
        conv_c,
        decay_rate,
        mod_weight,
        context[0],
        latent[0],
        w_x,
        w_b,
        w_c,
        w_z,
        jnp.swapaxes(w_dt, 1, 2),
        w_out,
    )
    return update[None]


def solution(mesh):
    nx = mesh.shape["tp"]
    ny = 8
    nz = mesh.shape["sp"] // ny
    return program(mesh, nz, ny, nx)


def program(mesh, nz, ny, nx):
    torus = Mesh(
        mesh.devices.reshape(nz, ny, nx, mesh.shape["dp"]), ("sp_0", "sp_1", "tp", "dp")
    )
    placed = (
        P("dp", SP_TP, None),
        P("dp", None),
        P("dp", SP, None),
        P(),
        P(None, SP, "tp"),
        P(),
        P("dp", "tp"),
        P("dp", "tp"),
        P("dp", "tp"),
        P("dp", "tp"),
        P(None, "dp", "tp"),
        P(None, "tp"),
        P(None, "tp"),
        P(None, "tp"),
        P(None, "tp"),
        P("tp"),
        P(("tp", "dp"), None),
    )
    return jax.shard_map(
        functools.partial(shards, (nz, ny, nx)),
        mesh=torus,
        in_specs=placed,
        out_specs=P("dp", SP_TP, None),
        check_vma=False,
    )
```

```python
import functools

import jax
import jax.numpy as jnp
from jax import lax
from jax.experimental import pallas as pl
from jax.experimental.pallas import tpu as pltpu
from jax.sharding import Mesh
from jax.sharding import PartitionSpec as P

SP = ("sp_0", "sp_1")
SP_TP = ("sp_0", "sp_1", "tp")
MESH = pl.DeviceIdType.MESH
EPSILON = 1e-06
F32 = jnp.float32
BF16 = jnp.bfloat16
TOKENS = 128
STATE = 128
LANES = 128
HEADS = 8
PAIRS = HEADS // 2
INNER = 512
MIXED = INNER + 2 * STATE
COL_B = INNER
COL_DT = COL_B + STATE
COL_C = COL_DT + LANES
COL_Z = COL_C + STATE
COLS = COL_Z + INNER
PIECE = 2 * LANES
CTX_ROWS = 8


def rounded(v):
    return v.astype(BF16).astype(F32)


def silu(v):
    return v / (1.0 + jnp.exp(-v))


def softplus(v):
    return jnp.maximum(v, 0.0) + jnp.log1p(jnp.exp(-jnp.abs(v)))


def rows_of(shape):
    return lax.broadcasted_iota(jnp.int32, shape, 0)


def lanes_of(shape):
    return lax.broadcasted_iota(jnp.int32, shape, 1)


def running_sums(v, heads):
    n = v.shape[0]
    row = rows_of(v.shape)
    down = up = v
    step = 1
    while step < n:
        down = down + jnp.where(row >= step, pltpu.roll(down, step, 0), 0.0)
        up = up + jnp.where(row < n - step, pltpu.roll(up, n - step, 0), 0.0)
        step *= 2
    return jnp.where(lanes_of(v.shape) < heads, down, up)


def spread(v, head):
    shape = (v.shape[0], LANES)
    left = jnp.broadcast_to(v[:, head : head + 1], shape)
    right = jnp.broadcast_to(v[:, head + 1 : head + 2], shape)
    return jnp.where(lanes_of(shape) < LANES // 2, left, right)


def convolved(mid, low, high, taps):
    n = mid.shape[0]
    row = rows_of(mid.shape)
    before = jnp.where(row == 0, low, pltpu.roll(mid, 1, 0))
    after = jnp.where(row == n - 1, high, pltpu.roll(mid, n - 1, 0))
    summed = before * taps[0:1] + mid * taps[1:2] + after * taps[2:3]
    return rounded(silu(summed))


class Exchange:
    def __init__(self, axis, size, place, source, target, sems, bulk):
        def copy(peer, origin, end):
            return pltpu.make_async_remote_copy(
                src_ref=origin,
                dst_ref=end,
                send_sem=sems.at[0],
                recv_sem=sems.at[1],
                device_id={axis: peer},
                device_id_type=MESH,
            )

        peers = [lax.rem(place + k, size) for k in range(1, size)]
        self.copies = [copy(peer, source(peer), target) for peer in peers]
        self.whole = copy(peers[0], bulk, bulk)

    def start(self):
        for c in self.copies:
            c.start()
        return self

    def arrived(self):
        self.whole.wait_recv()

    def left(self):
        self.whole.wait_send()


class Totals:
    def __init__(self, way, buf, size, place, sems):
        def copy(peer, ref):
            return pltpu.make_async_remote_copy(
                src_ref=ref,
                dst_ref=ref,
                send_sem=sems.at[0],
                recv_sem=sems.at[1],
                device_id={"sp_0": peer},
                device_id_type=MESH,
            )

        later, passed = size - 1 - place, place
        self.sends, self.gets = (later, passed) if way == 0 else (passed, later)
        self.way, self.size, self.place = way, size, place
        peers = [lax.rem(place + k, size) for k in range(1, size)]
        self.copies = [copy(peer, buf.at[place]) for peer in peers]
        self.wholes = [copy(peers[0], buf.at[pl.ds(0, m)]) for m in range(1, size)]

    def start(self):
        for k, c in enumerate(self.copies, 1):
            later = self.place + k < self.size
            pl.when(later if self.way == 0 else jnp.logical_not(later))(c.start)
        return self

    def arrived(self):
        for m, c in enumerate(self.wholes, 1):
            pl.when(self.gets == m)(c.wait_recv)

    def left(self):
        for m, c in enumerate(self.wholes, 1):
            pl.when(self.sends == m)(c.wait_send)


def mixer(
    dims,
    condition_in,
    source_in,
    gain_in,
    out_gain_in,
    conv_x_in,
    conv_b_in,
    conv_c_in,
    rate_in,
    modw_in,
    context,
    latent,
    w_x,
    w_b,
    w_c,
    w_z,
    w_dt,
    w_out,
    update,
    condition,
    source,
    gain,
    out_gain,
    conv_x,
    conv_b,
    conv_c,
    rate,
    modw,
    weights,
    out_weights,
    dt_rows,
    dt_wide,
    small,
    lat,
    ctx,
    placed,
    mod_z,
    mod_y,
    mod_x,
    gate_y,
    gate_z,
    gate_x,
    edge_send,
    edge_recv,
    misc,
    hidden,
    feats,
    moved,
    growth,
    inside,
    ctx_bt,
    ctx_z,
    ctx_dz,
    state_send,
    state_recv,
    decay_y,
    tot_z,
    tot_dz,
    before,
    enter_send,
    enter_recv,
    normed,
    part_send,
    parts,
    local_sem,
    core_send,
    core_recv,
    pair_sems,
    edge_sems,
    edge_got,
    tot_sems,
    last_sems,
):
    nz, ny, nx, model = dims
    width = model // nx
    own_rows = TOKENS // nx
    slab = STATE // ny
    lines = ny * CTX_ROWS
    ctx_at = TOKENS + 16
    z = lax.axis_index("sp_0")
    y = lax.axis_index("sp_1")
    x = lax.axis_index("tp")
    core = lax.axis_index("dp")
    place = z * ny + y
    count = nz * ny

    loads = [
        pltpu.make_async_copy(origin, target, local_sem.at[5 + i])
        for i, (origin, target) in enumerate(
            (
                (modw_in, modw),
                (condition_in, condition),
                (source_in, source),
                (gain_in, gain),
                (out_gain_in, out_gain),
                (conv_x_in, conv_x),
                (conv_b_in, conv_b),
                (conv_c_in, conv_c),
                (rate_in, rate),
                (context, ctx.at[y]),
            )
        )
    ]
    own_latent = pltpu.make_async_copy(latent, lat.at[x], local_sem.at[3])
    for c in loads[:3]:
        c.start()
    own_latent.start()
    barrier = pltpu.get_barrier_semaphore()
    up_place = lax.rem(place + 1, count)
    down_place = lax.rem(place + count - 1, count)
    above = {"sp_0": up_place // ny, "sp_1": lax.rem(up_place, ny)}
    below = {"sp_0": down_place // ny, "sp_1": lax.rem(down_place, ny)}
    peers = [{"sp_1": lax.rem(y + k, ny)} for k in range(1, ny)]
    peers += [{"sp_0": lax.rem(z + k, nz)} for k in range(1, nz)]
    peers += [{"tp": lax.rem(x + k, nx)} for k in range(1, nx)]
    peers += [{"dp": 1 - core}]
    for k in range(nx):
        peers += [dict(above, tp=k), dict(below, tp=k)]
    z_up, z_down = lax.rem(z + 1, nz), lax.rem(z + nz - 1, nz)
    for peer in peers:
        pl.semaphore_signal(barrier, inc=1, device_id=peer, device_id_type=MESH)

    for c in loads[3:]:
        c.start()
    half = model // 2
    own_half = pl.ds(pl.multiple_of(core * half, half), half)
    out_half = pl.ds(pl.multiple_of(core * (INNER // 2), INNER // 2), INNER // 2)
    pieces = (
        (w_dt, dt_rows.at[:, :, own_half]),
        (w_x, weights.at[own_half, pl.ds(0, INNER)]),
        (w_b, weights.at[own_half, pl.ds(COL_B, STATE)]),
        (w_c, weights.at[own_half, pl.ds(COL_C, STATE)]),
        (w_z, weights.at[own_half, pl.ds(COL_Z, INNER)]),
        (w_out, out_weights.at[out_half, :]),
    )
    groups = (0, 1, 1, 1, 1, 2)
    local = [
        pltpu.make_async_copy(origin, target, local_sem.at[i])
        for i, (origin, target) in zip(groups, pieces)
    ]
    in_bulk = weights.at[own_half, pl.ds(0, COLS - LANES)]
    bulk_local = [
        local[0],
        pltpu.make_async_copy(in_bulk, in_bulk, local_sem.at[1]),
        local[-1],
    ]
    def unpack(r, ref):
        piece = ref[...].astype(F32)
        for k in range(piece.shape[0]):
            small[r : r + 1, k * LANES : (k + 1) * LANES] = piece[k : k + 1]

    placed[...] = jnp.zeros_like(placed)
    for c in loads[:3]:
        c.wait()
    unpack(1, source)
    small[0:1, 0:model] = condition[...].astype(F32)

    rows = modw.shape[1]
    chunk = placed.shape[1]
    per = chunk // rows
    at = pl.ds(pl.multiple_of(lax.rem(place, per) * rows, rows), rows)
    placed[:, at, :] = modw[...]
    lane_at = pl.ds(pl.multiple_of((place // per) * chunk, chunk), chunk)
    act = jnp.broadcast_to(rounded(silu(small[0:1, lane_at])), (8, chunk))
    act_ctx = jnp.broadcast_to(rounded(silu(small[1:2, lane_at])), (8, chunk))
    row8 = rows_of((8, chunk))
    partial = jnp.zeros((8, width), F32)
    for k in range(3):
        left = jnp.where(row8 == (0, 1, 4)[k], act, 0.0)
        if k < 2:
            left = jnp.where(row8 == 2 + k, act_ctx, left)
        partial = partial + jnp.dot(
            left.astype(BF16), placed[k], preferred_element_type=F32
        )
    for r in range(4):
        mod_y[y, r] = partial[r : r + 1]
    gate_y[y, 0] = partial[4:5]

    pl.semaphore_wait(barrier, len(peers))
    pairs = iter(range(32))

    def along(axis, size, me, origin, target, bulk):
        return Exchange(axis, size, me, origin, target, pair_sems.at[next(pairs)], bulk)

    def gather(axis, size, me, buf):
        own = buf.at[me]
        return along(axis, size, me, lambda peer: own, own, buf.at[pl.ds(0, size - 1)])

    mods = [
        gather("sp_1", ny, y, mod_y),
        gather("sp_0", nz, z, mod_z),
        gather("tp", nx, x, mod_x),
    ]
    gates = [
        gather("sp_1", ny, y, gate_y),
        gather("sp_0", nz, z, gate_z),
        gather("tp", nx, x, gate_x),
    ]

    def summed(buf, size):
        total = buf[0]
        for k in range(1, size):
            total = total + buf[k]
        return total

    mods[0].start()
    ctx_copies = along(
        "sp_1", ny, y, lambda peer: context, ctx.at[y], ctx.at[pl.ds(0, ny - 1)]
    ).start()
    lat_copies = along(
        "tp", nx, x, lambda peer: latent, lat.at[x], lat.at[pl.ds(0, nx - 1)]
    ).start()
    swaps = [
        pltpu.make_async_remote_copy(
            src_ref=origin,
            dst_ref=target,
            send_sem=core_send.at[i],
            recv_sem=core_recv.at[i],
            device_id={"dp": 1 - core},
            device_id_type=MESH,
        )
        for i, (origin, target) in zip(groups, pieces)
    ]
    bulk_swaps = [
        swaps[0],
        pltpu.make_async_remote_copy(
            src_ref=in_bulk,
            dst_ref=in_bulk,
            send_sem=core_send.at[1],
            recv_sem=core_recv.at[1],
            device_id={"dp": 1 - core},
            device_id_type=MESH,
        ),
        swaps[-1],
    ]
    for c, d in zip(swaps, local):
        c.start()
        d.start()

    def edge(slot, to, bulk):
        def copy(origin, target, peer):
            return pltpu.make_async_remote_copy(
                src_ref=origin,
                dst_ref=target,
                send_sem=edge_sems.at[slot],
                recv_sem=edge_got.at[slot],
                device_id=peer,
                device_id_type=MESH,
            )

        each = [copy(edge_send.at[slot], edge_recv.at[slot], peer) for peer in to]
        return each, None if bulk is None else copy(bulk, bulk, to[0])

    lat_bulk = edge_send.at[pl.ds(0, nx)]
    edges = (
        (x == nx - 1, edge(0, [dict(above, tp=k) for k in range(nx)], lat_bulk)),
        (x == 0, edge(1, [dict(below, tp=k) for k in range(nx)], lat_bulk)),
    )
    ctx_edges = [
        edge(2, [{"sp_0": z_up}], None)[0][0],
        edge(3, [{"sp_0": z_down}], None)[0][0],
    ]
    own_latent.wait()
    for slot, (owner, (each, _)) in enumerate(edges):

        @pl.when(owner)
        def _(slot=slot, each=each):
            held = lat[x].astype(F32)
            at = 0 if slot == 1 else own_rows - 1
            edge_send[slot] = held[at : at + 1, :]
            for c in each:
                c.start()

    gates[0].start()
    small[2:7, :] = jnp.zeros((5, small.shape[1]), F32)
    for c in loads[3:]:
        c.wait()
    unpack(2, gain)
    unpack(3, out_gain)
    small[4:7, 0:INNER] = conv_x[...].astype(F32)
    small[4:7, INNER : INNER + STATE] = conv_b[...].astype(F32)
    small[4:7, INNER + STATE : MIXED] = conv_c[...].astype(F32)
    lane = lanes_of((1, LANES))
    rates = jnp.zeros((1, LANES), F32)
    for way in range(2):
        for h in range(HEADS):
            rates = jnp.where(lane == way * HEADS + h, rate[way : way + 1, h : h + 1], rates)

    mods[0].arrived()
    mod_z[z] = summed(mod_y, ny)
    mods[1].start()

    def inverse(v):
        return lax.rsqrt(jnp.mean(v * v, axis=1, keepdims=True) + EPSILON)

    mods[1].arrived()
    mod_x[x] = summed(mod_z, nz)
    mods[2].start()

    ctx_copies.arrived()
    edge_send[2] = ctx[ny - 1].astype(F32)[CTX_ROWS - 1 : CTX_ROWS, :]
    edge_send[3] = ctx[0].astype(F32)[0:1, :]
    for c in ctx_edges:
        c.start()
    ctx_scales = [inverse(ctx[j].astype(F32)) for j in range(ny)]
    lat_copies.arrived()
    scales = [inverse(lat[t].astype(F32)) for t in range(nx)]
    misc[...] = jnp.zeros_like(misc)
    for c in (edges[0][1][0][0], edges[1][1][0][0], *ctx_edges):
        c.wait_recv()
    has = (place > 0, place < count - 1, z > 0, z < nz - 1)
    for slot in range(4):
        misc[slot : slot + 1, :] = jnp.where(has[slot], edge_recv[slot], 0.0)
    misc_scale = inverse(misc[...])
    row16 = rows_of((16, 1))
    kept = jnp.zeros((16, 1), jnp.bool_)
    for slot in range(4):
        kept = jnp.logical_or(kept, jnp.logical_and(row16 == slot, has[slot]))

    bulk_local[0].wait()
    bulk_swaps[0].wait_recv()
    dt_wide[...] = jnp.zeros_like(dt_wide)
    for way in range(2):
        dt_wide[way * HEADS : (way + 1) * HEADS, :] = dt_rows[way].astype(F32)
    for b in range(model // LANES):
        at = slice(b * LANES, (b + 1) * LANES)
        weights[at, COL_DT:COL_C] = dt_wide[:, at].T.astype(BF16)
    bulk_local[1].wait()
    bulk_swaps[1].wait_recv()

    mods[2].arrived()

    def modulations(c, shift, scale):
        cols = slice(c * width, (c + 1) * width)
        return cols, small[2:3, cols] * (1.0 + mod_x[c, scale]), mod_x[c, shift]

    for c in range(nx):
        cols, scale, shift = modulations(c, 0, 1)
        _, scale_ctx, shift_ctx = modulations(c, 2, 3)
        for t in range(nx):
            value = lat[t, :, cols].astype(F32) * scales[t] * scale + shift
            hidden[t * own_rows : (t + 1) * own_rows, cols] = value.astype(BF16)
        value = misc[:, cols] * misc_scale * jnp.where(row16 < 2, scale, scale_ctx)
        value = value + jnp.where(row16 < 2, shift, shift_ctx)
        hidden[TOKENS:ctx_at, cols] = jnp.where(kept, value, 0.0).astype(BF16)
        for j in range(0, ny, 2):
            two = [
                ctx[i, :, cols].astype(F32) * ctx_scales[i] * scale_ctx + shift_ctx
                for i in (j, j + 1)
            ]
            at = ctx_at + j * CTX_ROWS
            hidden[at : at + 2 * CTX_ROWS, cols] = jnp.concatenate(two, axis=0).astype(BF16)

    def project(rows, left, right):
        while left < right:
            wide = min(256, right - left)
            cols = slice(left, left + wide)
            feats[rows, cols] = rounded(
                jnp.dot(hidden[rows, :], weights[:, cols], preferred_element_type=F32)
            )
            left += wide

    def smooth(rows, low, at, tap_at):
        cols = slice(at, at + LANES)
        feats[rows, cols] = convolved(
            feats[rows, cols],
            feats[low : low + 1, cols],
            feats[low + 1 : low + 2, cols],
            small[4:7, tap_at : tap_at + LANES],
        )

    own = slice(0, TOKENS)
    every = slice(0, ctx_at + lines)
    project(every, COL_B, COL_C)
    project(every, 0, PIECE)
    for at in (COL_B, 0, LANES):
        smooth(own, TOKENS, at, at)
    b_turned = feats[own, COL_B:COL_DT].T.astype(BF16)
    steps = softplus(feats[own, COL_DT:COL_C])
    sums = running_sums(-rates * steps, HEADS)
    ends = jnp.where(lane < HEADS, sums[TOKENS - 1 : TOKENS], sums[0:1])
    for way in range(2):
        for q in range(PAIRS):
            r = way * PAIRS + q
            decay_y[y, r : r + 1, :] = spread(ends, 2 * r)
    decay_copies = gather("sp_1", ny, y, decay_y).start()

    def slabs(axis, size, me, origin, target, piece):
        return along(
            axis,
            size,
            me,
            lambda peer: origin.at[piece, peer],
            target.at[piece, me],
            target.at[piece, pl.ds(0, size - 1)],
        )

    state_copies = []

    def send_states(way, pairs):
        for q in pairs:
            cols = slice(q * LANES, (q + 1) * LANES)
            piece = way * 2 + q // 2
            at = slice(q % 2 * LANES, (q % 2 + 1) * LANES)
            head = way * HEADS + 2 * q
            step = spread(steps, head)
            decay = spread(sums, head)
            end = decay[TOKENS - 1 : TOKENS] if way == 0 else decay[0:1]
            moved_x = rounded(feats[own, cols] * step)
            moved[way * TOKENS : (way + 1) * TOKENS, cols] = moved_x.astype(BF16)
            growth[way, :, cols] = jnp.exp(decay)
            at_end = (moved_x * jnp.exp(end - decay)).astype(BF16)
            state = jnp.dot(b_turned, at_end, preferred_element_type=F32).astype(BF16)
            for p in range(ny):
                state_send[piece, p, :, at] = state[p * slab : (p + 1) * slab]
            if q % 2 == 1:
                state_copies.append(
                    slabs("sp_1", ny, y, state_send, state_recv, piece).start()
                )
                state_recv[piece, y] = state_send[piece, y]

    send_states(0, (0, 1))
    project(every, PIECE, INNER)
    for at in range(PIECE, INNER, LANES):
        smooth(own, TOKENS, at, at)
    send_states(0, (2, 3))

    ctx_rows = slice(ctx_at, ctx_at + lines)
    for at in range(0, COL_DT, LANES):
        smooth(ctx_rows, TOKENS + 2, at, at)
    ctx_bt[...] = feats[ctx_rows, COL_B:COL_DT].T
    ctx_b = ctx_bt[pl.ds(pl.multiple_of(y * slab, slab), slab), :]
    ctx_steps = softplus(feats[ctx_rows, COL_DT:COL_C])
    ctx_sums = running_sums(-rates * ctx_steps, HEADS)
    ctx_ends = jnp.where(lane < HEADS, ctx_sums[lines - 1 : lines], ctx_sums[0:1])
    for r in range(2 * PAIRS):
        ctx_dz[z, r : r + 1, :] = spread(ctx_ends, 2 * r)
    ctx_dz_copies = gather("sp_0", nz, z, ctx_dz).start()
    ctx_copies_z = []
    is_last = z == nz - 1

    def last_copy(ref, peer):
        return pltpu.make_async_remote_copy(
            src_ref=ref,
            dst_ref=ref,
            send_sem=last_sems.at[0],
            recv_sem=last_sems.at[1],
            device_id={"sp_0": peer},
            device_id_type=MESH,
        )

    to_last = last_copy(ctx_z.at[1, z], nz - 1)
    at_last = last_copy(ctx_z.at[1, pl.ds(0, nz - 1)], z_down)

    def send_context(way):
        for q in range(PAIRS):
            cols = slice(q * LANES, (q + 1) * LANES)
            head = way * HEADS + 2 * q
            decay = spread(ctx_sums, head)
            end = decay[lines - 1 : lines] if way == 0 else decay[0:1]
            moved_x = rounded(feats[ctx_rows, cols] * spread(ctx_steps, head))
            ctx_z[way, z, :, cols] = jnp.dot(
                ctx_b,
                moved_x * jnp.exp(end - decay),
                preferred_element_type=F32,
                precision=lax.Precision.HIGHEST,
            ).astype(BF16)
        if way == 0:
            ctx_copies_z.append(gather("sp_0", nz, z, ctx_z.at[0]).start())
        else:
            pl.when(jnp.logical_not(is_last))(to_last.start)

    send_context(0)
    send_context(1)
    send_states(1, (0, 1, 2, 3))
    project(slice(0, ctx_at), COL_C, COL_Z)
    gates[0].arrived()
    gate_z[z] = summed(gate_y, ny)
    gates[1].start()

    smooth(own, TOKENS, COL_C, INNER + STATE)
    c_vals = feats[own, COL_C:COL_Z].astype(BF16)
    project(own, COL_Z, COLS)
    for at in range(COL_Z, COLS, LANES):
        feats[own, at : at + LANES] = silu(feats[own, at : at + LANES])
    scores = jnp.dot(c_vals, b_turned, preferred_element_type=F32)
    turned = sums.T
    square = (TOKENS, TOKENS)
    lower = rows_of(square) >= lanes_of(square)
    upper = rows_of(square) <= lanes_of(square)
    for q in range(PAIRS):
        cols = slice(q * LANES, (q + 1) * LANES)
        halves = []
        for h in (2 * q, 2 * q + 1):
            both = []
            for way, mask in ((0, lower), (1, upper)):
                col = way * HEADS + h
                gap = sums[:, col : col + 1] - turned[col : col + 1, :]
                decayed = scores * jnp.exp(jnp.minimum(gap, 0.0))
                both.append(jnp.where(mask, decayed, 0.0).astype(BF16))
            halves.append(
                jnp.dot(
                    jnp.concatenate(both, axis=1),
                    moved[:, cols],
                    preferred_element_type=F32,
                )
            )
        inside[:, cols] = jnp.where(lanes_of(square) < LANES // 2, halves[0], halves[1])

    decay_copies.arrived()
    decays = [decay_y[j] for j in range(ny)]
    is_fwd = rows_of((8, LANES)) < PAIRS
    ahead = [None] * ny
    acc_f = acc_b = jnp.zeros((8, LANES), F32)
    for j in range(ny):
        ahead[j] = acc_f
        acc_f = acc_f + decays[j]
    for j in reversed(range(ny)):
        ahead[j] = jnp.exp(jnp.where(is_fwd, ahead[j], acc_b))
        acc_b = acc_b + decays[j]
    tot_dz[z] = acc_f
    tot_dz_copies = gather("sp_0", nz, z, tot_dz).start()
    factors = [jnp.exp(d) for d in decays]
    tot_copies = []
    ctx_factors = []
    line_factor = jnp.exp(acc_f)

    def context_start(way, r):
        order = range(nz) if way == 0 else reversed(range(nz))
        at = (r - way * PAIRS) * LANES
        state = jnp.zeros((slab, LANES), F32)
        for j in order:
            fresh = ctx_z[way, j, :, at : at + LANES].astype(F32)
            state = state * ctx_factors[j][r : r + 1] + fresh
        return state

    last_starts = []
    for piece in range(4):
        way = piece // 2
        state_copies[piece].arrived()
        if piece == 2:
            ctx_dz_copies.arrived()
            ctx_factors += [jnp.exp(ctx_dz[j]) for j in range(nz)]
            pl.when(is_last)(at_last.wait_recv)
            for r in range(PAIRS, 2 * PAIRS):
                last_starts.append(jnp.where(is_last, context_start(1, r), 0.0))
        for q in range(2):
            cols = slice(q * LANES, (q + 1) * LANES)
            r = piece * 2 + q
            state = jnp.zeros((slab, LANES), F32)
            for j in range(ny) if way == 0 else reversed(range(ny)):
                before[piece, j, :, cols] = state
                state = state * factors[j][r : r + 1] + state_recv[piece, j, :, cols].astype(F32)
            if way == 1:
                state = state + line_factor[r : r + 1] * last_starts[r - PAIRS]
            tot_z[piece, z, :, cols] = state.astype(BF16)
        tot_copies.append(
            Totals(way, tot_z.at[piece], nz, z, tot_sems.at[piece]).start()
        )

    gates[1].arrived()
    gate_x[x] = summed(gate_z, nz)
    gates[2].start()
    tot_dz_copies.arrived()
    tot_factors = [jnp.exp(tot_dz[j]) for j in range(nz)]
    enter_copies = []
    for piece in range(4):
        way = piece // 2
        order = list(range(nz)) if way == 0 else list(reversed(range(nz)))
        if piece == 0:
            ctx_copies_z[0].arrived()
        starts = [
            context_start(0, r) if way == 0 else last_starts[r - PAIRS]
            for r in (piece * 2, piece * 2 + 1)
        ]
        tot_copies[piece].arrived()
        for q in range(2):
            cols = slice(q * LANES, (q + 1) * LANES)
            r = piece * 2 + q
            state = starts[q]
            for j in order:
                passed = j < z if way == 0 else j > z
                later = state * tot_factors[j][r : r + 1] + tot_z[piece, j, :, cols].astype(F32)
                state = jnp.where(passed, later, state)
            for j in range(ny):
                enter_send[piece, j, :, cols] = (
                    before[piece, j, :, cols] + ahead[j][r : r + 1] * state
                ).astype(BF16)
        enter_copies.append(slabs("sp_1", ny, y, enter_send, enter_recv, piece).start())
        enter_recv[piece, y] = enter_send[piece, y]

    squares = jnp.zeros((TOKENS, 1), F32)
    for piece in range(4):
        way = piece // 2
        enter_copies[piece].arrived()
        carried = jnp.dot(
            c_vals, enter_recv[piece].reshape(STATE, PIECE), preferred_element_type=F32
        )
        for q in range(2):
            at = (piece % 2) * PIECE + q * LANES
            cols = slice(at, at + LANES)
            value = inside[:, cols]
            value = value + growth[way, :, cols] * carried[:, q * LANES : (q + 1) * LANES]
            if way == 1:
                value = value * feats[own, COL_Z + at : COL_Z + at + LANES]
                squares = squares + jnp.sum(value * value, axis=1, keepdims=True)
            inside[:, cols] = value
    scale = lax.rsqrt(squares / INNER + EPSILON)
    for q in range(PAIRS):
        cols = slice(q * LANES, (q + 1) * LANES)
        normed[:, cols] = (inside[:, cols] * scale * small[3:4, cols]).astype(BF16)

    bulk_local[-1].wait()
    bulk_swaps[-1].wait_recv()
    part_copies = []
    for c in range(nx):
        cols = slice(c * width, (c + 1) * width)
        term = jnp.dot(normed[...], out_weights[:, cols], preferred_element_type=F32)
        term = term.astype(BF16)
        for t in range(nx):
            part_send[t, :, cols] = term[t * own_rows : (t + 1) * own_rows]
        part_copies.append(
            along(
                "tp",
                nx,
                x,
                lambda peer, cols=cols: part_send.at[peer, :, cols],
                parts.at[x, :, cols],
                parts.at[pl.ds(0, nx - 1), :, cols],
            ).start()
        )
    parts[x] = part_send[x]
    for e in bulk_swaps + ctx_edges:
        e.wait_send()
    pl.when(jnp.logical_not(is_last))(to_last.wait_send)
    gates[2].arrived()
    for owner, (_, whole) in edges:
        pl.when(owner)(whole.wait_send)

    done = mods + gates + [ctx_copies, lat_copies, decay_copies, ctx_dz_copies, tot_dz_copies]
    done += ctx_copies_z + state_copies + tot_copies + enter_copies
    for e in done + part_copies:
        e.left()
    for c in range(nx):
        cols = slice(c * width, (c + 1) * width)
        part_copies[c].arrived()
        value = parts[0, :, cols].astype(F32)
        for t in range(1, nx):
            value = value + parts[t, :, cols].astype(F32)
        update[:, cols] = (gate_x[c, 0] * value).astype(BF16)


def shards(
    sizes,
    latent,
    condition,
    context,
    context_source,
    mod_weight,
    norm_gain,
    w_x,
    w_b,
    w_c,
    w_z,
    w_dt,
    conv_x,
    conv_b,
    conv_c,
    decay_rate,
    out_gain,
    w_out,
):
    nz, ny, nx = sizes
    model = latent.shape[-1]
    own_rows = latent.shape[1]
    width = model // nx
    slab = STATE // ny
    span = max(model, 1024)
    rows = mod_weight.shape[1]
    lines = ny * CTX_ROWS
    total_rows = TOKENS + 16 + lines
    vmem = pl.BlockSpec(memory_space=pltpu.VMEM)
    hbm = pl.BlockSpec(memory_space=pl.ANY)
    dma = pltpu.SemaphoreType.DMA
    scratch = [
        pltpu.VMEM((1, model), BF16),
        pltpu.VMEM((model // LANES, LANES), BF16),
        pltpu.VMEM((model // LANES, LANES), BF16),
        pltpu.VMEM((INNER // LANES, LANES), BF16),
        pltpu.VMEM((3, INNER), BF16),
        pltpu.VMEM((3, STATE), BF16),
        pltpu.VMEM((3, STATE), BF16),
        pltpu.VMEM((2, HEADS), F32),
        pltpu.VMEM((3, rows, width), BF16),
        pltpu.VMEM((model, COLS), BF16),
        pltpu.VMEM((INNER, model), BF16),
        pltpu.VMEM((2, HEADS, model), BF16),
        pltpu.VMEM((LANES, model), F32),
        pltpu.VMEM((8, span), F32),
        pltpu.VMEM((nx, own_rows, model), BF16),
        pltpu.VMEM((ny, CTX_ROWS, model), BF16),
        pltpu.VMEM((3, max(rows, LANES), width), BF16),
        pltpu.VMEM((nz, 4, 1, width), F32),
        pltpu.VMEM((ny, 4, 1, width), F32),
        pltpu.VMEM((nx, 4, 1, width), F32),
        pltpu.VMEM((ny, 1, 1, width), F32),
        pltpu.VMEM((nz, 1, 1, width), F32),
        pltpu.VMEM((nx, 1, 1, width), F32),
        pltpu.VMEM((4, 1, model), F32),
        pltpu.VMEM((4, 1, model), F32),
        pltpu.VMEM((16, model), F32),
        pltpu.VMEM((total_rows, model), BF16),
        pltpu.VMEM((total_rows, COLS), F32),
        pltpu.VMEM((2 * TOKENS, INNER), BF16),
        pltpu.VMEM((2, TOKENS, INNER), F32),
        pltpu.VMEM((TOKENS, INNER), F32),
        pltpu.VMEM((STATE, lines), F32),
        pltpu.VMEM((2, nz, slab, INNER), BF16),
        pltpu.VMEM((nz, 8, LANES), F32),
        pltpu.VMEM((4, ny, slab, PIECE), BF16),
        pltpu.VMEM((4, ny, slab, PIECE), BF16),
        pltpu.VMEM((ny, 8, LANES), F32),
        pltpu.VMEM((4, nz, slab, PIECE), BF16),
        pltpu.VMEM((nz, 8, LANES), F32),
        pltpu.VMEM((4, ny, slab, PIECE), F32),
        pltpu.VMEM((4, ny, slab, PIECE), BF16),
        pltpu.VMEM((4, ny, slab, PIECE), BF16),
        pltpu.VMEM((TOKENS, INNER), BF16),
        pltpu.VMEM((nx, own_rows, model), BF16),
        pltpu.VMEM((nx, own_rows, model), BF16),
        dma((15,)),
        dma((3,)),
        dma((3,)),
        dma((20 + nx, 2)),
        dma((4,)),
        dma((4,)),
        dma((4, 2)),
        dma((2,)),
    ]
    update = pl.pallas_call(
        functools.partial(mixer, (nz, ny, nx, model)),
        out_shape=pltpu.VMEM((own_rows, model), BF16),
        in_specs=[hbm] * 17,
        out_specs=vmem,
        scratch_shapes=scratch,
        compiler_params=pltpu.CompilerParams(
            collective_id=0, has_side_effects=True, vmem_limit_bytes=56 * 1024 * 1024
        ),
    )(
        condition,
        context_source.reshape(-1, LANES),
        norm_gain.reshape(-1, LANES),
        out_gain.reshape(-1, LANES),
        conv_x,
        conv_b,
        conv_c,
        decay_rate,
        mod_weight,
        context[0],
        latent[0],
        w_x,
        w_b,
        w_c,
        w_z,
        jnp.swapaxes(w_dt, 1, 2),
        w_out,
    )
    return update[None]


def solution(mesh):
    nx = mesh.shape["tp"]
    ny = 8
    nz = mesh.shape["sp"] // ny
    return program(mesh, nz, ny, nx)


def program(mesh, nz, ny, nx):
    torus = Mesh(
        mesh.devices.reshape(nz, ny, nx, mesh.shape["dp"]), ("sp_0", "sp_1", "tp", "dp")
    )
    placed = (
        P("dp", SP_TP, None),
        P("dp", None),
        P("dp", SP, None),
        P(),
        P(None, SP, "tp"),
        P(),
        P("dp", "tp"),
        P("dp", "tp"),
        P("dp", "tp"),
        P("dp", "tp"),
        P(None, "dp", "tp"),
        P(None, "tp"),
        P(None, "tp"),
        P(None, "tp"),
        P(None, "tp"),
        P("tp"),
        P(("tp", "dp"), None),
    )
    return jax.shard_map(
        functools.partial(shards, (nz, ny, nx)),
        mesh=torus,
        in_specs=placed,
        out_specs=P("dp", SP_TP, None),
        check_vma=False,
    )
```

```python
import functools

import jax
import jax.numpy as jnp
from jax import lax
from jax.experimental import pallas as pl
from jax.experimental.pallas import tpu as pltpu
from jax.sharding import Mesh
from jax.sharding import PartitionSpec as P

SP = ("sp_0", "sp_1")
SP_TP = ("sp_0", "sp_1", "tp")
MESH = pl.DeviceIdType.MESH
EPSILON = 1e-06
F32 = jnp.float32
BF16 = jnp.bfloat16
TOKENS = 128
STATE = 128
LANES = 128
HEADS = 8
PAIRS = HEADS // 2
INNER = 512
MIXED = INNER + 2 * STATE
COL_B = INNER
COL_DT = COL_B + STATE
COL_C = COL_DT + LANES
COL_Z = COL_C + STATE
COLS = COL_Z + INNER
PIECE = 2 * LANES
CTX_ROWS = 8


def rounded(v):
    return v.astype(BF16).astype(F32)


def silu(v):
    return v / (1.0 + jnp.exp(-v))


def softplus(v):
    return jnp.maximum(v, 0.0) + jnp.log1p(jnp.exp(-jnp.abs(v)))


def rows_of(shape):
    return lax.broadcasted_iota(jnp.int32, shape, 0)


def lanes_of(shape):
    return lax.broadcasted_iota(jnp.int32, shape, 1)


def running_sums(v, heads):
    n = v.shape[0]
    row = rows_of(v.shape)
    down = up = v
    step = 1
    while step < n:
        down = down + jnp.where(row >= step, pltpu.roll(down, step, 0), 0.0)
        up = up + jnp.where(row < n - step, pltpu.roll(up, n - step, 0), 0.0)
        step *= 2
    return jnp.where(lanes_of(v.shape) < heads, down, up)


def spread(v, head):
    shape = (v.shape[0], LANES)
    left = jnp.broadcast_to(v[:, head : head + 1], shape)
    right = jnp.broadcast_to(v[:, head + 1 : head + 2], shape)
    return jnp.where(lanes_of(shape) < LANES // 2, left, right)


def convolved(mid, low, high, taps):
    n = mid.shape[0]
    row = rows_of(mid.shape)
    before = jnp.where(row == 0, low, pltpu.roll(mid, 1, 0))
    after = jnp.where(row == n - 1, high, pltpu.roll(mid, n - 1, 0))
    summed = before * taps[0:1] + mid * taps[1:2] + after * taps[2:3]
    return rounded(silu(summed))


class Exchange:
    def __init__(self, axis, size, place, source, target, sems, bulk):
        def copy(peer, origin, end):
            return pltpu.make_async_remote_copy(
                src_ref=origin,
                dst_ref=end,
                send_sem=sems.at[0],
                recv_sem=sems.at[1],
                device_id={axis: peer},
                device_id_type=MESH,
            )

        peers = [lax.rem(place + k, size) for k in range(1, size)]
        self.copies = [copy(peer, source(peer), target) for peer in peers]
        self.whole = copy(peers[0], bulk, bulk)

    def start(self):
        for c in self.copies:
            c.start()
        return self

    def arrived(self):
        self.whole.wait_recv()

    def left(self):
        self.whole.wait_send()


class Totals:
    def __init__(self, way, buf, size, place, sems):
        def copy(peer, ref):
            return pltpu.make_async_remote_copy(
                src_ref=ref,
                dst_ref=ref,
                send_sem=sems.at[0],
                recv_sem=sems.at[1],
                device_id={"sp_0": peer},
                device_id_type=MESH,
            )

        later, passed = size - 1 - place, place
        self.sends, self.gets = (later, passed) if way == 0 else (passed, later)
        self.way, self.size, self.place = way, size, place
        peers = [lax.rem(place + k, size) for k in range(1, size)]
        self.copies = [copy(peer, buf.at[place]) for peer in peers]
        self.wholes = [copy(peers[0], buf.at[pl.ds(0, m)]) for m in range(1, size)]

    def start(self):
        for k, c in enumerate(self.copies, 1):
            later = self.place + k < self.size
            pl.when(later if self.way == 0 else jnp.logical_not(later))(c.start)
        return self

    def arrived(self):
        for m, c in enumerate(self.wholes, 1):
            pl.when(self.gets == m)(c.wait_recv)

    def left(self):
        for m, c in enumerate(self.wholes, 1):
            pl.when(self.sends == m)(c.wait_send)


def mixer(
    dims,
    condition_in,
    source_in,
    gain_in,
    out_gain_in,
    conv_x_in,
    conv_b_in,
    conv_c_in,
    rate_in,
    modw_in,
    context,
    latent,
    w_x,
    w_b,
    w_c,
    w_z,
    w_dt,
    w_out,
    update,
    condition,
    source,
    gain,
    out_gain,
    conv_x,
    conv_b,
    conv_c,
    rate,
    modw,
    weights,
    out_weights,
    dt_rows,
    dt_wide,
    small,
    lat,
    ctx,
    placed,
    mod_z,
    mod_y,
    mod_x,
    gate_y,
    gate_z,
    gate_x,
    edge_send,
    edge_recv,
    line_edge,
    misc,
    hidden,
    feats,
    moved,
    growth,
    inside,
    ctx_bt,
    ctx_z,
    ctx_dz,
    state_send,
    state_recv,
    decay_y,
    tot_z,
    tot_dz,
    before,
    enter_send,
    enter_recv,
    normed,
    part_send,
    parts,
    local_sem,
    core_send,
    core_recv,
    pair_sems,
    edge_sems,
    edge_got,
    tot_sems,
    last_sems,
    line_sems,
):
    nz, ny, nx, model = dims
    width = model // nx
    own_rows = TOKENS // nx
    slab = STATE // ny
    lines = ny * CTX_ROWS
    ctx_at = TOKENS + 16
    z = lax.axis_index("sp_0")
    y = lax.axis_index("sp_1")
    x = lax.axis_index("tp")
    core = lax.axis_index("dp")
    place = z * ny + y
    count = nz * ny

    loads = [
        pltpu.make_async_copy(origin, target, local_sem.at[5 + i])
        for i, (origin, target) in enumerate(
            (
                (modw_in, modw),
                (condition_in, condition),
                (source_in, source),
                (gain_in, gain),
                (out_gain_in, out_gain),
                (conv_x_in, conv_x),
                (conv_b_in, conv_b),
                (conv_c_in, conv_c),
                (rate_in, rate),
                (context, ctx.at[y]),
            )
        )
    ]
    own_latent = pltpu.make_async_copy(latent, lat.at[x], local_sem.at[3])
    for c in loads[:3]:
        c.start()
    own_latent.start()
    barrier = pltpu.get_barrier_semaphore()
    up_place = lax.rem(place + 1, count)
    down_place = lax.rem(place + count - 1, count)
    above = {"sp_0": up_place // ny, "sp_1": lax.rem(up_place, ny)}
    below = {"sp_0": down_place // ny, "sp_1": lax.rem(down_place, ny)}
    peers = [{"sp_1": lax.rem(y + k, ny)} for k in range(1, ny)]
    peers += [{"sp_0": lax.rem(z + k, nz)} for k in range(1, nz)]
    peers += [{"tp": lax.rem(x + k, nx)} for k in range(1, nx)]
    peers += [{"dp": 1 - core}]
    for k in range(nx):
        peers += [dict(above, tp=k), dict(below, tp=k)]
    z_down = lax.rem(z + nz - 1, nz)
    for peer in peers:
        pl.semaphore_signal(barrier, inc=1, device_id=peer, device_id_type=MESH)

    for c in loads[3:]:
        c.start()
    half = model // 2
    own_half = pl.ds(pl.multiple_of(core * half, half), half)
    out_half = pl.ds(pl.multiple_of(core * (INNER // 2), INNER // 2), INNER // 2)
    pieces = (
        (w_dt, dt_rows.at[:, :, own_half]),
        (w_x, weights.at[own_half, pl.ds(0, INNER)]),
        (w_b, weights.at[own_half, pl.ds(COL_B, STATE)]),
        (w_c, weights.at[own_half, pl.ds(COL_C, STATE)]),
        (w_z, weights.at[own_half, pl.ds(COL_Z, INNER)]),
        (w_out, out_weights.at[out_half, :]),
    )
    groups = (0, 1, 1, 1, 1, 2)
    local = [
        pltpu.make_async_copy(origin, target, local_sem.at[i])
        for i, (origin, target) in zip(groups, pieces)
    ]
    in_bulk = weights.at[own_half, pl.ds(0, COLS - LANES)]
    bulk_local = [
        local[0],
        pltpu.make_async_copy(in_bulk, in_bulk, local_sem.at[1]),
        local[-1],
    ]
    def unpack(r, ref):
        piece = ref[...].astype(F32)
        for k in range(piece.shape[0]):
            small[r : r + 1, k * LANES : (k + 1) * LANES] = piece[k : k + 1]

    placed[...] = jnp.zeros_like(placed)
    for c in loads[:3]:
        c.wait()
    unpack(1, source)
    small[0:1, 0:model] = condition[...].astype(F32)

    rows = modw.shape[1]
    chunk = placed.shape[1]
    per = chunk // rows
    at = pl.ds(pl.multiple_of(lax.rem(place, per) * rows, rows), rows)
    placed[:, at, :] = modw[...]
    lane_at = pl.ds(pl.multiple_of((place // per) * chunk, chunk), chunk)
    act = jnp.broadcast_to(rounded(silu(small[0:1, lane_at])), (8, chunk))
    act_ctx = jnp.broadcast_to(rounded(silu(small[1:2, lane_at])), (8, chunk))
    row8 = rows_of((8, chunk))
    partial = jnp.zeros((8, width), F32)
    for k in range(3):
        left = jnp.where(row8 == (0, 1, 4)[k], act, 0.0)
        if k < 2:
            left = jnp.where(row8 == 2 + k, act_ctx, left)
        partial = partial + jnp.dot(
            left.astype(BF16), placed[k], preferred_element_type=F32
        )
    for r in range(4):
        mod_y[y, r] = partial[r : r + 1]
    gate_y[y, 0] = partial[4:5]

    pl.semaphore_wait(barrier, len(peers))
    pairs = iter(range(32))

    def along(axis, size, me, origin, target, bulk):
        return Exchange(axis, size, me, origin, target, pair_sems.at[next(pairs)], bulk)

    def gather(axis, size, me, buf):
        own = buf.at[me]
        return along(axis, size, me, lambda peer: own, own, buf.at[pl.ds(0, size - 1)])

    mods = [
        gather("sp_1", ny, y, mod_y),
        gather("sp_0", nz, z, mod_z),
        gather("tp", nx, x, mod_x),
    ]
    gates = [
        gather("sp_1", ny, y, gate_y),
        gather("sp_0", nz, z, gate_z),
        gather("tp", nx, x, gate_x),
    ]

    def summed(buf, size):
        total = buf[0]
        for k in range(1, size):
            total = total + buf[k]
        return total

    mods[0].start()
    ctx_copies = along(
        "sp_1", ny, y, lambda peer: context, ctx.at[y], ctx.at[pl.ds(0, ny - 1)]
    ).start()
    lat_copies = along(
        "tp", nx, x, lambda peer: latent, lat.at[x], lat.at[pl.ds(0, nx - 1)]
    ).start()
    swaps = [
        pltpu.make_async_remote_copy(
            src_ref=origin,
            dst_ref=target,
            send_sem=core_send.at[i],
            recv_sem=core_recv.at[i],
            device_id={"dp": 1 - core},
            device_id_type=MESH,
        )
        for i, (origin, target) in zip(groups, pieces)
    ]
    bulk_swaps = [
        swaps[0],
        pltpu.make_async_remote_copy(
            src_ref=in_bulk,
            dst_ref=in_bulk,
            send_sem=core_send.at[1],
            recv_sem=core_recv.at[1],
            device_id={"dp": 1 - core},
            device_id_type=MESH,
        ),
        swaps[-1],
    ]
    for c, d in zip(swaps, local):
        c.start()
        d.start()

    def edge(slot, to, bulk):
        def copy(origin, target, peer):
            return pltpu.make_async_remote_copy(
                src_ref=origin,
                dst_ref=target,
                send_sem=edge_sems.at[slot],
                recv_sem=edge_got.at[slot],
                device_id=peer,
                device_id_type=MESH,
            )

        each = [copy(edge_send.at[slot], edge_recv.at[slot], peer) for peer in to]
        return each, copy(bulk, bulk, to[0])

    lat_bulk = edge_send.at[pl.ds(0, nx)]
    edges = (
        (x == nx - 1, edge(0, [dict(above, tp=k) for k in range(nx)], lat_bulk)),
        (x == 0, edge(1, [dict(below, tp=k) for k in range(nx)], lat_bulk)),
        (y == ny - 1, edge(2, [above], edge_send.at[2])),
        (y == 0, edge(3, [below], edge_send.at[3])),
    )
    own_latent.wait()
    loads[9].wait()
    for slot, (owner, (each, _)) in enumerate(edges):

        @pl.when(owner)
        def _(slot=slot, each=each):
            held = (lat[x] if slot < 2 else ctx[y]).astype(F32)
            at = 0 if slot % 2 == 1 else held.shape[0] - 1
            edge_send[slot] = held[at : at + 1, :]
            for c in each:
                c.start()

    gates[0].start()
    small[2:7, :] = jnp.zeros((5, small.shape[1]), F32)
    for c in loads[3:9]:
        c.wait()
    unpack(2, gain)
    unpack(3, out_gain)
    small[4:7, 0:INNER] = conv_x[...].astype(F32)
    small[4:7, INNER : INNER + STATE] = conv_b[...].astype(F32)
    small[4:7, INNER + STATE : MIXED] = conv_c[...].astype(F32)
    lane = lanes_of((1, LANES))
    rates = jnp.zeros((1, LANES), F32)
    for way in range(2):
        for h in range(HEADS):
            rates = jnp.where(lane == way * HEADS + h, rate[way : way + 1, h : h + 1], rates)

    line = []
    for slot, owner in ((0, y == 0), (1, y == ny - 1)):

        def line_copy(origin, target, k, slot=slot):
            return pltpu.make_async_remote_copy(
                src_ref=origin,
                dst_ref=target,
                send_sem=line_sems.at[slot, 0],
                recv_sem=line_sems.at[slot, 1],
                device_id={"sp_1": lax.rem(y + k, ny)},
                device_id_type=MESH,
            )

        origin, target = edge_recv.at[2 + slot], line_edge.at[slot]
        each = [line_copy(origin, target, k) for k in range(1, ny)]
        line_bulk = line_edge.at[pl.ds(0, ny - 1)]
        line.append((owner, each[0], line_copy(line_bulk, line_bulk, 1)))

        @pl.when(owner)
        def _(slot=slot, each=each):
            edges[2 + slot][1][0][0].wait_recv()
            line_edge[slot] = edge_recv[2 + slot]
            for c in each:
                c.start()

    mods[0].arrived()
    mod_z[z] = summed(mod_y, ny)
    mods[1].start()

    def inverse(v):
        return lax.rsqrt(jnp.mean(v * v, axis=1, keepdims=True) + EPSILON)

    mods[1].arrived()
    mod_x[x] = summed(mod_z, nz)
    mods[2].start()

    lat_copies.arrived()
    scales = [inverse(lat[t].astype(F32)) for t in range(nx)]
    ctx_copies.arrived()
    ctx_scales = [inverse(ctx[j].astype(F32)) for j in range(ny)]
    misc[...] = jnp.zeros_like(misc)
    for c in (edges[0][1][0][0], edges[1][1][0][0]):
        c.wait_recv()
    for owner, c, _ in line:
        pl.when(jnp.logical_not(owner))(c.wait_recv)
    has = (place > 0, place < count - 1, z > 0, z < nz - 1)
    for slot in range(4):
        edge_row = edge_recv[slot] if slot < 2 else line_edge[slot - 2]
        misc[slot : slot + 1, :] = jnp.where(has[slot], edge_row, 0.0)
    misc_scale = inverse(misc[...])
    row16 = rows_of((16, 1))
    kept = jnp.zeros((16, 1), jnp.bool_)
    for slot in range(4):
        kept = jnp.logical_or(kept, jnp.logical_and(row16 == slot, has[slot]))

    bulk_local[0].wait()
    bulk_swaps[0].wait_recv()
    dt_wide[...] = jnp.zeros_like(dt_wide)
    for way in range(2):
        dt_wide[way * HEADS : (way + 1) * HEADS, :] = dt_rows[way].astype(F32)
    for b in range(model // LANES):
        at = slice(b * LANES, (b + 1) * LANES)
        weights[at, COL_DT:COL_C] = dt_wide[:, at].T.astype(BF16)
    bulk_local[1].wait()
    bulk_swaps[1].wait_recv()

    mods[2].arrived()

    def modulations(c, shift, scale):
        cols = slice(c * width, (c + 1) * width)
        return cols, small[2:3, cols] * (1.0 + mod_x[c, scale]), mod_x[c, shift]

    for c in range(nx):
        cols, scale, shift = modulations(c, 0, 1)
        _, scale_ctx, shift_ctx = modulations(c, 2, 3)
        for t in range(nx):
            value = lat[t, :, cols].astype(F32) * scales[t] * scale + shift
            hidden[t * own_rows : (t + 1) * own_rows, cols] = value.astype(BF16)
        value = misc[:, cols] * misc_scale * jnp.where(row16 < 2, scale, scale_ctx)
        value = value + jnp.where(row16 < 2, shift, shift_ctx)
        hidden[TOKENS:ctx_at, cols] = jnp.where(kept, value, 0.0).astype(BF16)
        for j in range(0, ny, 2):
            two = [
                ctx[i, :, cols].astype(F32) * ctx_scales[i] * scale_ctx + shift_ctx
                for i in (j, j + 1)
            ]
            at = ctx_at + j * CTX_ROWS
            hidden[at : at + 2 * CTX_ROWS, cols] = jnp.concatenate(two, axis=0).astype(BF16)

    def project(rows, left, right):
        while left < right:
            wide = min(256, right - left)
            cols = slice(left, left + wide)
            feats[rows, cols] = rounded(
                jnp.dot(hidden[rows, :], weights[:, cols], preferred_element_type=F32)
            )
            left += wide

    def smooth(rows, low, at, tap_at):
        cols = slice(at, at + LANES)
        feats[rows, cols] = convolved(
            feats[rows, cols],
            feats[low : low + 1, cols],
            feats[low + 1 : low + 2, cols],
            small[4:7, tap_at : tap_at + LANES],
        )

    own = slice(0, TOKENS)
    every = slice(0, ctx_at + lines)
    project(every, COL_B, COL_C)
    project(every, 0, PIECE)
    for at in (COL_B, 0, LANES):
        smooth(own, TOKENS, at, at)
    b_turned = feats[own, COL_B:COL_DT].T.astype(BF16)
    steps = softplus(feats[own, COL_DT:COL_C])
    sums = running_sums(-rates * steps, HEADS)
    ends = jnp.where(lane < HEADS, sums[TOKENS - 1 : TOKENS], sums[0:1])
    for way in range(2):
        for q in range(PAIRS):
            r = way * PAIRS + q
            decay_y[y, r : r + 1, :] = spread(ends, 2 * r)
    decay_copies = gather("sp_1", ny, y, decay_y).start()

    def slabs(axis, size, me, origin, target, piece):
        return along(
            axis,
            size,
            me,
            lambda peer: origin.at[piece, peer],
            target.at[piece, me],
            target.at[piece, pl.ds(0, size - 1)],
        )

    state_copies = []

    def send_states(way, pairs):
        for q in pairs:
            cols = slice(q * LANES, (q + 1) * LANES)
            piece = way * 2 + q // 2
            at = slice(q % 2 * LANES, (q % 2 + 1) * LANES)
            head = way * HEADS + 2 * q
            step = spread(steps, head)
            decay = spread(sums, head)
            end = decay[TOKENS - 1 : TOKENS] if way == 0 else decay[0:1]
            moved_x = rounded(feats[own, cols] * step)
            moved[way * TOKENS : (way + 1) * TOKENS, cols] = moved_x.astype(BF16)
            growth[way, :, cols] = jnp.exp(decay)
            at_end = (moved_x * jnp.exp(end - decay)).astype(BF16)
            state = jnp.dot(b_turned, at_end, preferred_element_type=F32).astype(BF16)
            for p in range(ny):
                state_send[piece, p, :, at] = state[p * slab : (p + 1) * slab]
            if q % 2 == 1:
                state_copies.append(
                    slabs("sp_1", ny, y, state_send, state_recv, piece).start()
                )
                state_recv[piece, y] = state_send[piece, y]

    send_states(0, (0, 1))
    project(every, PIECE, INNER)
    for at in range(PIECE, INNER, LANES):
        smooth(own, TOKENS, at, at)
    send_states(0, (2, 3))

    ctx_rows = slice(ctx_at, ctx_at + lines)
    for at in range(0, COL_DT, LANES):
        smooth(ctx_rows, TOKENS + 2, at, at)
    ctx_bt[...] = feats[ctx_rows, COL_B:COL_DT].T
    ctx_b = ctx_bt[pl.ds(pl.multiple_of(y * slab, slab), slab), :]
    ctx_steps = softplus(feats[ctx_rows, COL_DT:COL_C])
    ctx_sums = running_sums(-rates * ctx_steps, HEADS)
    ctx_ends = jnp.where(lane < HEADS, ctx_sums[lines - 1 : lines], ctx_sums[0:1])
    for r in range(2 * PAIRS):
        ctx_dz[z, r : r + 1, :] = spread(ctx_ends, 2 * r)
    ctx_dz_copies = gather("sp_0", nz, z, ctx_dz).start()
    ctx_copies_z = []
    is_last = z == nz - 1

    def last_copy(ref, peer):
        return pltpu.make_async_remote_copy(
            src_ref=ref,
            dst_ref=ref,
            send_sem=last_sems.at[0],
            recv_sem=last_sems.at[1],
            device_id={"sp_0": peer},
            device_id_type=MESH,
        )

    to_last = last_copy(ctx_z.at[1, z], nz - 1)
    at_last = last_copy(ctx_z.at[1, pl.ds(0, nz - 1)], z_down)

    def send_context(way):
        for q in range(PAIRS):
            cols = slice(q * LANES, (q + 1) * LANES)
            head = way * HEADS + 2 * q
            decay = spread(ctx_sums, head)
            end = decay[lines - 1 : lines] if way == 0 else decay[0:1]
            moved_x = rounded(feats[ctx_rows, cols] * spread(ctx_steps, head))
            ctx_z[way, z, :, cols] = jnp.dot(
                ctx_b,
                moved_x * jnp.exp(end - decay),
                preferred_element_type=F32,
                precision=lax.Precision.HIGHEST,
            ).astype(BF16)
        if way == 0:
            ctx_copies_z.append(gather("sp_0", nz, z, ctx_z.at[0]).start())
        else:
            pl.when(jnp.logical_not(is_last))(to_last.start)

    send_context(0)
    send_context(1)
    send_states(1, (0, 1, 2, 3))
    project(slice(0, ctx_at), COL_C, COL_Z)
    gates[0].arrived()
    gate_z[z] = summed(gate_y, ny)
    gates[1].start()

    smooth(own, TOKENS, COL_C, INNER + STATE)
    c_vals = feats[own, COL_C:COL_Z].astype(BF16)
    project(own, COL_Z, COLS)
    for at in range(COL_Z, COLS, LANES):
        feats[own, at : at + LANES] = silu(feats[own, at : at + LANES])
    scores = jnp.dot(c_vals, b_turned, preferred_element_type=F32)
    turned = sums.T
    square = (TOKENS, TOKENS)
    lower = rows_of(square) >= lanes_of(square)
    upper = rows_of(square) <= lanes_of(square)
    for q in range(PAIRS):
        cols = slice(q * LANES, (q + 1) * LANES)
        halves = []
        for h in (2 * q, 2 * q + 1):
            both = []
            for way, mask in ((0, lower), (1, upper)):
                col = way * HEADS + h
                gap = sums[:, col : col + 1] - turned[col : col + 1, :]
                decayed = scores * jnp.exp(jnp.minimum(gap, 0.0))
                both.append(jnp.where(mask, decayed, 0.0).astype(BF16))
            halves.append(
                jnp.dot(
                    jnp.concatenate(both, axis=1),
                    moved[:, cols],
                    preferred_element_type=F32,
                )
            )
        inside[:, cols] = jnp.where(lanes_of(square) < LANES // 2, halves[0], halves[1])

    decay_copies.arrived()
    decays = [decay_y[j] for j in range(ny)]
    is_fwd = rows_of((8, LANES)) < PAIRS
    ahead = [None] * ny
    acc_f = acc_b = jnp.zeros((8, LANES), F32)
    for j in range(ny):
        ahead[j] = acc_f
        acc_f = acc_f + decays[j]
    for j in reversed(range(ny)):
        ahead[j] = jnp.exp(jnp.where(is_fwd, ahead[j], acc_b))
        acc_b = acc_b + decays[j]
    tot_dz[z] = acc_f
    tot_dz_copies = gather("sp_0", nz, z, tot_dz).start()
    factors = [jnp.exp(d) for d in decays]
    tot_copies = []
    ctx_factors = []
    line_factor = jnp.exp(acc_f)

    def context_start(way, r):
        order = range(nz) if way == 0 else reversed(range(nz))
        at = (r - way * PAIRS) * LANES
        state = jnp.zeros((slab, LANES), F32)
        for j in order:
            fresh = ctx_z[way, j, :, at : at + LANES].astype(F32)
            state = state * ctx_factors[j][r : r + 1] + fresh
        return state

    last_starts = []
    for piece in range(4):
        way = piece // 2
        state_copies[piece].arrived()
        if piece == 2:
            ctx_dz_copies.arrived()
            ctx_factors += [jnp.exp(ctx_dz[j]) for j in range(nz)]
            pl.when(is_last)(at_last.wait_recv)
            for r in range(PAIRS, 2 * PAIRS):
                last_starts.append(jnp.where(is_last, context_start(1, r), 0.0))
        for q in range(2):
            cols = slice(q * LANES, (q + 1) * LANES)
            r = piece * 2 + q
            state = jnp.zeros((slab, LANES), F32)
            for j in range(ny) if way == 0 else reversed(range(ny)):
                before[piece, j, :, cols] = state
                state = state * factors[j][r : r + 1] + state_recv[piece, j, :, cols].astype(F32)
            if way == 1:
                state = state + line_factor[r : r + 1] * last_starts[r - PAIRS]
            tot_z[piece, z, :, cols] = state.astype(BF16)
        tot_copies.append(
            Totals(way, tot_z.at[piece], nz, z, tot_sems.at[piece]).start()
        )

    gates[1].arrived()
    gate_x[x] = summed(gate_z, nz)
    gates[2].start()
    tot_dz_copies.arrived()
    tot_factors = [jnp.exp(tot_dz[j]) for j in range(nz)]
    enter_copies = []
    for piece in range(4):
        way = piece // 2
        order = list(range(nz)) if way == 0 else list(reversed(range(nz)))
        if piece == 0:
            ctx_copies_z[0].arrived()
        starts = [
            context_start(0, r) if way == 0 else last_starts[r - PAIRS]
            for r in (piece * 2, piece * 2 + 1)
        ]
        tot_copies[piece].arrived()
        for q in range(2):
            cols = slice(q * LANES, (q + 1) * LANES)
            r = piece * 2 + q
            state = starts[q]
            for j in order:
                passed = j < z if way == 0 else j > z
                later = state * tot_factors[j][r : r + 1] + tot_z[piece, j, :, cols].astype(F32)
                state = jnp.where(passed, later, state)
            for j in range(ny):
                enter_send[piece, j, :, cols] = (
                    before[piece, j, :, cols] + ahead[j][r : r + 1] * state
                ).astype(BF16)
        enter_copies.append(slabs("sp_1", ny, y, enter_send, enter_recv, piece).start())
        enter_recv[piece, y] = enter_send[piece, y]

    squares = jnp.zeros((TOKENS, 1), F32)
    for piece in range(4):
        way = piece // 2
        enter_copies[piece].arrived()
        carried = jnp.dot(
            c_vals, enter_recv[piece].reshape(STATE, PIECE), preferred_element_type=F32
        )
        for q in range(2):
            at = (piece % 2) * PIECE + q * LANES
            cols = slice(at, at + LANES)
            value = inside[:, cols]
            value = value + growth[way, :, cols] * carried[:, q * LANES : (q + 1) * LANES]
            if way == 1:
                value = value * feats[own, COL_Z + at : COL_Z + at + LANES]
                squares = squares + jnp.sum(value * value, axis=1, keepdims=True)
            inside[:, cols] = value
    scale = lax.rsqrt(squares / INNER + EPSILON)
    for q in range(PAIRS):
        cols = slice(q * LANES, (q + 1) * LANES)
        normed[:, cols] = (inside[:, cols] * scale * small[3:4, cols]).astype(BF16)

    bulk_local[-1].wait()
    bulk_swaps[-1].wait_recv()
    part_copies = []
    for c in range(nx):
        cols = slice(c * width, (c + 1) * width)
        term = jnp.dot(normed[...], out_weights[:, cols], preferred_element_type=F32)
        term = term.astype(BF16)
        for t in range(nx):
            part_send[t, :, cols] = term[t * own_rows : (t + 1) * own_rows]
        part_copies.append(
            along(
                "tp",
                nx,
                x,
                lambda peer, cols=cols: part_send.at[peer, :, cols],
                parts.at[x, :, cols],
                parts.at[pl.ds(0, nx - 1), :, cols],
            ).start()
        )
    parts[x] = part_send[x]
    for owner, _, whole in line:
        pl.when(owner)(whole.wait_send)
    for e in bulk_swaps:
        e.wait_send()
    pl.when(jnp.logical_not(is_last))(to_last.wait_send)
    gates[2].arrived()
    for owner, (_, whole) in edges:
        pl.when(owner)(whole.wait_send)

    done = mods + gates + [ctx_copies, lat_copies, decay_copies, ctx_dz_copies, tot_dz_copies]
    done += ctx_copies_z + state_copies + tot_copies + enter_copies
    for e in done + part_copies:
        e.left()
    for c in range(nx):
        cols = slice(c * width, (c + 1) * width)
        part_copies[c].arrived()
        value = parts[0, :, cols].astype(F32)
        for t in range(1, nx):
            value = value + parts[t, :, cols].astype(F32)
        update[:, cols] = (gate_x[c, 0] * value).astype(BF16)


def shards(
    sizes,
    latent,
    condition,
    context,
    context_source,
    mod_weight,
    norm_gain,
    w_x,
    w_b,
    w_c,
    w_z,
    w_dt,
    conv_x,
    conv_b,
    conv_c,
    decay_rate,
    out_gain,
    w_out,
):
    nz, ny, nx = sizes
    model = latent.shape[-1]
    own_rows = latent.shape[1]
    width = model // nx
    slab = STATE // ny
    span = max(model, 1024)
    rows = mod_weight.shape[1]
    lines = ny * CTX_ROWS
    total_rows = TOKENS + 16 + lines
    vmem = pl.BlockSpec(memory_space=pltpu.VMEM)
    hbm = pl.BlockSpec(memory_space=pl.ANY)
    dma = pltpu.SemaphoreType.DMA
    scratch = [
        pltpu.VMEM((1, model), BF16),
        pltpu.VMEM((model // LANES, LANES), BF16),
        pltpu.VMEM((model // LANES, LANES), BF16),
        pltpu.VMEM((INNER // LANES, LANES), BF16),
        pltpu.VMEM((3, INNER), BF16),
        pltpu.VMEM((3, STATE), BF16),
        pltpu.VMEM((3, STATE), BF16),
        pltpu.VMEM((2, HEADS), F32),
        pltpu.VMEM((3, rows, width), BF16),
        pltpu.VMEM((model, COLS), BF16),
        pltpu.VMEM((INNER, model), BF16),
        pltpu.VMEM((2, HEADS, model), BF16),
        pltpu.VMEM((LANES, model), F32),
        pltpu.VMEM((8, span), F32),
        pltpu.VMEM((nx, own_rows, model), BF16),
        pltpu.VMEM((ny, CTX_ROWS, model), BF16),
        pltpu.VMEM((3, max(rows, LANES), width), BF16),
        pltpu.VMEM((nz, 4, 1, width), F32),
        pltpu.VMEM((ny, 4, 1, width), F32),
        pltpu.VMEM((nx, 4, 1, width), F32),
        pltpu.VMEM((ny, 1, 1, width), F32),
        pltpu.VMEM((nz, 1, 1, width), F32),
        pltpu.VMEM((nx, 1, 1, width), F32),
        pltpu.VMEM((4, 1, model), F32),
        pltpu.VMEM((4, 1, model), F32),
        pltpu.VMEM((ny, 1, model), F32),
        pltpu.VMEM((16, model), F32),
        pltpu.VMEM((total_rows, model), BF16),
        pltpu.VMEM((total_rows, COLS), F32),
        pltpu.VMEM((2 * TOKENS, INNER), BF16),
        pltpu.VMEM((2, TOKENS, INNER), F32),
        pltpu.VMEM((TOKENS, INNER), F32),
        pltpu.VMEM((STATE, lines), F32),
        pltpu.VMEM((2, nz, slab, INNER), BF16),
        pltpu.VMEM((nz, 8, LANES), F32),
        pltpu.VMEM((4, ny, slab, PIECE), BF16),
        pltpu.VMEM((4, ny, slab, PIECE), BF16),
        pltpu.VMEM((ny, 8, LANES), F32),
        pltpu.VMEM((4, nz, slab, PIECE), BF16),
        pltpu.VMEM((nz, 8, LANES), F32),
        pltpu.VMEM((4, ny, slab, PIECE), F32),
        pltpu.VMEM((4, ny, slab, PIECE), BF16),
        pltpu.VMEM((4, ny, slab, PIECE), BF16),
        pltpu.VMEM((TOKENS, INNER), BF16),
        pltpu.VMEM((nx, own_rows, model), BF16),
        pltpu.VMEM((nx, own_rows, model), BF16),
        dma((15,)),
        dma((3,)),
        dma((3,)),
        dma((20 + nx, 2)),
        dma((4,)),
        dma((4,)),
        dma((4, 2)),
        dma((2,)),
        dma((2, 2)),
    ]
    update = pl.pallas_call(
        functools.partial(mixer, (nz, ny, nx, model)),
        out_shape=pltpu.VMEM((own_rows, model), BF16),
        in_specs=[hbm] * 17,
        out_specs=vmem,
        scratch_shapes=scratch,
        compiler_params=pltpu.CompilerParams(
            collective_id=0, has_side_effects=True, vmem_limit_bytes=56 * 1024 * 1024
        ),
    )(
        condition,
        context_source.reshape(-1, LANES),
        norm_gain.reshape(-1, LANES),
        out_gain.reshape(-1, LANES),
        conv_x,
        conv_b,
        conv_c,
        decay_rate,
        mod_weight,
        context[0],
        latent[0],
        w_x,
        w_b,
        w_c,
        w_z,
        jnp.swapaxes(w_dt, 1, 2),
        w_out,
    )
    return update[None]


def solution(mesh):
    nx = mesh.shape["tp"]
    ny = 8
    nz = mesh.shape["sp"] // ny
    return program(mesh, nz, ny, nx)


def program(mesh, nz, ny, nx):
    torus = Mesh(
        mesh.devices.reshape(nz, ny, nx, mesh.shape["dp"]), ("sp_0", "sp_1", "tp", "dp")
    )
    placed = (
        P("dp", SP_TP, None),
        P("dp", None),
        P("dp", SP, None),
        P(),
        P(None, SP, "tp"),
        P(),
        P("dp", "tp"),
        P("dp", "tp"),
        P("dp", "tp"),
        P("dp", "tp"),
        P(None, "dp", "tp"),
        P(None, "tp"),
        P(None, "tp"),
        P(None, "tp"),
        P(None, "tp"),
        P("tp"),
        P(("tp", "dp"), None),
    )
    return jax.shard_map(
        functools.partial(shards, (nz, ny, nx)),
        mesh=torus,
        in_specs=placed,
        out_specs=P("dp", SP_TP, None),
        check_vma=False,
    )
```

```python
import functools

import jax
import jax.numpy as jnp
from jax import lax
from jax.experimental import pallas as pl
from jax.experimental.pallas import tpu as pltpu
from jax.sharding import Mesh
from jax.sharding import PartitionSpec as P

SP = ("sp_0", "sp_1")
SP_TP = ("sp_0", "sp_1", "tp")
MESH = pl.DeviceIdType.MESH
EPSILON = 1e-06
F32 = jnp.float32
BF16 = jnp.bfloat16
TOKENS = 128
STATE = 128
LANES = 128
HEADS = 8
PAIRS = HEADS // 2
INNER = 512
MIXED = INNER + 2 * STATE
COL_B = INNER
COL_DT = COL_B + STATE
COL_C = COL_DT + LANES
COL_Z = COL_C + STATE
COLS = COL_Z + INNER
PIECE = 2 * LANES
CTX_ROWS = 8


def rounded(v):
    return v.astype(BF16).astype(F32)


def silu(v):
    return v / (1.0 + jnp.exp(-v))


def softplus(v):
    return jnp.maximum(v, 0.0) + jnp.log1p(jnp.exp(-jnp.abs(v)))


def rows_of(shape):
    return lax.broadcasted_iota(jnp.int32, shape, 0)


def lanes_of(shape):
    return lax.broadcasted_iota(jnp.int32, shape, 1)


def running_sums(v, heads):
    n = v.shape[0]
    row = rows_of(v.shape)
    down = up = v
    step = 1
    while step < n:
        down = down + jnp.where(row >= step, pltpu.roll(down, step, 0), 0.0)
        up = up + jnp.where(row < n - step, pltpu.roll(up, n - step, 0), 0.0)
        step *= 2
    return jnp.where(lanes_of(v.shape) < heads, down, up)


def spread(v, head):
    shape = (v.shape[0], LANES)
    left = jnp.broadcast_to(v[:, head : head + 1], shape)
    right = jnp.broadcast_to(v[:, head + 1 : head + 2], shape)
    return jnp.where(lanes_of(shape) < LANES // 2, left, right)


def convolved(mid, low, high, taps):
    n = mid.shape[0]
    row = rows_of(mid.shape)
    before = jnp.where(row == 0, low, pltpu.roll(mid, 1, 0))
    after = jnp.where(row == n - 1, high, pltpu.roll(mid, n - 1, 0))
    summed = before * taps[0:1] + mid * taps[1:2] + after * taps[2:3]
    return rounded(silu(summed))


class Exchange:
    def __init__(self, axis, size, place, source, target, sems, bulk):
        def copy(peer, origin, end):
            return pltpu.make_async_remote_copy(
                src_ref=origin,
                dst_ref=end,
                send_sem=sems.at[0],
                recv_sem=sems.at[1],
                device_id={axis: peer},
                device_id_type=MESH,
            )

        peers = [lax.rem(place + k, size) for k in range(1, size)]
        self.copies = [copy(peer, source(peer), target) for peer in peers]
        self.whole = copy(peers[0], bulk, bulk)

    def start(self):
        for c in self.copies:
            c.start()
        return self

    def arrived(self):
        self.whole.wait_recv()

    def left(self):
        self.whole.wait_send()


class Totals:
    def __init__(self, way, buf, size, place, sems):
        def copy(peer, ref):
            return pltpu.make_async_remote_copy(
                src_ref=ref,
                dst_ref=ref,
                send_sem=sems.at[0],
                recv_sem=sems.at[1],
                device_id={"sp_0": peer},
                device_id_type=MESH,
            )

        later, passed = size - 1 - place, place
        self.sends, self.gets = (later, passed) if way == 0 else (passed, later)
        self.way, self.size, self.place = way, size, place
        peers = [lax.rem(place + k, size) for k in range(1, size)]
        self.copies = [copy(peer, buf.at[place]) for peer in peers]
        self.wholes = [copy(peers[0], buf.at[pl.ds(0, m)]) for m in range(1, size)]

    def start(self):
        for k, c in enumerate(self.copies, 1):
            later = self.place + k < self.size
            pl.when(later if self.way == 0 else jnp.logical_not(later))(c.start)
        return self

    def arrived(self):
        for m, c in enumerate(self.wholes, 1):
            pl.when(self.gets == m)(c.wait_recv)

    def left(self):
        for m, c in enumerate(self.wholes, 1):
            pl.when(self.sends == m)(c.wait_send)


def mixer(
    dims,
    condition_in,
    source_in,
    gain_in,
    out_gain_in,
    conv_x_in,
    conv_b_in,
    conv_c_in,
    rate_in,
    modw_in,
    context,
    latent,
    w_x,
    w_b,
    w_c,
    w_z,
    w_dt,
    w_out,
    update,
    condition,
    source,
    gain,
    out_gain,
    conv_x,
    conv_b,
    conv_c,
    rate,
    modw,
    weights,
    out_weights,
    dt_rows,
    dt_wide,
    small,
    lat,
    ctx,
    placed,
    mod_z,
    mod_y,
    mod_x,
    gate_y,
    gate_z,
    gate_x,
    edge_send,
    edge_recv,
    line_edge,
    misc,
    hidden,
    feats,
    moved,
    growth,
    inside,
    ctx_bt,
    ctx_z,
    ctx_dz,
    state_send,
    state_recv,
    decay_y,
    tot_z,
    tot_dz,
    before,
    enter_send,
    enter_recv,
    normed,
    part_send,
    parts,
    local_sem,
    core_send,
    core_recv,
    pair_sems,
    edge_sems,
    edge_got,
    tot_sems,
    last_sems,
    line_sems,
):
    nz, ny, nx, model = dims
    width = model // nx
    own_rows = TOKENS // nx
    slab = STATE // ny
    lines = ny * CTX_ROWS
    ctx_at = TOKENS + 16
    z = lax.axis_index("sp_0")
    y = lax.axis_index("sp_1")
    x = lax.axis_index("tp")
    core = lax.axis_index("dp")
    place = z * ny + y
    count = nz * ny

    loads = [
        pltpu.make_async_copy(origin, target, local_sem.at[5 + i])
        for i, (origin, target) in enumerate(
            (
                (modw_in, modw),
                (condition_in, condition),
                (source_in, source),
                (gain_in, gain),
                (out_gain_in, out_gain),
                (conv_x_in, conv_x),
                (conv_b_in, conv_b),
                (conv_c_in, conv_c),
                (rate_in, rate),
                (context, ctx.at[y]),
            )
        )
    ]
    own_latent = pltpu.make_async_copy(latent, lat.at[x], local_sem.at[3])
    for c in loads[:3]:
        c.start()
    own_latent.start()
    barrier = pltpu.get_barrier_semaphore()
    up_place = lax.rem(place + 1, count)
    down_place = lax.rem(place + count - 1, count)
    above = {"sp_0": up_place // ny, "sp_1": lax.rem(up_place, ny)}
    below = {"sp_0": down_place // ny, "sp_1": lax.rem(down_place, ny)}
    peers = [{"sp_1": lax.rem(y + k, ny)} for k in range(1, ny)]
    peers += [{"sp_0": lax.rem(z + k, nz)} for k in range(1, nz)]
    peers += [{"tp": lax.rem(x + k, nx)} for k in range(1, nx)]
    peers += [{"dp": 1 - core}]
    for k in range(nx):
        peers += [dict(above, tp=k), dict(below, tp=k)]
    z_down = lax.rem(z + nz - 1, nz)
    for peer in peers:
        pl.semaphore_signal(barrier, inc=1, device_id=peer, device_id_type=MESH)

    for c in loads[3:]:
        c.start()
    half = model // 2
    own_half = pl.ds(pl.multiple_of(core * half, half), half)
    out_half = pl.ds(pl.multiple_of(core * (INNER // 2), INNER // 2), INNER // 2)
    pieces = (
        (w_dt, dt_rows.at[:, :, own_half]),
        (w_x, weights.at[own_half, pl.ds(0, INNER)]),
        (w_b, weights.at[own_half, pl.ds(COL_B, STATE)]),
        (w_c, weights.at[own_half, pl.ds(COL_C, STATE)]),
        (w_z, weights.at[own_half, pl.ds(COL_Z, INNER)]),
        (w_out, out_weights.at[out_half, :]),
    )
    groups = (0, 1, 1, 1, 1, 2)
    local = [
        pltpu.make_async_copy(origin, target, local_sem.at[i])
        for i, (origin, target) in zip(groups, pieces)
    ]
    in_bulk = weights.at[own_half, pl.ds(0, COLS - LANES)]
    bulk_local = [
        local[0],
        pltpu.make_async_copy(in_bulk, in_bulk, local_sem.at[1]),
        local[-1],
    ]
    def unpack(r, ref):
        piece = ref[...].astype(F32)
        for k in range(piece.shape[0]):
            small[r : r + 1, k * LANES : (k + 1) * LANES] = piece[k : k + 1]

    placed[...] = jnp.zeros_like(placed)
    for c in loads[:3]:
        c.wait()
    unpack(1, source)
    small[0:1, 0:model] = condition[...].astype(F32)

    rows = modw.shape[1]
    chunk = placed.shape[1]
    per = chunk // rows
    at = pl.ds(pl.multiple_of(lax.rem(place, per) * rows, rows), rows)
    placed[:, at, :] = modw[...]
    lane_at = pl.ds(pl.multiple_of((place // per) * chunk, chunk), chunk)
    act = jnp.broadcast_to(rounded(silu(small[0:1, lane_at])), (8, chunk))
    act_ctx = jnp.broadcast_to(rounded(silu(small[1:2, lane_at])), (8, chunk))
    row8 = rows_of((8, chunk))
    partial = jnp.zeros((8, width), F32)
    for k in range(3):
        left = jnp.where(row8 == (0, 1, 4)[k], act, 0.0)
        if k < 2:
            left = jnp.where(row8 == 2 + k, act_ctx, left)
        partial = partial + jnp.dot(
            left.astype(BF16), placed[k], preferred_element_type=F32
        )
    for r in range(4):
        mod_y[y, r] = partial[r : r + 1]
    gate_y[y, 0] = partial[4:5]

    pl.semaphore_wait(barrier, len(peers))
    pairs = iter(range(32))

    def along(axis, size, me, origin, target, bulk):
        return Exchange(axis, size, me, origin, target, pair_sems.at[next(pairs)], bulk)

    def gather(axis, size, me, buf):
        own = buf.at[me]
        return along(axis, size, me, lambda peer: own, own, buf.at[pl.ds(0, size - 1)])

    mods = [
        gather("sp_1", ny, y, mod_y),
        gather("sp_0", nz, z, mod_z),
        gather("tp", nx, x, mod_x),
    ]
    gates = [
        gather("sp_1", ny, y, gate_y),
        gather("sp_0", nz, z, gate_z),
        gather("tp", nx, x, gate_x),
    ]

    def summed(buf, size):
        total = buf[0]
        for k in range(1, size):
            total = total + buf[k]
        return total

    mods[0].start()

    def edge(slot, to, bulk):
        def copy(origin, target, peer):
            return pltpu.make_async_remote_copy(
                src_ref=origin,
                dst_ref=target,
                send_sem=edge_sems.at[slot],
                recv_sem=edge_got.at[slot],
                device_id=peer,
                device_id_type=MESH,
            )

        each = [copy(edge_send.at[slot], edge_recv.at[slot], peer) for peer in to]
        return each, copy(bulk, bulk, to[0])

    lat_bulk = edge_send.at[pl.ds(0, nx)]
    edges = (
        (x == nx - 1, edge(0, [dict(above, tp=k) for k in range(nx)], lat_bulk)),
        (x == 0, edge(1, [dict(below, tp=k) for k in range(nx)], lat_bulk)),
        (y == ny - 1, edge(2, [above], edge_send.at[2])),
        (y == 0, edge(3, [below], edge_send.at[3])),
    )
    own_latent.wait()
    loads[9].wait()
    for slot, (owner, (each, _)) in enumerate(edges):

        @pl.when(owner)
        def _(slot=slot, each=each):
            held = (lat[x] if slot < 2 else ctx[y]).astype(F32)
            at = 0 if slot % 2 == 1 else held.shape[0] - 1
            edge_send[slot] = held[at : at + 1, :]
            for c in each:
                c.start()

    ctx_copies = along(
        "sp_1", ny, y, lambda peer: context, ctx.at[y], ctx.at[pl.ds(0, ny - 1)]
    ).start()
    lat_copies = along(
        "tp", nx, x, lambda peer: latent, lat.at[x], lat.at[pl.ds(0, nx - 1)]
    ).start()
    swaps = [
        pltpu.make_async_remote_copy(
            src_ref=origin,
            dst_ref=target,
            send_sem=core_send.at[i],
            recv_sem=core_recv.at[i],
            device_id={"dp": 1 - core},
            device_id_type=MESH,
        )
        for i, (origin, target) in zip(groups, pieces)
    ]
    bulk_swaps = [
        swaps[0],
        pltpu.make_async_remote_copy(
            src_ref=in_bulk,
            dst_ref=in_bulk,
            send_sem=core_send.at[1],
            recv_sem=core_recv.at[1],
            device_id={"dp": 1 - core},
            device_id_type=MESH,
        ),
        swaps[-1],
    ]
    for c, d in zip(swaps, local):
        c.start()
        d.start()

    gates[0].start()
    small[2:7, :] = jnp.zeros((5, small.shape[1]), F32)
    for c in loads[3:9]:
        c.wait()
    unpack(2, gain)
    unpack(3, out_gain)
    small[4:7, 0:INNER] = conv_x[...].astype(F32)
    small[4:7, INNER : INNER + STATE] = conv_b[...].astype(F32)
    small[4:7, INNER + STATE : MIXED] = conv_c[...].astype(F32)
    lane = lanes_of((1, LANES))
    rates = jnp.zeros((1, LANES), F32)
    for way in range(2):
        for h in range(HEADS):
            rates = jnp.where(lane == way * HEADS + h, rate[way : way + 1, h : h + 1], rates)

    mods[0].arrived()
    mod_z[z] = summed(mod_y, ny)
    mods[1].start()

    line = []
    for slot, owner in ((0, y == 0), (1, y == ny - 1)):

        def line_copy(origin, target, k, slot=slot):
            return pltpu.make_async_remote_copy(
                src_ref=origin,
                dst_ref=target,
                send_sem=line_sems.at[slot, 0],
                recv_sem=line_sems.at[slot, 1],
                device_id={"sp_1": lax.rem(y + k, ny)},
                device_id_type=MESH,
            )

        origin, target = edge_recv.at[2 + slot], line_edge.at[slot]
        each = [line_copy(origin, target, k) for k in range(1, ny)]
        line_bulk = line_edge.at[pl.ds(0, ny - 1)]
        line.append((owner, each[0], line_copy(line_bulk, line_bulk, 1)))

        @pl.when(owner)
        def _(slot=slot, each=each):
            edges[2 + slot][1][0][0].wait_recv()
            line_edge[slot] = edge_recv[2 + slot]
            for c in each:
                c.start()


    def inverse(v):
        return lax.rsqrt(jnp.mean(v * v, axis=1, keepdims=True) + EPSILON)

    mods[1].arrived()
    mod_x[x] = summed(mod_z, nz)
    mods[2].start()

    lat_copies.arrived()
    scales = [inverse(lat[t].astype(F32)) for t in range(nx)]
    ctx_copies.arrived()
    ctx_scales = [inverse(ctx[j].astype(F32)) for j in range(ny)]
    misc[...] = jnp.zeros_like(misc)
    for c in (edges[0][1][0][0], edges[1][1][0][0]):
        c.wait_recv()
    for owner, c, _ in line:
        pl.when(jnp.logical_not(owner))(c.wait_recv)
    has = (place > 0, place < count - 1, z > 0, z < nz - 1)
    for slot in range(4):
        edge_row = edge_recv[slot] if slot < 2 else line_edge[slot - 2]
        misc[slot : slot + 1, :] = jnp.where(has[slot], edge_row, 0.0)
    misc_scale = inverse(misc[...])
    row16 = rows_of((16, 1))
    kept = jnp.zeros((16, 1), jnp.bool_)
    for slot in range(4):
        kept = jnp.logical_or(kept, jnp.logical_and(row16 == slot, has[slot]))

    bulk_local[0].wait()
    bulk_swaps[0].wait_recv()
    dt_wide[...] = jnp.zeros_like(dt_wide)
    for way in range(2):
        dt_wide[way * HEADS : (way + 1) * HEADS, :] = dt_rows[way].astype(F32)
    for b in range(model // LANES):
        at = slice(b * LANES, (b + 1) * LANES)
        weights[at, COL_DT:COL_C] = dt_wide[:, at].T.astype(BF16)
    bulk_local[1].wait()
    bulk_swaps[1].wait_recv()

    mods[2].arrived()

    def modulations(c, shift, scale):
        cols = slice(c * width, (c + 1) * width)
        return cols, small[2:3, cols] * (1.0 + mod_x[c, scale]), mod_x[c, shift]

    for c in range(nx):
        cols, scale, shift = modulations(c, 0, 1)
        _, scale_ctx, shift_ctx = modulations(c, 2, 3)
        for t in range(nx):
            value = lat[t, :, cols].astype(F32) * scales[t] * scale + shift
            hidden[t * own_rows : (t + 1) * own_rows, cols] = value.astype(BF16)
        value = misc[:, cols] * misc_scale * jnp.where(row16 < 2, scale, scale_ctx)
        value = value + jnp.where(row16 < 2, shift, shift_ctx)
        hidden[TOKENS:ctx_at, cols] = jnp.where(kept, value, 0.0).astype(BF16)
        for j in range(0, ny, 2):
            two = [
                ctx[i, :, cols].astype(F32) * ctx_scales[i] * scale_ctx + shift_ctx
                for i in (j, j + 1)
            ]
            at = ctx_at + j * CTX_ROWS
            hidden[at : at + 2 * CTX_ROWS, cols] = jnp.concatenate(two, axis=0).astype(BF16)

    def project(rows, left, right):
        while left < right:
            wide = min(256, right - left)
            cols = slice(left, left + wide)
            feats[rows, cols] = rounded(
                jnp.dot(hidden[rows, :], weights[:, cols], preferred_element_type=F32)
            )
            left += wide

    def smooth(rows, low, at, tap_at):
        cols = slice(at, at + LANES)
        feats[rows, cols] = convolved(
            feats[rows, cols],
            feats[low : low + 1, cols],
            feats[low + 1 : low + 2, cols],
            small[4:7, tap_at : tap_at + LANES],
        )

    own = slice(0, TOKENS)
    every = slice(0, ctx_at + lines)
    project(every, COL_B, COL_C)
    project(every, 0, PIECE)
    for at in (COL_B, 0, LANES):
        smooth(own, TOKENS, at, at)
    b_turned = feats[own, COL_B:COL_DT].T.astype(BF16)
    steps = softplus(feats[own, COL_DT:COL_C])
    sums = running_sums(-rates * steps, HEADS)
    ends = jnp.where(lane < HEADS, sums[TOKENS - 1 : TOKENS], sums[0:1])
    for way in range(2):
        for q in range(PAIRS):
            r = way * PAIRS + q
            decay_y[y, r : r + 1, :] = spread(ends, 2 * r)
    decay_copies = gather("sp_1", ny, y, decay_y).start()

    def slabs(axis, size, me, origin, target, piece):
        return along(
            axis,
            size,
            me,
            lambda peer: origin.at[piece, peer],
            target.at[piece, me],
            target.at[piece, pl.ds(0, size - 1)],
        )

    state_copies = []

    def send_states(way, pairs):
        for q in pairs:
            cols = slice(q * LANES, (q + 1) * LANES)
            piece = way * 2 + q // 2
            at = slice(q % 2 * LANES, (q % 2 + 1) * LANES)
            head = way * HEADS + 2 * q
            step = spread(steps, head)
            decay = spread(sums, head)
            end = decay[TOKENS - 1 : TOKENS] if way == 0 else decay[0:1]
            moved_x = rounded(feats[own, cols] * step)
            moved[way * TOKENS : (way + 1) * TOKENS, cols] = moved_x.astype(BF16)
            growth[way, :, cols] = jnp.exp(decay)
            at_end = (moved_x * jnp.exp(end - decay)).astype(BF16)
            state = jnp.dot(b_turned, at_end, preferred_element_type=F32).astype(BF16)
            for p in range(ny):
                state_send[piece, p, :, at] = state[p * slab : (p + 1) * slab]
            if q % 2 == 1:
                state_copies.append(
                    slabs("sp_1", ny, y, state_send, state_recv, piece).start()
                )
                state_recv[piece, y] = state_send[piece, y]

    send_states(0, (0, 1))
    project(every, PIECE, INNER)
    for at in range(PIECE, INNER, LANES):
        smooth(own, TOKENS, at, at)
    send_states(0, (2, 3))

    ctx_rows = slice(ctx_at, ctx_at + lines)
    for at in range(0, COL_DT, LANES):
        smooth(ctx_rows, TOKENS + 2, at, at)
    ctx_bt[...] = feats[ctx_rows, COL_B:COL_DT].T
    ctx_b = ctx_bt[pl.ds(pl.multiple_of(y * slab, slab), slab), :]
    ctx_steps = softplus(feats[ctx_rows, COL_DT:COL_C])
    ctx_sums = running_sums(-rates * ctx_steps, HEADS)
    ctx_ends = jnp.where(lane < HEADS, ctx_sums[lines - 1 : lines], ctx_sums[0:1])
    for r in range(2 * PAIRS):
        ctx_dz[z, r : r + 1, :] = spread(ctx_ends, 2 * r)
    ctx_dz_copies = gather("sp_0", nz, z, ctx_dz).start()
    ctx_copies_z = []
    is_last = z == nz - 1

    def last_copy(ref, peer):
        return pltpu.make_async_remote_copy(
            src_ref=ref,
            dst_ref=ref,
            send_sem=last_sems.at[0],
            recv_sem=last_sems.at[1],
            device_id={"sp_0": peer},
            device_id_type=MESH,
        )

    to_last = last_copy(ctx_z.at[1, z], nz - 1)
    at_last = last_copy(ctx_z.at[1, pl.ds(0, nz - 1)], z_down)

    def send_context(way):
        for q in range(PAIRS):
            cols = slice(q * LANES, (q + 1) * LANES)
            head = way * HEADS + 2 * q
            decay = spread(ctx_sums, head)
            end = decay[lines - 1 : lines] if way == 0 else decay[0:1]
            moved_x = rounded(feats[ctx_rows, cols] * spread(ctx_steps, head))
            ctx_z[way, z, :, cols] = jnp.dot(
                ctx_b,
                moved_x * jnp.exp(end - decay),
                preferred_element_type=F32,
                precision=lax.Precision.HIGHEST,
            ).astype(BF16)
        if way == 0:
            ctx_copies_z.append(gather("sp_0", nz, z, ctx_z.at[0]).start())
        else:
            pl.when(jnp.logical_not(is_last))(to_last.start)

    send_context(0)
    send_context(1)
    send_states(1, (0, 1, 2, 3))
    project(slice(0, ctx_at), COL_C, COL_Z)
    gates[0].arrived()
    gate_z[z] = summed(gate_y, ny)
    gates[1].start()

    smooth(own, TOKENS, COL_C, INNER + STATE)
    c_vals = feats[own, COL_C:COL_Z].astype(BF16)
    project(own, COL_Z, COLS)
    for at in range(COL_Z, COLS, LANES):
        feats[own, at : at + LANES] = silu(feats[own, at : at + LANES])
    scores = jnp.dot(c_vals, b_turned, preferred_element_type=F32)
    turned = sums.T
    square = (TOKENS, TOKENS)
    lower = rows_of(square) >= lanes_of(square)
    upper = rows_of(square) <= lanes_of(square)
    for q in range(PAIRS):
        cols = slice(q * LANES, (q + 1) * LANES)
        halves = []
        for h in (2 * q, 2 * q + 1):
            both = []
            for way, mask in ((0, lower), (1, upper)):
                col = way * HEADS + h
                gap = sums[:, col : col + 1] - turned[col : col + 1, :]
                decayed = scores * jnp.exp(jnp.minimum(gap, 0.0))
                both.append(jnp.where(mask, decayed, 0.0).astype(BF16))
            halves.append(
                jnp.dot(
                    jnp.concatenate(both, axis=1),
                    moved[:, cols],
                    preferred_element_type=F32,
                )
            )
        inside[:, cols] = jnp.where(lanes_of(square) < LANES // 2, halves[0], halves[1])

    decay_copies.arrived()
    decays = [decay_y[j] for j in range(ny)]
    is_fwd = rows_of((8, LANES)) < PAIRS
    ahead = [None] * ny
    acc_f = acc_b = jnp.zeros((8, LANES), F32)
    for j in range(ny):
        ahead[j] = acc_f
        acc_f = acc_f + decays[j]
    for j in reversed(range(ny)):
        ahead[j] = jnp.exp(jnp.where(is_fwd, ahead[j], acc_b))
        acc_b = acc_b + decays[j]
    tot_dz[z] = acc_f
    tot_dz_copies = gather("sp_0", nz, z, tot_dz).start()
    factors = [jnp.exp(d) for d in decays]
    tot_copies = []
    ctx_factors = []
    line_factor = jnp.exp(acc_f)

    def context_start(way, r):
        order = range(nz) if way == 0 else reversed(range(nz))
        at = (r - way * PAIRS) * LANES
        state = jnp.zeros((slab, LANES), F32)
        for j in order:
            fresh = ctx_z[way, j, :, at : at + LANES].astype(F32)
            state = state * ctx_factors[j][r : r + 1] + fresh
        return state

    last_starts = []
    for piece in range(4):
        way = piece // 2
        state_copies[piece].arrived()
        if piece == 2:
            ctx_dz_copies.arrived()
            ctx_factors += [jnp.exp(ctx_dz[j]) for j in range(nz)]
            pl.when(is_last)(at_last.wait_recv)
            for r in range(PAIRS, 2 * PAIRS):
                last_starts.append(jnp.where(is_last, context_start(1, r), 0.0))
        for q in range(2):
            cols = slice(q * LANES, (q + 1) * LANES)
            r = piece * 2 + q
            state = jnp.zeros((slab, LANES), F32)
            for j in range(ny) if way == 0 else reversed(range(ny)):
                before[piece, j, :, cols] = state
                state = state * factors[j][r : r + 1] + state_recv[piece, j, :, cols].astype(F32)
            if way == 1:
                state = state + line_factor[r : r + 1] * last_starts[r - PAIRS]
            tot_z[piece, z, :, cols] = state.astype(BF16)
        tot_copies.append(
            Totals(way, tot_z.at[piece], nz, z, tot_sems.at[piece]).start()
        )

    gates[1].arrived()
    gate_x[x] = summed(gate_z, nz)
    gates[2].start()
    tot_dz_copies.arrived()
    tot_factors = [jnp.exp(tot_dz[j]) for j in range(nz)]
    enter_copies = []
    for piece in range(4):
        way = piece // 2
        order = list(range(nz)) if way == 0 else list(reversed(range(nz)))
        if piece == 0:
            ctx_copies_z[0].arrived()
        starts = [
            context_start(0, r) if way == 0 else last_starts[r - PAIRS]
            for r in (piece * 2, piece * 2 + 1)
        ]
        tot_copies[piece].arrived()
        for q in range(2):
            cols = slice(q * LANES, (q + 1) * LANES)
            r = piece * 2 + q
            state = starts[q]
            for j in order:
                passed = j < z if way == 0 else j > z
                later = state * tot_factors[j][r : r + 1] + tot_z[piece, j, :, cols].astype(F32)
                state = jnp.where(passed, later, state)
            for j in range(ny):
                enter_send[piece, j, :, cols] = (
                    before[piece, j, :, cols] + ahead[j][r : r + 1] * state
                ).astype(BF16)
        enter_copies.append(slabs("sp_1", ny, y, enter_send, enter_recv, piece).start())
        enter_recv[piece, y] = enter_send[piece, y]

    squares = jnp.zeros((TOKENS, 1), F32)
    for piece in range(4):
        way = piece // 2
        enter_copies[piece].arrived()
        carried = jnp.dot(
            c_vals, enter_recv[piece].reshape(STATE, PIECE), preferred_element_type=F32
        )
        for q in range(2):
            at = (piece % 2) * PIECE + q * LANES
            cols = slice(at, at + LANES)
            value = inside[:, cols]
            value = value + growth[way, :, cols] * carried[:, q * LANES : (q + 1) * LANES]
            if way == 1:
                value = value * feats[own, COL_Z + at : COL_Z + at + LANES]
                squares = squares + jnp.sum(value * value, axis=1, keepdims=True)
            inside[:, cols] = value
    scale = lax.rsqrt(squares / INNER + EPSILON)
    for q in range(PAIRS):
        cols = slice(q * LANES, (q + 1) * LANES)
        normed[:, cols] = (inside[:, cols] * scale * small[3:4, cols]).astype(BF16)

    bulk_local[-1].wait()
    bulk_swaps[-1].wait_recv()
    part_copies = []
    for c in range(nx):
        cols = slice(c * width, (c + 1) * width)
        term = jnp.dot(normed[...], out_weights[:, cols], preferred_element_type=F32)
        term = term.astype(BF16)
        for t in range(nx):
            part_send[t, :, cols] = term[t * own_rows : (t + 1) * own_rows]
        part_copies.append(
            along(
                "tp",
                nx,
                x,
                lambda peer, cols=cols: part_send.at[peer, :, cols],
                parts.at[x, :, cols],
                parts.at[pl.ds(0, nx - 1), :, cols],
            ).start()
        )
    parts[x] = part_send[x]
    for owner, _, whole in line:
        pl.when(owner)(whole.wait_send)
    for e in bulk_swaps:
        e.wait_send()
    pl.when(jnp.logical_not(is_last))(to_last.wait_send)
    gates[2].arrived()
    for owner, (_, whole) in edges:
        pl.when(owner)(whole.wait_send)

    done = mods + gates + [ctx_copies, lat_copies, decay_copies, ctx_dz_copies, tot_dz_copies]
    done += ctx_copies_z + state_copies + tot_copies + enter_copies
    for e in done + part_copies:
        e.left()
    for c in range(nx):
        cols = slice(c * width, (c + 1) * width)
        part_copies[c].arrived()
        value = parts[0, :, cols].astype(F32)
        for t in range(1, nx):
            value = value + parts[t, :, cols].astype(F32)
        update[:, cols] = (gate_x[c, 0] * value).astype(BF16)


def shards(
    sizes,
    latent,
    condition,
    context,
    context_source,
    mod_weight,
    norm_gain,
    w_x,
    w_b,
    w_c,
    w_z,
    w_dt,
    conv_x,
    conv_b,
    conv_c,
    decay_rate,
    out_gain,
    w_out,
):
    nz, ny, nx = sizes
    model = latent.shape[-1]
    own_rows = latent.shape[1]
    width = model // nx
    slab = STATE // ny
    span = max(model, 1024)
    rows = mod_weight.shape[1]
    lines = ny * CTX_ROWS
    total_rows = TOKENS + 16 + lines
    vmem = pl.BlockSpec(memory_space=pltpu.VMEM)
    hbm = pl.BlockSpec(memory_space=pl.ANY)
    dma = pltpu.SemaphoreType.DMA
    scratch = [
        pltpu.VMEM((1, model), BF16),
        pltpu.VMEM((model // LANES, LANES), BF16),
        pltpu.VMEM((model // LANES, LANES), BF16),
        pltpu.VMEM((INNER // LANES, LANES), BF16),
        pltpu.VMEM((3, INNER), BF16),
        pltpu.VMEM((3, STATE), BF16),
        pltpu.VMEM((3, STATE), BF16),
        pltpu.VMEM((2, HEADS), F32),
        pltpu.VMEM((3, rows, width), BF16),
        pltpu.VMEM((model, COLS), BF16),
        pltpu.VMEM((INNER, model), BF16),
        pltpu.VMEM((2, HEADS, model), BF16),
        pltpu.VMEM((LANES, model), F32),
        pltpu.VMEM((8, span), F32),
        pltpu.VMEM((nx, own_rows, model), BF16),
        pltpu.VMEM((ny, CTX_ROWS, model), BF16),
        pltpu.VMEM((3, max(rows, LANES), width), BF16),
        pltpu.VMEM((nz, 4, 1, width), F32),
        pltpu.VMEM((ny, 4, 1, width), F32),
        pltpu.VMEM((nx, 4, 1, width), F32),
        pltpu.VMEM((ny, 1, 1, width), F32),
        pltpu.VMEM((nz, 1, 1, width), F32),
        pltpu.VMEM((nx, 1, 1, width), F32),
        pltpu.VMEM((4, 1, model), F32),
        pltpu.VMEM((4, 1, model), F32),
        pltpu.VMEM((ny, 1, model), F32),
        pltpu.VMEM((16, model), F32),
        pltpu.VMEM((total_rows, model), BF16),
        pltpu.VMEM((total_rows, COLS), F32),
        pltpu.VMEM((2 * TOKENS, INNER), BF16),
        pltpu.VMEM((2, TOKENS, INNER), F32),
        pltpu.VMEM((TOKENS, INNER), F32),
        pltpu.VMEM((STATE, lines), F32),
        pltpu.VMEM((2, nz, slab, INNER), BF16),
        pltpu.VMEM((nz, 8, LANES), F32),
        pltpu.VMEM((4, ny, slab, PIECE), BF16),
        pltpu.VMEM((4, ny, slab, PIECE), BF16),
        pltpu.VMEM((ny, 8, LANES), F32),
        pltpu.VMEM((4, nz, slab, PIECE), BF16),
        pltpu.VMEM((nz, 8, LANES), F32),
        pltpu.VMEM((4, ny, slab, PIECE), F32),
        pltpu.VMEM((4, ny, slab, PIECE), BF16),
        pltpu.VMEM((4, ny, slab, PIECE), BF16),
        pltpu.VMEM((TOKENS, INNER), BF16),
        pltpu.VMEM((nx, own_rows, model), BF16),
        pltpu.VMEM((nx, own_rows, model), BF16),
        dma((15,)),
        dma((3,)),
        dma((3,)),
        dma((20 + nx, 2)),
        dma((4,)),
        dma((4,)),
        dma((4, 2)),
        dma((2,)),
        dma((2, 2)),
    ]
    update = pl.pallas_call(
        functools.partial(mixer, (nz, ny, nx, model)),
        out_shape=pltpu.VMEM((own_rows, model), BF16),
        in_specs=[hbm] * 17,
        out_specs=vmem,
        scratch_shapes=scratch,
        compiler_params=pltpu.CompilerParams(
            collective_id=0, has_side_effects=True, vmem_limit_bytes=56 * 1024 * 1024
        ),
    )(
        condition,
        context_source.reshape(-1, LANES),
        norm_gain.reshape(-1, LANES),
        out_gain.reshape(-1, LANES),
        conv_x,
        conv_b,
        conv_c,
        decay_rate,
        mod_weight,
        context[0],
        latent[0],
        w_x,
        w_b,
        w_c,
        w_z,
        jnp.swapaxes(w_dt, 1, 2),
        w_out,
    )
    return update[None]


def solution(mesh):
    nx = mesh.shape["tp"]
    ny = 8
    nz = mesh.shape["sp"] // ny
    return program(mesh, nz, ny, nx)


def program(mesh, nz, ny, nx):
    torus = Mesh(
        mesh.devices.reshape(nz, ny, nx, mesh.shape["dp"]), ("sp_0", "sp_1", "tp", "dp")
    )
    placed = (
        P("dp", SP_TP, None),
        P("dp", None),
        P("dp", SP, None),
        P(),
        P(None, SP, "tp"),
        P(),
        P("dp", "tp"),
        P("dp", "tp"),
        P("dp", "tp"),
        P("dp", "tp"),
        P(None, "dp", "tp"),
        P(None, "tp"),
        P(None, "tp"),
        P(None, "tp"),
        P(None, "tp"),
        P("tp"),
        P(("tp", "dp"), None),
    )
    return jax.shard_map(
        functools.partial(shards, (nz, ny, nx)),
        mesh=torus,
        in_specs=placed,
        out_specs=P("dp", SP_TP, None),
        check_vma=False,
    )
```
